32 devices in a mesh: grp: 2 (over y), sp: 4 (over z), tp: 4 (over x, core).
Axes of the slice: x: 2, y: 2, z: 4, core: 2. Of those that a mesh axis runs over, the one named last changes fastest.
Arguments:
- stream: bfloat16 [3072, 4096], P(('grp', 'sp'), 'tp'), parts along dimension 0, may hold values from -6 to 6
- norm_gain: bfloat16 [2, 4096], replicated, may hold values from 0.099609375 to 1.8984375
- w_signal: bfloat16 [2, 4096, 1024], P(None, 'sp', 'tp'), may hold values from -0.09375 to 0.09375
- w_gate: bfloat16 [2, 4096, 1024], P(None, 'sp', 'tp'), may hold values from -0.09375 to 0.09375
- conv_taps: bfloat16 [2, 31, 1024], P(None, None, 'tp'), may hold values from -4 to 4
- conv_bias: bfloat16 [2, 1024], P(None, 'tp'), may hold values from -3 to 3
- ln_gain: bfloat16 [2, 1024], P(None, 'tp'), may hold values from 0.099609375 to 1.8984375
- ln_shift: bfloat16 [2, 1024], P(None, 'tp'), may hold values from -3 to 3
- w_out: bfloat16 [2, 1024, 4096], P(None, 'sp', 'tp'), may hold values from -0.375 to 0.375
Outputs:
- mixed_stream: bfloat16 [3072, 4096], P(('grp', 'sp'), 'tp'), parts along dimension 0
The draws below stay inside these ranges and needn't reach their ends.
There are 2 independent parts, one for each index of `grp`. The reference program is written for one: setup_inputs(seed, part) draws one part's arguments, and reference() takes and returns one part's arrays. A program takes and returns all parts, laid end to end along the dimension named above; an argument that names none is the same for every part. Nothing has to cross between parts.
All inputs are finite; a program needn't handle non-finite values.
Results may differ from the reference program's by a relative error of at most 0.01.
Values may be sent and summed in bfloat16 or wider, within the bound.
A program may use at most 64 MiB of HBM per device.

```python
import jax
import jax.numpy as jnp
from jax import lax

D = 4096
C = 1024
KERNEL = 31
LAYERS = 2
TOKENS = 1536


def draw_conv_taps(key, part):
    key_base = jax.random.fold_in(key, 11)
    key_scale = jax.random.fold_in(key, 12)
    base = jnp.clip(jax.random.normal(key_base, (LAYERS, KERNEL, C), jnp.float32), -4.0, 4.0) * KERNEL ** (-0.5)
    log_scale = jax.random.uniform(key_scale, (LAYERS, 8), jnp.float32, jnp.log(0.3), jnp.log(3.0))
    scales = jnp.repeat(jnp.exp(log_scale), C // 8, axis=1)
    return (base * scales[:, None, :]).astype(jnp.bfloat16)


def levels(stream_key, shape, pieces, least, high):
    def one(position, blocks):
        heights = jax.random.uniform(jax.random.fold_in(jax.random.fold_in(stream_key, 6), position), (blocks,), jnp.float32, least / len(pieces), high / len(pieces))
        return jnp.repeat(jnp.exp(heights), shape[position] // blocks).reshape((-1,) + (1,) * (len(shape) - position - 1))

    level = one(*pieces[0])
    for cut in pieces[1:]:
        level = level * one(*cut)
    return level


def gaussian(rng, dims, scale, most, pieces=(), kind=jnp.bfloat16):
    values = jax.random.normal(rng, dims, jnp.float32) * scale
    if len(pieces) > 0:
        values = levels(rng, dims, pieces, -0.22, 0.18) * values
    return jnp.clip(values, min=-most, max=most).astype(kind)


def setup_inputs(seed: int = 0, part: int = 0) -> dict:
    arg_keys = jax.random.split(jax.random.key(seed), 10)
    part_keys = jax.random.split(jax.random.fold_in(arg_keys[9], part), 10)
    stream = gaussian(part_keys[0], (TOKENS, D), 1.0, 6.0, ((0, 4), (1, 4)))
    norm_gain = jnp.clip(1.0 + 0.18 * jax.random.normal(arg_keys[1], (LAYERS, D), jnp.float32), 0.099609375, 1.8984375).astype(jnp.bfloat16)
    w_signal = gaussian(arg_keys[2], (LAYERS, D, C), D ** -0.5, 0.09375, ((1, 4), (2, 4)))
    w_gate = gaussian(arg_keys[3], (LAYERS, D, C), D ** -0.5, 0.09375, ((1, 4), (2, 4)))
    conv_taps = draw_conv_taps(jax.random.fold_in(arg_keys[9], 71), part)
    conv_bias = gaussian(arg_keys[5], (LAYERS, C), 0.5, 3.0, ((1, 4),))
    ln_gain = jnp.clip(1.0 + 0.18 * jax.random.normal(arg_keys[6], (LAYERS, C), jnp.float32), 0.099609375, 1.8984375).astype(jnp.bfloat16)
    ln_shift = gaussian(arg_keys[7], (LAYERS, C), 0.5, 3.0, ((1, 4),))
    w_out = gaussian(arg_keys[8], (LAYERS, C, D), (C // 4) ** -0.5, 0.375, ((1, 4), (2, 4)))
    return {"stream": stream, "norm_gain": norm_gain, "w_signal": w_signal, "w_gate": w_gate, "conv_taps": conv_taps, "conv_bias": conv_bias, "ln_gain": ln_gain, "ln_shift": ln_shift, "w_out": w_out}


EPS = 1e-05

def product(left, right):
    return jnp.dot(left, right, preferred_element_type=jnp.float32)

def layer_step(stream, gain, signal_w, gate_w, taps, bias, norm_g, norm_b, out_w):
    widened = stream.astype(jnp.float32)
    normed = (widened * lax.rsqrt(lax.optimization_barrier(jnp.mean(widened * widened, axis=-1, keepdims=True)) + EPS) * gain.astype(jnp.float32)).astype(jnp.bfloat16)
    signal = product(normed, signal_w)
    gate_pre = product(normed, gate_w)
    blended = (signal * jax.nn.sigmoid(gate_pre)).astype(jnp.bfloat16)
    fringe_rows = taps.shape[0] - 1
    padded = jnp.concatenate([jnp.zeros((fringe_rows, blended.shape[1]), jnp.bfloat16), blended], axis=0)
    length = blended.shape[0]
    filtered = jnp.zeros((length, blended.shape[1]), jnp.float32) + bias.astype(jnp.float32)
    tap_rows = taps.astype(jnp.float32)
    for tap_index in range(fringe_rows + 1):
        filtered = filtered + tap_rows[tap_index] * padded[tap_index:tap_index + length].astype(jnp.float32)
    average = lax.optimization_barrier(jnp.mean(filtered, axis=-1, keepdims=True))
    spread = lax.optimization_barrier(jnp.mean(filtered * filtered, axis=-1, keepdims=True)) - average * average
    scaled = (filtered - average) * lax.rsqrt(spread + EPS) * norm_g.astype(jnp.float32) + norm_b.astype(jnp.float32)
    activated = jax.nn.silu(scaled).astype(jnp.bfloat16)
    return (widened + product(activated, out_w)).astype(jnp.bfloat16)

def reference(stream, norm_gain, w_signal, w_gate, conv_taps, conv_bias, ln_gain, ln_shift, w_out):
    current = stream
    for layer_index in range(LAYERS):
        current = layer_step(current, norm_gain[layer_index], w_signal[layer_index], w_gate[layer_index], conv_taps[layer_index], conv_bias[layer_index], ln_gain[layer_index], ln_shift[layer_index], w_out[layer_index])
    return current
```

```python
import functools

import jax
import jax.numpy as jnp
from jax import lax
from jax.experimental import pallas as pl
from jax.experimental.pallas import tpu as pltpu
from jax.sharding import PartitionSpec as P

MESH = pl.DeviceIdType.MESH
EPS = 1e-05
F32 = jnp.float32
BF16 = jnp.bfloat16
SIG, GATE, OUT = 0, 1, 2
CHUNK = 32
PIECES = 2


def sigmoid(v):
    return 1.0 / (1.0 + jnp.exp(-v))


def kernel(
    sizes,
    stream, gain, w_signal, w_gate, taps, bias, ln_gain, ln_shift, w_out,
    result,
    sig_all, gate_all, out_all, feats, scaled_feats, inv, acc_sig, acc_gate,
    tail, halo, padded, filt, stat_cols, stat_rows, acts,
    load_sem, stream_sem, own_send, z_send, z_recv, y_send, y_recv,
    cross_send, cross_recv, core_send, core_recv,
    halo_send, halo_recv, stat_send, stat_recv,
):
    groups, sp, tp, layers, rows, kernel_taps, hp, width, channels = sizes
    g, s, t = lax.axis_index("grp"), lax.axis_index("sp"), lax.axis_index("tp")
    chips = tp // 2
    core, chip = lax.rem(t, 2), lax.div(t, 2)
    mate = t + 1 - 2 * core
    share = sp // tp
    banks = (sig_all, gate_all, out_all)
    held = (w_signal, w_gate, w_out)

    inner = (s > 0) & (s < sp - 1)
    pieces = [w.shape[2] for w in held]

    def load(l, k):
        return pltpu.make_async_copy(held[k].at[l], banks[k].at[l, s], load_sem.at[l, k])

    own_stream = pltpu.make_async_copy(stream, feats.at[0, t], stream_sem)
    own_stream.start()
    for l in range(layers):
        for k in range(3):
            load(l, k).start()

    barrier = pltpu.get_barrier_semaphore()

    def greet(where):
        pl.semaphore_signal(barrier, inc=1, device_id=where, device_id_type=MESH)

    @pl.when(s > 0)
    def _():
        greet({"sp": s - 1})

    @pl.when(s < sp - 1)
    def _():
        greet({"sp": s + 1})

    for i in range(1, groups):
        greet({"grp": lax.rem(g + i, groups)})
    for i in range(1, tp):
        greet({"tp": lax.rem(t + i, tp)})
    pl.semaphore_wait(
        barrier,
        jnp.where(s > 0, 1, 0) + jnp.where(s < sp - 1, 1, 0) + (groups - 1 + tp - 1),
    )

    def z_copy(l, k, q, shard, way, mine=False):
        ref = banks[k].at[l, shard, g, q]
        return pltpu.make_async_remote_copy(
            src_ref=ref, dst_ref=ref,
            send_sem=own_send.at[l, k, q] if mine and way else z_send.at[l, k, q, shard],
            recv_sem=z_recv.at[l, k, q, shard],
            device_id={"sp": s + 1 if way == 0 else s - 1}, device_id_type=MESH,
        )

    def y_copy(l, k, q, shard, half, where):
        ref = banks[k].at[l, shard, half, q]
        return pltpu.make_async_remote_copy(
            src_ref=ref, dst_ref=ref,
            send_sem=y_send.at[l, k, q, shard], recv_sem=y_recv.at[l, k, q, shard],
            device_id=where, device_id_type=MESH,
        )

    def own(l, k, done=False):
        if not done:
            load(l, k).wait()
        for way, there, end in ((0, s < sp - 1, s == 0), (1, s > 0, s == sp - 1)):
            @pl.when(there)
            def _(way=way, end=end):
                for q in range(pieces[k]):
                    copy = z_copy(l, k, q, s, way, True)
                    copy.wait_send() if done else copy.start()

                @pl.when(end)
                def _():
                    for q in range(pieces[k]):
                        where = {"sp": s + 1 if way == 0 else s - 1}
                        copy = y_copy(l, k, q, s, 1 - g, where)
                        copy.wait_send() if done else copy.start()

    def sides(d):
        left, right = s - 1 - d, s + 1 + d
        return (
            (0, left, left >= 0, s < sp - 1, (left > 0) | (d > 0)),
            (1, right, right <= sp - 1, s > 0, (right < sp - 1) | (d > 0)),
        )

    def relay(l, k, d, done=False):
        for way, shard, here, onward, across in sides(d):
            @pl.when(here)
            def _(way=way, shard=shard, onward=onward, across=across):
                for q in range(pieces[k]):
                    if not done:
                        z_copy(l, k, q, shard, way).wait_recv()

                    @pl.when(onward)
                    def _():
                        copy = z_copy(l, k, q, shard, way)
                        copy.wait_send() if done else copy.start()

                    @pl.when(across)
                    def _():
                        copy = y_copy(l, k, q, shard, g, {"grp": 1 - g})
                        copy.wait_send() if done else copy.start()

    def other_half(l, k, d):
        for _, shard, here, _, _ in sides(d):
            @pl.when(here)
            def _(shard=shard):
                for q in range(pieces[k]):
                    y_copy(l, k, q, shard, 1 - g, {"grp": 1 - g}).wait_recv()

    def cross_copy(buf, n, block, i):
        ref = buf.at[block]
        return pltpu.make_async_remote_copy(
            src_ref=ref, dst_ref=ref,
            send_sem=cross_send.at[n, i], recv_sem=cross_recv.at[n, block],
            device_id={"tp": lax.rem(chip + i, chips) * 2 + core}, device_id_type=MESH,
        )

    def core_copy(buf, n, block):
        ref = buf.at[block]
        return pltpu.make_async_remote_copy(
            src_ref=ref, dst_ref=ref,
            send_sem=core_send.at[n, block], recv_sem=core_recv.at[n, block],
            device_id={"tp": mate}, device_id_type=MESH,
        )

    def spread_start(buf, n):
        for i in range(1, chips):
            cross_copy(buf, n, t, i).start()
        core_copy(buf, n, t).start()

    def spread_relay(buf, n):
        for i in range(1, chips):
            block = lax.rem(chip + i, chips) * 2 + core
            cross_copy(buf, n, block, i).wait_recv()
            core_copy(buf, n, block).start()

    def spread_wait(buf, n):
        for j in range(chips):
            core_copy(buf, n, j * 2 + 1 - core).wait_recv()

    def spread_done(buf, n):
        for i in range(1, chips):
            cross_copy(buf, n, t, i).wait_send()
        for j in range(chips):
            core_copy(buf, n, j * 2 + core).wait_send()

    def stat_copy(l, i, block):
        return pltpu.make_async_remote_copy(
            src_ref=stat_rows.at[l, block], dst_ref=stat_rows.at[l, block],
            send_sem=stat_send.at[l, i], recv_sem=stat_recv.at[l, block],
            device_id={"tp": lax.rem(t + i, tp)}, device_id_type=MESH,
        )

    def halo_copy(l):
        return pltpu.make_async_remote_copy(
            src_ref=tail.at[l], dst_ref=halo.at[l],
            send_sem=halo_send.at[l], recv_sem=halo_recv.at[l],
            device_id={"sp": s + 1}, device_id_type=MESH,
        )

    def normalise(l):
        part = width // tp

        def body(c, carry):
            at = pl.ds(pl.multiple_of(c * CHUNK, CHUNK), CHUNK)
            total = jnp.zeros((CHUNK, 1), F32)
            for b in range(tp):
                x = feats[l, b, at, :].astype(F32)
                total = total + jnp.sum(x * x, axis=1, keepdims=True)
                scaled_feats[b, at, :] = (
                    x * gain[l : l + 1, b * part : (b + 1) * part].astype(F32)
                ).astype(BF16)
            inv[at, :] = jnp.broadcast_to(lax.rsqrt(total / width + EPS), (CHUNK, 128))
            return carry

        lax.fori_loop(0, rows // CHUNK, body, 0)

    local = channels // tp

    def project(l):
        for k, acc in ((SIG, acc_sig), (GATE, acc_gate)):
            def body(b, carry, k=k, acc=acc):
                w = banks[k][l, pl.ds(b * share, share)].reshape(width // tp, local)
                acc[...] += jnp.dot(scaled_feats[b], w, preferred_element_type=F32)
                return carry

            acc[...] = jnp.zeros_like(acc)
            for d in range(sp - 1):
                other_half(l, k, d)
            lax.fori_loop(0, tp, body, 0)

        def blend(c, carry):
            at = pl.ds(pl.multiple_of(c * CHUNK, CHUNK), CHUNK)
            r = inv[at, 0:1]
            v = (acc_sig[at, :] * r) * sigmoid(acc_gate[at, :] * r)
            to = pl.ds(pl.multiple_of(hp + c * CHUNK, 8), CHUNK)
            padded[to, :] = v.astype(BF16).astype(F32)
            return carry

        lax.fori_loop(0, rows // CHUNK, blend, 0)
        tail[l] = padded[rows : rows + hp, :].astype(BF16)

        @pl.when(s < sp - 1)
        def _():
            halo_copy(l).start()

    def convolve(l):
        def settle():
            @pl.when(s > 0)
            def _():
                halo_copy(l).wait_recv()
                padded[0:hp, :] = halo[l].astype(F32)

            @pl.when(s == 0)
            def _():
                padded[0:hp, :] = jnp.zeros((hp, local), F32)

        tap_rows = taps[:, l, :].astype(F32)
        first = hp - (kernel_taps - 1)
        lane = lax.broadcasted_iota(jnp.int32, (CHUNK, 128), 1)
        for c in [*range(1, rows // CHUNK), 0]:
            if c == 0:
                settle()
            low = c * CHUNK
            total = jnp.broadcast_to(bias[l : l + 1, :].astype(F32), (CHUNK, local))
            for j in range(kernel_taps):
                start = low + first + j
                total = total + tap_rows[j : j + 1, :] * padded[start : start + CHUNK, :]
            filt[low : low + CHUNK, :] = total
            one = jnp.sum(total, axis=1, keepdims=True)
            two = jnp.sum(total * total, axis=1, keepdims=True)
            stat_cols[low : low + CHUNK, :] = jnp.where(
                lane == 0, one, jnp.where(lane == 1, two, 0.0)
            )
        stat_rows[l, t] = jnp.transpose(stat_cols[...])[0:8, :]
        for i in range(1, tp):
            stat_copy(l, i, t).start()

    def activate(l):
        for i in range(1, tp):
            stat_copy(l, i, lax.rem(t + i, tp)).wait_recv()
        sums = jnp.sum(stat_rows[l], axis=0)
        stat_cols[...] = jnp.transpose(
            jnp.concatenate([sums, jnp.zeros((120, rows), F32)], axis=0)
        )
        gains, shifts = ln_gain[l : l + 1, :].astype(F32), ln_shift[l : l + 1, :].astype(F32)

        def body(c, carry):
            at = pl.ds(pl.multiple_of(c * CHUNK, CHUNK), CHUNK)
            average = stat_cols[at, 0:1] / channels
            spread = stat_cols[at, 1:2] / channels - average * average
            v = (filt[at, :] - average) * lax.rsqrt(spread + EPS) * gains + shifts
            acts[l, t, at, :] = (v * sigmoid(v)).astype(BF16)
            return carry

        lax.fori_loop(0, rows // CHUNK, body, 0)

    def update(l):
        columns = width // tp
        tile = min(256, columns)
        deep = 128

        def body(c, carry):
            at = pl.ds(pl.multiple_of(c * deep, deep), deep)
            for n in range(columns // tile):
                cut = slice(n * tile, (n + 1) * tile)
                total = feats[l, t, at, cut].astype(F32)
                for b in range(tp):
                    w = out_all[l, b * share : (b + 1) * share, :, :, :, cut].reshape(local, tile)
                    total = total + jnp.dot(acts[l, b, at, :], w, preferred_element_type=F32)
                if l + 1 < layers:
                    feats[l + 1, t, at, cut] = total.astype(BF16)
                else:
                    result[at, cut] = total.astype(BF16)
            return carry

        lax.fori_loop(0, rows // deep, body, 0)

    hops = range(sp - 1)
    own(0, SIG)
    own(0, GATE)
    own_stream.wait()
    spread_start(feats.at[0], 0)
    for l in range(layers):
        x_cut = [(d, k) for d in hops for k in (SIG, GATE)]
        middle = len(x_cut) - 3 if l == 0 else len(x_cut) - 2
        for i, (d, k) in enumerate(x_cut):
            if l and i == 0:
                continue
            if i == middle:
                if l:
                    own(l, OUT)
                spread_relay(feats.at[l], 2 * l)
            relay(l, k, d)
        if l == 0:
            own(l, OUT)
        spread_wait(feats.at[l], 2 * l)
        normalise(l)
        project(l)

        @pl.when(inner)
        def _(l=l):
            for d in hops:
                relay(l, OUT, d)

        if l + 1 < layers:
            own(l + 1, SIG)
            own(l + 1, GATE)
        convolve(l)

        @pl.when(jnp.logical_not(inner))
        def _(l=l):
            for d in hops:
                relay(l, OUT, d)

        activate(l)
        spread_start(acts.at[l], 2 * l + 1)
        if l + 1 < layers:
            relay(l + 1, SIG, 0)
        spread_relay(acts.at[l], 2 * l + 1)
        for d in hops:
            other_half(l, OUT, d)
        spread_wait(acts.at[l], 2 * l + 1)
        update(l)
        if l + 1 < layers:
            spread_start(feats.at[l + 1], 2 * l + 2)

    for l in range(layers):
        for k in (SIG, GATE, OUT):
            own(l, k, done=True)
            for d in hops:
                relay(l, k, d, done=True)
        spread_done(feats.at[l], 2 * l)
        spread_done(acts.at[l], 2 * l + 1)
        for i in range(1, tp):
            stat_copy(l, i, t).wait_send()

        @pl.when(s < sp - 1)
        def _(l=l):
            halo_copy(l).wait_send()


def direct(l, k, q, count):
    return l > 0 or k == OUT or q < count - 1 or count == 1


def fold_kernel(
    sizes,
    stream, gain, w_signal, w_gate, taps, bias, ln_gain, ln_shift, w_out,
    result,
    sig_all, gate_all, out_all, feats, far, scaled, squares, acc_sig, acc_gate,
    back, tail, halo, padded, filt, stat_cols, stat_rows, acts,
    load_sem, stream_sem, z_send, end_send, z_recv, y_send, y_recv,
    cross_send, cross_recv, core_send, core_recv,
    far_send, far_recv, back_send, back_recv,
    halo_send, halo_recv, stat_send, stat_recv,
):
    groups, sp, tp, layers, rows, kernel_taps, hp, width, channels = sizes
    g, s, t = lax.axis_index("grp"), lax.axis_index("sp"), lax.axis_index("tp")
    chips = tp // 2
    core, chip = lax.rem(t, 2), lax.div(t, 2)
    mate = t + 1 - 2 * core
    last, middle = sp - 1, sp // 2
    outer = (s == 0) | (s == last)
    inner = jnp.logical_not(outer)
    pair = s + 1 - 2 * lax.rem(s, 2)
    mid = jnp.where(outer, pair, s)
    end = jnp.where(outer, s, pair)
    mid2, end2 = last - mid, last - end
    banks = (sig_all, gate_all, out_all)
    held = (w_signal, w_gate, w_out)
    pieces = [w.shape[2] for w in held]
    local, part = channels // tp, width // tp
    parts = ((128, rows - 128), (0, 128))
    both = range(len(parts))
    other_group = {"grp": 1 - g}

    def load(l, k):
        return pltpu.make_async_copy(held[k].at[l], banks[k].at[l, s], load_sem.at[l, k])

    own_stream = pltpu.make_async_copy(stream, feats.at[0, t], stream_sem)
    own_stream.start()
    for l in range(layers):
        for k in range(3):
            load(l, k).start()

    barrier = pltpu.get_barrier_semaphore()

    def greet(where):
        pl.semaphore_signal(barrier, inc=1, device_id=where, device_id_type=MESH)

    @pl.when(s > 0)
    def _():
        greet({"sp": s - 1})

    @pl.when(s < last)
    def _():
        greet({"sp": s + 1})

    for i in range(1, groups):
        greet({"grp": lax.rem(g + i, groups)})
    for i in range(1, tp):
        greet({"tp": lax.rem(t + i, tp)})
    pl.semaphore_wait(
        barrier,
        jnp.where(s > 0, 1, 0) + jnp.where(s < last, 1, 0) + (groups - 1 + tp - 1),
    )

    def z_copy(l, k, q, shard, to, sems):
        ref = banks[k].at[l, shard, g, q]
        return pltpu.make_async_remote_copy(
            src_ref=ref, dst_ref=ref,
            send_sem=sems.at[l, k, q, shard], recv_sem=z_recv.at[l, k, q, shard],
            device_id={"sp": to}, device_id_type=MESH,
        )

    def y_copy(l, k, q, shard, half, where):
        ref = banks[k].at[l, shard, half, q]
        return pltpu.make_async_remote_copy(
            src_ref=ref, dst_ref=ref,
            send_sem=y_send.at[l, k, q, shard], recv_sem=y_recv.at[l, k, q, shard],
            device_id=where, device_id_type=MESH,
        )

    def flow(copy, done):
        copy.wait_send() if done else copy.start()

    def across(l, k, q, shard, done=False):
        flow(y_copy(l, k, q, shard, g, other_group), done)

    def to_end(l, k, q, shard, done=False):
        flow(z_copy(l, k, q, shard, end, end_send), done)

    def to_middle(l, k, q, shard, done=False):
        flow(z_copy(l, k, q, shard, mid2, z_send), done)

    def lift(l, k, q, done=False):
        flow(z_copy(l, k, q, s, mid, z_send), done)

    def lift_other(l, k, q, done=False):
        if direct(l, k, q, pieces[k]):
            flow(y_copy(l, k, q, s, 1 - g, {"sp": mid}), done)

    def arrived(l, k, q, shard):
        z_copy(l, k, q, shard, mid, z_send).wait_recv()

    def each(l, kinds, act):
        for k in kinds:
            for q in range(pieces[k]):
                act(l, k, q)

    def pass_on(l, k, q):
        arrived(l, k, q, end)
        to_middle(l, k, q, end)
        if not direct(l, k, q, pieces[k]):
            across(l, k, q, end)

    def take(shard, onward=True):
        def act(l, k, q):
            arrived(l, k, q, shard)
            across(l, k, q, shard)
            if onward:
                to_end(l, k, q, shard)
        return act

    def onward(shard):
        return lambda l, k, q: to_end(l, k, q, shard)

    def ready(l, k, shard):
        for q in range(pieces[k]):
            y_copy(l, k, q, shard, 1 - g, other_group).wait_recv()

    def ready_all(l, k):
        for shard in (pair, mid2, end2):
            ready(l, k, shard)

    def rows_of(h):
        return pl.ds(parts[h][0], parts[h][1])

    def cross_copy(buf, n, h, block, i):
        ref = buf.at[block, rows_of(h)]
        return pltpu.make_async_remote_copy(
            src_ref=ref, dst_ref=ref,
            send_sem=cross_send.at[n, h, i], recv_sem=cross_recv.at[n, h, block],
            device_id={"tp": lax.rem(chip + i, chips) * 2 + core}, device_id_type=MESH,
        )

    def core_copy(buf, n, h, block):
        ref = buf.at[block, rows_of(h)]
        return pltpu.make_async_remote_copy(
            src_ref=ref, dst_ref=ref,
            send_sem=core_send.at[n, h, block], recv_sem=core_recv.at[n, h, block],
            device_id={"tp": mate}, device_id_type=MESH,
        )

    def spread_start(buf, n, h):
        for i in range(1, chips):
            cross_copy(buf, n, h, t, i).start()
        core_copy(buf, n, h, t).start()

    def spread_relay(buf, n, h):
        for i in range(1, chips):
            block = lax.rem(chip + i, chips) * 2 + core
            cross_copy(buf, n, h, block, i).wait_recv()
            core_copy(buf, n, h, block).start()

    def spread_near(buf, n, h):
        core_copy(buf, n, h, mate).wait_recv()

    def spread_rest(buf, n, h):
        for i in range(1, chips):
            core_copy(buf, n, h, lax.rem(chip + i, chips) * 2 + 1 - core).wait_recv()

    def spread_done(buf, n):
        for h in both:
            for i in range(1, chips):
                cross_copy(buf, n, h, t, i).wait_send()
            for j in range(chips):
                core_copy(buf, n, h, j * 2 + core).wait_send()

    far_blocks = [lax.rem(chip + i, chips) * 2 + c for i in range(1, chips) for c in (core, 1 - core)]
    near_blocks = [t, mate]

    def far_copy(h):
        return pltpu.make_async_remote_copy(
            src_ref=feats.at[0, t, rows_of(h)], dst_ref=far.at[t, rows_of(h)],
            send_sem=far_send.at[h], recv_sem=far_recv.at[h],
            device_id={"sp": mid}, device_id_type=MESH,
        )

    def back_copy(h):
        ref = back.at[rows_of(h)]
        return pltpu.make_async_remote_copy(
            src_ref=ref, dst_ref=ref,
            send_sem=back_send.at[h], recv_sem=back_recv.at[h],
            device_id={"sp": end}, device_id_type=MESH,
        )

    def stat_copy(l, h, i, block):
        ref = stat_rows.at[l, block, :, rows_of(h)]
        return pltpu.make_async_remote_copy(
            src_ref=ref, dst_ref=ref,
            send_sem=stat_send.at[l, h, i], recv_sem=stat_recv.at[l, h, block],
            device_id={"tp": lax.rem(t + i, tp)}, device_id_type=MESH,
        )

    def halo_copy(l):
        return pltpu.make_async_remote_copy(
            src_ref=tail.at[l], dst_ref=halo.at[l],
            send_sem=halo_send.at[l], recv_sem=halo_recv.at[l],
            device_id={"sp": s + 1}, device_id_type=MESH,
        )

    def halo_goes(l):
        return s < last if l else inner

    def over(h, body):
        first, count = parts[h]

        def step(c, carry):
            body(pl.multiple_of(first + c * CHUNK, CHUNK))
            return carry

        lax.fori_loop(0, count // CHUNK, step, 0)

    def scale(which, l, source, b, h, fresh):
        cut = pl.ds(pl.multiple_of(b * part, 128), part)

        def body(low):
            at = pl.ds(low, CHUNK)
            x = source[b, at, :].astype(F32)
            square = x * x
            total = square[:, 0:128]
            for j in range(1, part // 128):
                total = total + square[:, j * 128 : (j + 1) * 128]
            squares[which, at, :] = total if fresh else squares[which, at, :] + total
            scaled[which, b, at, :] = (x * gain[l : l + 1, cut].astype(F32)).astype(BF16)

        over(h, body)

    def accumulate(which, l, b, h, fresh):
        at = rows_of(h)
        for k, acc in ((SIG, acc_sig), (GATE, acc_gate)):
            w = banks[k][l, b].reshape(part, local)
            more = jnp.dot(scaled[which, b, at, :], w, preferred_element_type=F32)
            acc[which, at, :] = more if fresh else acc[which, at, :] + more

    def blend(which, h):
        def body(low):
            at = pl.ds(low, CHUNK)
            total = jnp.sum(squares[which, at, :], axis=1, keepdims=True)
            r = lax.rsqrt(total / width + EPS)
            v = (acc_sig[which, at, :] * r) * sigmoid(acc_gate[which, at, :] * r)
            v = v.astype(BF16)
            if which:
                back[at, :] = v
            else:
                padded[pl.ds(pl.multiple_of(hp + low, 8), CHUNK), :] = v.astype(F32)

        over(h, body)

    def send_tail(l):
        tail[l] = padded[rows : rows + hp, :].astype(BF16)

        @pl.when(halo_goes(l))
        def _():
            halo_copy(l).start()

    def settle(l):
        @pl.when(s >= middle if l == 0 else s > 0)
        def _():
            halo_copy(l).wait_recv()
            padded[0:hp, :] = halo[l].astype(F32)

        if l == 0:
            @pl.when(inner & (s < middle))
            def _():
                padded[0:hp, :] = back[rows - hp : rows, :].astype(F32)

        @pl.when(s == 0)
        def _():
            padded[0:hp, :] = jnp.zeros((hp, local), F32)

    def convolve(l, h):
        begin, count = parts[h]
        tap_rows = taps[:, l, :].astype(F32)
        first = hp - (kernel_taps - 1)
        lane = lax.broadcasted_iota(jnp.int32, (CHUNK, 128), 1)
        chunks = list(range(begin // CHUNK, (begin + count) // CHUNK))
        if chunks[0] == 0:
            chunks = chunks[1:] + chunks[:1]
        for c in chunks:
            if c == 0:
                settle(l)
            low = c * CHUNK
            total = jnp.broadcast_to(bias[l : l + 1, :].astype(F32), (CHUNK, local))
            for j in range(kernel_taps):
                start = low + first + j
                total = total + tap_rows[j : j + 1, :] * padded[start : start + CHUNK, :]
            filt[low : low + CHUNK, :] = total
            one = jnp.sum(total, axis=1, keepdims=True)
            two = jnp.sum(total * total, axis=1, keepdims=True)
            stat_cols[low : low + CHUNK, :] = jnp.where(
                lane == 0, one, jnp.where(lane == 1, two, 0.0)
            )
        at = slice(begin, begin + count)
        stat_rows[l, t, :, at] = jnp.transpose(stat_cols[at, :])[0:8, :]
        for i in range(1, tp):
            stat_copy(l, h, i, t).start()

    def activate(l, h):
        begin, count = parts[h]
        at = slice(begin, begin + count)
        for i in range(1, tp):
            stat_copy(l, h, i, lax.rem(t + i, tp)).wait_recv()
        sums = stat_rows[l, 0, :, at]
        for b in range(1, tp):
            sums = sums + stat_rows[l, b, :, at]
        stat_cols[at, :] = jnp.transpose(
            jnp.concatenate([sums, jnp.zeros((120, count), F32)], axis=0)
        )
        gains, shifts = ln_gain[l : l + 1, :].astype(F32), ln_shift[l : l + 1, :].astype(F32)

        def body(low):
            at = pl.ds(low, CHUNK)
            average = stat_cols[at, 0:1] / channels
            spread = stat_cols[at, 1:2] / channels - average * average
            v = (filt[at, :] - average) * lax.rsqrt(spread + EPS) * gains + shifts
            acts[l, t, at, :] = (v * sigmoid(v)).astype(BF16)

        over(h, body)
        spread_start(acts.at[l], layers + l, h)

    def update(l, h):
        begin, count = parts[h]
        tile = min(256, part)
        deep = 128

        def body(c, carry):
            at = pl.ds(pl.multiple_of(begin + c * deep, deep), deep)
            for n in range(part // tile):
                cut = slice(n * tile, (n + 1) * tile)
                total = feats[l, t, at, cut].astype(F32)
                for b in range(tp):
                    w = out_all[l, b, :, :, :, cut].reshape(local, tile)
                    total = total + jnp.dot(acts[l, b, at, :], w, preferred_element_type=F32)
                if l + 1 < layers:
                    feats[l + 1, t, at, cut] = total.astype(BF16)
                else:
                    result[at, cut] = total.astype(BF16)
            return carry

        lax.fori_loop(0, count // deep, body, 0)

    far_n = 2 * layers
    both_in = (SIG, GATE)

    @pl.when(outer)
    def _():
        own_stream.wait()
        for k in range(3):
            load(0, k).wait()
        each(0, (SIG,), lift)
        far_copy(0).start()
        each(0, (GATE,), lift)
        far_copy(1).start()
        each(0, both_in, lift_other)
        each(0, (OUT,), lift)
        each(0, (OUT,), lift_other)
        for l in range(1, layers):
            for k in range(3):
                load(l, k).wait()
            each(l, range(3), lift)
        for l in range(1, layers):
            each(l, range(3), lift_other)
        each(0, (OUT,), take(mid, False))
        for l in range(1, layers):
            each(l, range(3), take(mid, False))
        each(0, (OUT,), take(mid2, False))
        for h in both:
            back_copy(h).wait_recv()

            def body(low):
                to = pl.ds(pl.multiple_of(hp + low, 8), CHUNK)
                padded[to, :] = back[pl.ds(low, CHUNK), :].astype(F32)

            over(h, body)

    @pl.when(inner)
    def _():
        load(0, SIG).wait()
        load(0, GATE).wait()
        each(0, both_in, lambda l, k, q: to_middle(l, k, q, s))
        own_stream.wait()
        for h in both:
            spread_start(feats.at[0], 0, h)
        load(0, OUT).wait()
        each(0, (OUT,), onward(s))
        for l in range(1, layers):
            for k in range(3):
                load(l, k).wait()
            each(l, range(3), onward(s))
        for q in range(pieces[SIG]):
            pass_on(0, SIG, q)
            take(mid2, False)(0, SIG, q)
        each(0, (GATE,), take(mid2, False))
        spread_relay(feats.at[0], 0, 0)
        each(0, (SIG,), take(end2, False))
        far_copy(0).wait_recv()
        spread_start(far, far_n, 0)
        spread_relay(feats.at[0], 0, 1)
        each(0, (GATE,), pass_on)
        each(0, (OUT,), lambda l, k, q: to_middle(l, k, q, s))
        each(1, both_in, lambda l, k, q: to_middle(l, k, q, s))
        for h in both:
            spread_near(feats.at[0], 0, h)
            spread_rest(feats.at[0], 0, h)
        for h in both:
            for i, b in enumerate(near_blocks + far_blocks):
                scale(0, 0, feats.at[0], b, h, i == 0)
        each(0, (GATE,), take(end2, False))
        for h in both:
            accumulate(0, 0, s, h, True)
        for k in both_in:
            ready(0, k, mid2)
        for h in both:
            accumulate(0, 0, mid2, h, False)
        far_copy(1).wait_recv()
        spread_start(far, far_n, 1)
        each(0, (OUT,), take(mid2))
        for h in both:
            spread_relay(far, far_n, h)
            spread_near(far, far_n, h)
            spread_rest(far, far_n, h)
            for i, b in enumerate(near_blocks + far_blocks):
                scale(1, 0, far, b, h, i == 0)
            if h == 0:
                for k in both_in:
                    ready(0, k, end2)
                    ready(0, k, end)
            for i, b in enumerate((s, mid2, end2, end)):
                accumulate(1, 0, b, h, i == 0)
            blend(1, h)
            back_copy(h).start()
            if h == 0:
                each(1, (SIG,), take(mid2))
        for h in both:
            for b in (end2, end):
                accumulate(0, 0, b, h, False)
            blend(0, h)
            if h == 0:
                send_tail(0)
        each(0, (OUT,), pass_on)
        each(1, (GATE,), take(mid2, False))

    for h in both:
        convolve(0, h)

    @pl.when(inner)
    def _():
        each(0, (OUT,), take(end2))
        each(1, (GATE,), onward(mid2))

    activate(0, 0)

    @pl.when(inner)
    def _():
        each(1, (SIG,), pass_on)
        each(1, (OUT,), lambda l, k, q: to_middle(l, k, q, s))

    @pl.when(outer)
    def _():
        each(0, (OUT,), take(end2, False))
        each(1, (SIG,), take(mid2, False))

    activate(0, 1)
    for h in both:
        spread_relay(acts.at[0], layers, h)
    ready_all(0, OUT)
    for h in both:
        spread_near(acts.at[0], layers, h)
        spread_rest(acts.at[0], layers, h)
        update(0, h)
        spread_start(feats.at[1], 1, h)

    for l in range(1, layers):
        x = feats.at[l]
        for h in both:
            scale(0, l, x, t, h, True)

        @pl.when(inner)
        def _(l=l):
            each(l, (GATE,), pass_on)
            each(l, both_in, take(end2))
            each(l, (OUT,), pass_on)
            each(l, (OUT,), take(mid2))

        @pl.when(outer)
        def _(l=l):
            each(l, (GATE,), take(mid2, False))
            each(l, both_in, take(end2, False))

        for h in both:
            spread_near(x, l, h)
            scale(0, l, x, mate, h, False)
        for k in both_in:
            ready_all(l, k)
        for h in both:
            for i, b in enumerate(near_blocks):
                accumulate(0, l, b, h, i == 0)
        spread_relay(x, l, 0)

        @pl.when(outer)
        def _(l=l):
            each(l, (OUT,), take(mid2, False))

        for h in both:
            if h:
                spread_relay(x, l, h)
            spread_rest(x, l, h)
            for b in far_blocks:
                scale(0, l, x, b, h, False)
                accumulate(0, l, b, h, False)
            blend(0, h)
            if h == 0:
                send_tail(l)
                each_role = (inner, outer)
                for role, further in zip(each_role, (True, False)):
                    @pl.when(role)
                    def _(l=l, further=further):
                        each(l, (OUT,), take(end2, further))
        for h in both:
            convolve(l, h)
        for h in both:
            activate(l, h)
        for h in both:
            spread_relay(acts.at[l], layers + l, h)
        ready_all(l, OUT)
        for h in both:
            spread_near(acts.at[l], layers + l, h)
            spread_rest(acts.at[l], layers + l, h)
            update(l, h)
            if l + 1 < layers:
                spread_start(feats.at[l + 1], l + 1, h)

    @pl.when(outer)
    def _():
        for h in both:
            far_copy(h).wait_send()
        for l in range(layers):
            each(l, range(3), lambda l, k, q: lift(l, k, q, True))
            each(l, range(3), lambda l, k, q: lift_other(l, k, q, True))
            for shard in (mid, mid2, end2):
                each(l, range(3) if l else (OUT,), lambda l, k, q: across(l, k, q, shard, True))

    @pl.when(inner)
    def _():
        spread_done(feats.at[0], 0)
        spread_done(far, far_n)
        for h in both:
            back_copy(h).wait_send()
        for l in range(layers):
            for shard in (s, end):
                each(l, range(3), lambda l, k, q: to_middle(l, k, q, shard, True))
            for shard in (s, mid2, end2):
                each(l, range(3) if l else (OUT,), lambda l, k, q: to_end(l, k, q, shard, True))
            for shard in (mid2, end2):
                each(l, range(3), lambda l, k, q: across(l, k, q, shard, True))
            for k in range(3):
                for q in range(pieces[k]):
                    if not direct(l, k, q, pieces[k]):
                        across(l, k, q, end, True)

    for l in range(layers):
        if l:
            spread_done(feats.at[l], l)
        spread_done(acts.at[l], layers + l)
        for h in both:
            for i in range(1, tp):
                stat_copy(l, h, i, t).wait_send()

        @pl.when(halo_goes(l))
        def _(l=l):
            halo_copy(l).wait_send()


def shards(counts, stream, norm_gain, w_signal, w_gate, conv_taps, conv_bias, ln_gain, ln_shift, w_out):
    groups, sp, tp = counts
    layers, deep, local = w_signal.shape
    rows, part = stream.shape
    kernel_taps = conv_taps.shape[1]
    hp = -(-(kernel_taps - 1) // 16) * 16
    width, channels = part * tp, local * tp

    def cut(w):
        half = w.shape[1] // groups
        count = PIECES if half % (16 * PIECES) == 0 else 1
        return w.reshape(layers, groups, count, half // count, w.shape[2])

    w_signal, w_gate, w_out = cut(w_signal), cut(w_gate), cut(w_out)
    bank = lambda w: pltpu.VMEM((layers, sp) + w.shape[1:], BF16)
    most = max(w.shape[2] for w in (w_signal, w_gate, w_out))
    line = (layers, 3, most, sp)
    dma = lambda *shape: pltpu.SemaphoreType.DMA(shape)
    anywhere = pl.BlockSpec(memory_space=pl.ANY)
    inside = pl.BlockSpec(memory_space=pltpu.VMEM)
    spreads = (2 * layers + 1, 2, tp)
    folds = groups == 2 and layers == 2 and sp == tp and sp // 2 == 2 and rows % 128 == 0 and rows > 128
    if folds:
        body = fold_kernel
        scratch = [
            bank(w_signal), bank(w_gate), bank(w_out),
            pltpu.VMEM((layers, tp, rows, part), BF16),
            pltpu.VMEM((tp, rows, part), BF16),
            pltpu.VMEM((2, tp, rows, part), BF16),
            pltpu.VMEM((2, rows, 128), F32),
            pltpu.VMEM((2, rows, local), F32),
            pltpu.VMEM((2, rows, local), F32),
            pltpu.VMEM((rows, local), BF16),
            pltpu.VMEM((layers, hp, local), BF16),
            pltpu.VMEM((layers, hp, local), BF16),
            pltpu.VMEM((hp + rows, local), F32),
            pltpu.VMEM((rows, local), F32),
            pltpu.VMEM((rows, 128), F32),
            pltpu.VMEM((layers, tp, 8, rows), F32),
            pltpu.VMEM((layers, tp, rows, local), BF16),
            dma(layers, 3), pltpu.SemaphoreType.DMA,
            dma(*line), dma(*line), dma(*line), dma(*line), dma(*line),
            dma(*spreads), dma(*spreads), dma(*spreads), dma(*spreads),
            dma(2), dma(2), dma(2), dma(2),
            dma(layers), dma(layers), dma(layers, 2, tp), dma(layers, 2, tp),
        ]
    else:
        body = kernel
        scratch = [
            bank(w_signal), bank(w_gate), bank(w_out),
            pltpu.VMEM((layers, tp, rows, part), BF16),
            pltpu.VMEM((tp, rows, part), BF16),
            pltpu.VMEM((rows, 128), F32),
            pltpu.VMEM((rows, local), F32),
            pltpu.VMEM((rows, local), F32),
            pltpu.VMEM((layers, hp, local), BF16),
            pltpu.VMEM((layers, hp, local), BF16),
            pltpu.VMEM((hp + rows, local), F32),
            pltpu.VMEM((rows, local), F32),
            pltpu.VMEM((rows, 128), F32),
            pltpu.VMEM((layers, tp, 8, rows), F32),
            pltpu.VMEM((layers, tp, rows, local), BF16),
            dma(layers, 3), pltpu.SemaphoreType.DMA,
            dma(layers, 3, most), dma(*line), dma(*line), dma(*line), dma(*line),
            dma(2 * layers, tp), dma(2 * layers, tp), dma(2 * layers, tp), dma(2 * layers, tp),
            dma(layers), dma(layers), dma(layers, tp), dma(layers, tp),
        ]
    return pl.pallas_call(
        functools.partial(
            body, (groups, sp, tp, layers, rows, kernel_taps, hp, width, channels)
        ),
        out_shape=jax.ShapeDtypeStruct(stream.shape, BF16),
        in_specs=[anywhere, inside, anywhere, anywhere, inside, inside, inside, inside, anywhere],
        out_specs=inside,
        scratch_shapes=scratch,
        compiler_params=pltpu.CompilerParams(
            collective_id=0, has_side_effects=True, vmem_limit_bytes=60 * 1024 * 1024
        ),
    )(
        stream, norm_gain, w_signal, w_gate, jnp.transpose(conv_taps, (1, 0, 2)), conv_bias,
        ln_gain, ln_shift, w_out,
    )


def solution(mesh):
    counts = tuple(mesh.shape[name] for name in ("grp", "sp", "tp"))
    return jax.shard_map(
        functools.partial(shards, counts),
        mesh=mesh,
        in_specs=(
            P(("grp", "sp"), "tp"),
            P(),
            P(None, "sp", "tp"),
            P(None, "sp", "tp"),
            P(None, None, "tp"),
            P(None, "tp"),
            P(None, "tp"),
            P(None, "tp"),
            P(None, "sp", "tp"),
        ),
        out_specs=P(("grp", "sp"), "tp"),
        check_vma=False,
    )
```

```python
import functools

import jax
import jax.numpy as jnp
from jax import lax
from jax.experimental import pallas as pl
from jax.experimental.pallas import tpu as pltpu
from jax.sharding import PartitionSpec as P

MESH = pl.DeviceIdType.MESH
EPS = 1e-05
F32 = jnp.float32
BF16 = jnp.bfloat16
SIG, GATE, OUT = 0, 1, 2
CHUNK = 32
PIECES = 2
FOLD_PIECES = 4
DEEP = 128
PAIR, FAR_MID, FAR_END, OWN = 0, 1, 2, 3


def sigmoid(v):
    return 1.0 / (1.0 + jnp.exp(-v))


def kernel(
    sizes,
    stream, gain, w_signal, w_gate, taps, bias, ln_gain, ln_shift, w_out,
    result,
    sig_all, gate_all, out_all, feats, scaled_feats, inv, acc_sig, acc_gate,
    tail, halo, padded, filt, stat_cols, stat_rows, acts,
    load_sem, stream_sem, own_send, z_send, z_recv, y_send, y_recv,
    cross_send, cross_recv, core_send, core_recv,
    halo_send, halo_recv, stat_send, stat_recv,
):
    groups, sp, tp, layers, rows, kernel_taps, hp, width, channels = sizes
    g, s, t = lax.axis_index("grp"), lax.axis_index("sp"), lax.axis_index("tp")
    chips = tp // 2
    core, chip = lax.rem(t, 2), lax.div(t, 2)
    mate = t + 1 - 2 * core
    share = sp // tp
    banks = (sig_all, gate_all, out_all)
    held = (w_signal, w_gate, w_out)

    inner = (s > 0) & (s < sp - 1)
    pieces = [w.shape[2] for w in held]

    def load(l, k):
        return pltpu.make_async_copy(held[k].at[l], banks[k].at[l, s], load_sem.at[l, k])

    own_stream = pltpu.make_async_copy(stream, feats.at[0, t], stream_sem)
    own_stream.start()
    for l in range(layers):
        for k in range(3):
            load(l, k).start()

    barrier = pltpu.get_barrier_semaphore()

    def greet(where):
        pl.semaphore_signal(barrier, inc=1, device_id=where, device_id_type=MESH)

    @pl.when(s > 0)
    def _():
        greet({"sp": s - 1})

    @pl.when(s < sp - 1)
    def _():
        greet({"sp": s + 1})

    for i in range(1, groups):
        greet({"grp": lax.rem(g + i, groups)})
    for i in range(1, tp):
        greet({"tp": lax.rem(t + i, tp)})
    pl.semaphore_wait(
        barrier,
        jnp.where(s > 0, 1, 0) + jnp.where(s < sp - 1, 1, 0) + (groups - 1 + tp - 1),
    )

    def z_copy(l, k, q, shard, way, mine=False):
        ref = banks[k].at[l, shard, g, q]
        return pltpu.make_async_remote_copy(
            src_ref=ref, dst_ref=ref,
            send_sem=own_send.at[l, k, q] if mine and way else z_send.at[l, k, q, shard],
            recv_sem=z_recv.at[l, k, q, shard],
            device_id={"sp": s + 1 if way == 0 else s - 1}, device_id_type=MESH,
        )

    def y_copy(l, k, q, shard, half, where):
        ref = banks[k].at[l, shard, half, q]
        return pltpu.make_async_remote_copy(
            src_ref=ref, dst_ref=ref,
            send_sem=y_send.at[l, k, q, shard], recv_sem=y_recv.at[l, k, q, shard],
            device_id=where, device_id_type=MESH,
        )

    def own(l, k, done=False):
        if not done:
            load(l, k).wait()
        for way, there, end in ((0, s < sp - 1, s == 0), (1, s > 0, s == sp - 1)):
            @pl.when(there)
            def _(way=way, end=end):
                for q in range(pieces[k]):
                    copy = z_copy(l, k, q, s, way, True)
                    copy.wait_send() if done else copy.start()

                @pl.when(end)
                def _():
                    for q in range(pieces[k]):
                        where = {"sp": s + 1 if way == 0 else s - 1}
                        copy = y_copy(l, k, q, s, 1 - g, where)
                        copy.wait_send() if done else copy.start()

    def sides(d):
        left, right = s - 1 - d, s + 1 + d
        return (
            (0, left, left >= 0, s < sp - 1, (left > 0) | (d > 0)),
            (1, right, right <= sp - 1, s > 0, (right < sp - 1) | (d > 0)),
        )

    def relay(l, k, d, done=False):
        for way, shard, here, onward, across in sides(d):
            @pl.when(here)
            def _(way=way, shard=shard, onward=onward, across=across):
                for q in range(pieces[k]):
                    if not done:
                        z_copy(l, k, q, shard, way).wait_recv()

                    @pl.when(onward)
                    def _():
                        copy = z_copy(l, k, q, shard, way)
                        copy.wait_send() if done else copy.start()

                    @pl.when(across)
                    def _():
                        copy = y_copy(l, k, q, shard, g, {"grp": 1 - g})
                        copy.wait_send() if done else copy.start()

    def other_half(l, k, d):
        for _, shard, here, _, _ in sides(d):
            @pl.when(here)
            def _(shard=shard):
                for q in range(pieces[k]):
                    y_copy(l, k, q, shard, 1 - g, {"grp": 1 - g}).wait_recv()

    def cross_copy(buf, n, block, i):
        ref = buf.at[block]
        return pltpu.make_async_remote_copy(
            src_ref=ref, dst_ref=ref,
            send_sem=cross_send.at[n, i], recv_sem=cross_recv.at[n, block],
            device_id={"tp": lax.rem(chip + i, chips) * 2 + core}, device_id_type=MESH,
        )

    def core_copy(buf, n, block):
        ref = buf.at[block]
        return pltpu.make_async_remote_copy(
            src_ref=ref, dst_ref=ref,
            send_sem=core_send.at[n, block], recv_sem=core_recv.at[n, block],
            device_id={"tp": mate}, device_id_type=MESH,
        )

    def spread_start(buf, n):
        for i in range(1, chips):
            cross_copy(buf, n, t, i).start()
        core_copy(buf, n, t).start()

    def spread_relay(buf, n):
        for i in range(1, chips):
            block = lax.rem(chip + i, chips) * 2 + core
            cross_copy(buf, n, block, i).wait_recv()
            core_copy(buf, n, block).start()

    def spread_wait(buf, n):
        for j in range(chips):
            core_copy(buf, n, j * 2 + 1 - core).wait_recv()

    def spread_done(buf, n):
        for i in range(1, chips):
            cross_copy(buf, n, t, i).wait_send()
        for j in range(chips):
            core_copy(buf, n, j * 2 + core).wait_send()

    def stat_copy(l, i, block):
        return pltpu.make_async_remote_copy(
            src_ref=stat_rows.at[l, block], dst_ref=stat_rows.at[l, block],
            send_sem=stat_send.at[l, i], recv_sem=stat_recv.at[l, block],
            device_id={"tp": lax.rem(t + i, tp)}, device_id_type=MESH,
        )

    def halo_copy(l):
        return pltpu.make_async_remote_copy(
            src_ref=tail.at[l], dst_ref=halo.at[l],
            send_sem=halo_send.at[l], recv_sem=halo_recv.at[l],
            device_id={"sp": s + 1}, device_id_type=MESH,
        )

    def normalise(l):
        part = width // tp

        def body(c, carry):
            at = pl.ds(pl.multiple_of(c * CHUNK, CHUNK), CHUNK)
            total = jnp.zeros((CHUNK, 1), F32)
            for b in range(tp):
                x = feats[l, b, at, :].astype(F32)
                total = total + jnp.sum(x * x, axis=1, keepdims=True)
                scaled_feats[b, at, :] = (
                    x * gain[l : l + 1, b * part : (b + 1) * part].astype(F32)
                ).astype(BF16)
            inv[at, :] = jnp.broadcast_to(lax.rsqrt(total / width + EPS), (CHUNK, 128))
            return carry

        lax.fori_loop(0, rows // CHUNK, body, 0)

    local = channels // tp

    def project(l):
        for k, acc in ((SIG, acc_sig), (GATE, acc_gate)):
            def body(b, carry, k=k, acc=acc):
                w = banks[k][l, pl.ds(b * share, share)].reshape(width // tp, local)
                acc[...] += jnp.dot(scaled_feats[b], w, preferred_element_type=F32)
                return carry

            acc[...] = jnp.zeros_like(acc)
            for d in range(sp - 1):
                other_half(l, k, d)
            lax.fori_loop(0, tp, body, 0)

        def blend(c, carry):
            at = pl.ds(pl.multiple_of(c * CHUNK, CHUNK), CHUNK)
            r = inv[at, 0:1]
            v = (acc_sig[at, :] * r) * sigmoid(acc_gate[at, :] * r)
            to = pl.ds(pl.multiple_of(hp + c * CHUNK, 8), CHUNK)
            padded[to, :] = v.astype(BF16).astype(F32)
            return carry

        lax.fori_loop(0, rows // CHUNK, blend, 0)
        tail[l] = padded[rows : rows + hp, :].astype(BF16)

        @pl.when(s < sp - 1)
        def _():
            halo_copy(l).start()

    def convolve(l):
        def settle():
            @pl.when(s > 0)
            def _():
                halo_copy(l).wait_recv()
                padded[0:hp, :] = halo[l].astype(F32)

            @pl.when(s == 0)
            def _():
                padded[0:hp, :] = jnp.zeros((hp, local), F32)

        tap_rows = taps[:, l, :].astype(F32)
        first = hp - (kernel_taps - 1)
        lane = lax.broadcasted_iota(jnp.int32, (CHUNK, 128), 1)
        for c in [*range(1, rows // CHUNK), 0]:
            if c == 0:
                settle()
            low = c * CHUNK
            total = jnp.broadcast_to(bias[l : l + 1, :].astype(F32), (CHUNK, local))
            for j in range(kernel_taps):
                start = low + first + j
                total = total + tap_rows[j : j + 1, :] * padded[start : start + CHUNK, :]
            filt[low : low + CHUNK, :] = total
            one = jnp.sum(total, axis=1, keepdims=True)
            two = jnp.sum(total * total, axis=1, keepdims=True)
            stat_cols[low : low + CHUNK, :] = jnp.where(
                lane == 0, one, jnp.where(lane == 1, two, 0.0)
            )
        stat_rows[l, t] = jnp.transpose(stat_cols[...])[0:8, :]
        for i in range(1, tp):
            stat_copy(l, i, t).start()

    def activate(l):
        for i in range(1, tp):
            stat_copy(l, i, lax.rem(t + i, tp)).wait_recv()
        sums = jnp.sum(stat_rows[l], axis=0)
        stat_cols[...] = jnp.transpose(
            jnp.concatenate([sums, jnp.zeros((120, rows), F32)], axis=0)
        )
        gains, shifts = ln_gain[l : l + 1, :].astype(F32), ln_shift[l : l + 1, :].astype(F32)

        def body(c, carry):
            at = pl.ds(pl.multiple_of(c * CHUNK, CHUNK), CHUNK)
            average = stat_cols[at, 0:1] / channels
            spread = stat_cols[at, 1:2] / channels - average * average
            v = (filt[at, :] - average) * lax.rsqrt(spread + EPS) * gains + shifts
            acts[l, t, at, :] = (v * sigmoid(v)).astype(BF16)
            return carry

        lax.fori_loop(0, rows // CHUNK, body, 0)

    def update(l):
        columns = width // tp
        tile = min(256, columns)
        deep = 128

        def body(c, carry):
            at = pl.ds(pl.multiple_of(c * deep, deep), deep)
            for n in range(columns // tile):
                cut = slice(n * tile, (n + 1) * tile)
                total = feats[l, t, at, cut].astype(F32)
                for b in range(tp):
                    w = out_all[l, b * share : (b + 1) * share, :, :, :, cut].reshape(local, tile)
                    total = total + jnp.dot(acts[l, b, at, :], w, preferred_element_type=F32)
                if l + 1 < layers:
                    feats[l + 1, t, at, cut] = total.astype(BF16)
                else:
                    result[at, cut] = total.astype(BF16)
            return carry

        lax.fori_loop(0, rows // deep, body, 0)

    hops = range(sp - 1)
    own(0, SIG)
    own(0, GATE)
    own_stream.wait()
    spread_start(feats.at[0], 0)
    for l in range(layers):
        x_cut = [(d, k) for d in hops for k in (SIG, GATE)]
        middle = len(x_cut) - 3 if l == 0 else len(x_cut) - 2
        for i, (d, k) in enumerate(x_cut):
            if l and i == 0:
                continue
            if i == middle:
                if l:
                    own(l, OUT)
                spread_relay(feats.at[l], 2 * l)
            relay(l, k, d)
        if l == 0:
            own(l, OUT)
        spread_wait(feats.at[l], 2 * l)
        normalise(l)
        project(l)

        @pl.when(inner)
        def _(l=l):
            for d in hops:
                relay(l, OUT, d)

        if l + 1 < layers:
            own(l + 1, SIG)
            own(l + 1, GATE)
        convolve(l)

        @pl.when(jnp.logical_not(inner))
        def _(l=l):
            for d in hops:
                relay(l, OUT, d)

        activate(l)
        spread_start(acts.at[l], 2 * l + 1)
        if l + 1 < layers:
            relay(l + 1, SIG, 0)
        spread_relay(acts.at[l], 2 * l + 1)
        for d in hops:
            other_half(l, OUT, d)
        spread_wait(acts.at[l], 2 * l + 1)
        update(l)
        if l + 1 < layers:
            spread_start(feats.at[l + 1], 2 * l + 2)

    for l in range(layers):
        for k in (SIG, GATE, OUT):
            own(l, k, done=True)
            for d in hops:
                relay(l, k, d, done=True)
        spread_done(feats.at[l], 2 * l)
        spread_done(acts.at[l], 2 * l + 1)
        for i in range(1, tp):
            stat_copy(l, i, t).wait_send()

        @pl.when(s < sp - 1)
        def _(l=l):
            halo_copy(l).wait_send()


def direct(l, k, q, count):
    return l > 0 or k == OUT or q < count // 2 or count == 1


def fold_kernel(
    sizes,
    stream, gain, w_signal, w_gate, taps, bias, ln_gain, ln_shift, w_out,
    result,
    sig_all, gate_all, out_all, feats, far, scaled, squares, acc_sig, acc_gate,
    back, tail, halo, padded, filt, stat_cols, stat_rows, acts,
    final, load_sem, stream_sem, final_sem, z_send, end_send, z_recv, y_send, y_recv,
    cross_send, cross_recv, core_send, core_recv,
    far_send, far_recv, back_send, back_recv,
    halo_send, halo_recv, stat_send, stat_recv,
):
    groups, sp, tp, layers, rows, kernel_taps, hp, width, channels = sizes
    g, s, t = lax.axis_index("grp"), lax.axis_index("sp"), lax.axis_index("tp")
    chips = tp // 2
    core, chip = lax.rem(t, 2), lax.div(t, 2)
    mate = t + 1 - 2 * core
    last, middle = sp - 1, sp // 2
    outer = (s == 0) | (s == last)
    inner = jnp.logical_not(outer)
    pair = s + 1 - 2 * lax.rem(s, 2)
    mid = jnp.where(outer, pair, s)
    end = jnp.where(outer, s, pair)
    mid2, end2 = last - mid, last - end
    banks = (sig_all, gate_all, out_all)
    held = (w_signal, w_gate, w_out)
    pieces = [w.shape[2] for w in held]
    local, part = channels // tp, width // tp
    parts = [(rows - (h + 1) * DEEP, DEEP) for h in range(rows // DEEP)]
    every = range(len(parts))
    other_group = {"grp": 1 - g}

    def load(l, k):
        return pltpu.make_async_copy(held[k].at[l], banks[k].at[l, s], load_sem.at[l, k])

    own_stream = pltpu.make_async_copy(stream, feats.at[0, t], stream_sem)
    own_stream.start()
    for l in range(layers):
        for k in range(3):
            load(l, k).start()

    barrier = pltpu.get_barrier_semaphore()

    def greet(where):
        pl.semaphore_signal(barrier, inc=1, device_id=where, device_id_type=MESH)

    @pl.when(s > 0)
    def _():
        greet({"sp": s - 1})

    @pl.when(s < last)
    def _():
        greet({"sp": s + 1})

    for i in range(1, groups):
        greet({"grp": lax.rem(g + i, groups)})
    for i in range(1, tp):
        greet({"tp": lax.rem(t + i, tp)})
    pl.semaphore_wait(
        barrier,
        jnp.where(s > 0, 1, 0) + jnp.where(s < last, 1, 0) + (groups - 1 + tp - 1),
    )

    where = (pair, mid2, end2, s)

    def z_copy(l, k, q, kind, to, sems, spot):
        ref = banks[k].at[l, where[kind], g, q]
        return pltpu.make_async_remote_copy(
            src_ref=ref, dst_ref=ref,
            send_sem=sems.at[l, k, spot], recv_sem=z_recv.at[l, k, q, spot],
            device_id={"sp": to}, device_id_type=MESH,
        )

    def y_copy(l, k, q, kind, half, to, sems, spot):
        ref = banks[k].at[l, where[kind], half, q]
        return pltpu.make_async_remote_copy(
            src_ref=ref, dst_ref=ref,
            send_sem=sems.at[l, k, spot], recv_sem=y_recv.at[l, k, spot],
            device_id=to, device_id_type=MESH,
        )

    def across(l, k, q, kind):
        y_copy(l, k, q, kind, g, other_group, y_send, kind).start()

    def to_end(l, k, q, kind):
        z_copy(l, k, q, kind, end, end_send, PAIR if kind == OWN else kind).start()

    def to_middle(l, k, q, kind):
        z_copy(l, k, q, kind, mid2, z_send, FAR_MID if kind == OWN else FAR_END).start()

    def lift(l, k, q):
        z_copy(l, k, q, OWN, mid, z_send, PAIR).start()

    def lift_other(l, k, q):
        if direct(l, k, q, pieces[k]):
            y_copy(l, k, q, OWN, 1 - g, {"sp": mid}, end_send, PAIR).start()

    def arrived(l, k, q, kind):
        z_copy(l, k, q, kind, mid, z_send, kind).wait_recv()

    def each(l, kinds, act, low=0, high=4):
        for k in kinds:
            for q in range(pieces[k] * low // 4, pieces[k] * high // 4):
                act(l, k, q)

    def pass_on(l, k, q):
        arrived(l, k, q, PAIR)
        to_middle(l, k, q, PAIR)

    def take(kind, onward=True):
        def act(l, k, q):
            arrived(l, k, q, kind)
            across(l, k, q, kind)
            if onward:
                to_end(l, k, q, kind)
        return act

    def onward(kind):
        return lambda l, k, q: to_end(l, k, q, kind)

    def bypass(kind):
        return lambda l, k, q: across(l, k, q, kind)

    def share_rest(l, k, q):
        if not direct(l, k, q, pieces[k]):
            across(l, k, q, PAIR)

    def got(kind):
        return lambda l, k, q: arrived(l, k, q, kind)

    def own_in(l, k, q):
        to_middle(l, k, q, OWN)

    def ready(l, k, kind):
        ref = banks[k].at[l, where[kind], 1 - g]
        pltpu.make_async_copy(ref, ref, y_recv.at[l, k, kind]).wait()

    def ready_all(l, k):
        for kind in (PAIR, FAR_MID, FAR_END):
            ready(l, k, kind)

    def sent(l, k, sems, spot, low=0):
        ref = banks[k].at[l, s, g, pl.ds(low, pieces[k] - low)]
        pltpu.make_async_copy(ref, ref, sems.at[l, k, spot]).wait()

    def rows_of(h):
        return pl.ds(parts[h][0], parts[h][1])

    def cross_copy(buf, n, h, block, i):
        ref = buf.at[block, rows_of(h)]
        return pltpu.make_async_remote_copy(
            src_ref=ref, dst_ref=ref,
            send_sem=cross_send.at[n, i - 1], recv_sem=cross_recv.at[n, h, i - 1],
            device_id={"tp": lax.rem(chip + i, chips) * 2 + core}, device_id_type=MESH,
        )

    def core_copy(buf, n, h, block, i):
        ref = buf.at[block, rows_of(h)]
        return pltpu.make_async_remote_copy(
            src_ref=ref, dst_ref=ref,
            send_sem=core_send.at[n, i], recv_sem=core_recv.at[n, h, i],
            device_id={"tp": mate}, device_id_type=MESH,
        )

    def chip_at(i):
        return lax.rem(chip + i, chips) * 2

    def spread_start(buf, n, h):
        for i in range(1, chips):
            cross_copy(buf, n, h, t, i).start()
        core_copy(buf, n, h, t, 0).start()

    def spread_relay(buf, n, h):
        for i in range(1, chips):
            block = chip_at(i) + core
            cross_copy(buf, n, h, block, chips - i).wait_recv()
            core_copy(buf, n, h, block, i).start()

    def spread_near(buf, n, h):
        core_copy(buf, n, h, mate, 0).wait_recv()

    def spread_rest(buf, n, h):
        for i in range(1, chips):
            core_copy(buf, n, h, chip_at(i) + 1 - core, i).wait_recv()

    def spread_done(buf, n):
        ref = buf.at[t]
        for i in range(1, chips):
            pltpu.make_async_copy(ref, ref, cross_send.at[n, i - 1]).wait()
        for i in range(chips):
            pltpu.make_async_copy(ref, ref, core_send.at[n, i]).wait()

    far_blocks = [lax.rem(chip + i, chips) * 2 + c for i in range(1, chips) for c in (core, 1 - core)]
    near_blocks = [t, mate]

    def far_copy(h):
        return pltpu.make_async_remote_copy(
            src_ref=feats.at[0, t, rows_of(h)], dst_ref=far.at[t, rows_of(h)],
            send_sem=far_send, recv_sem=far_recv.at[h],
            device_id={"sp": mid}, device_id_type=MESH,
        )

    def back_copy(h):
        ref = back.at[rows_of(h)]
        return pltpu.make_async_remote_copy(
            src_ref=ref, dst_ref=ref,
            send_sem=back_send, recv_sem=back_recv.at[h],
            device_id={"sp": end}, device_id_type=MESH,
        )

    def stat_copy(l, h, i, block):
        ref = stat_rows.at[l, block, :, rows_of(h)]
        return pltpu.make_async_remote_copy(
            src_ref=ref, dst_ref=ref,
            send_sem=stat_send.at[l, i - 1], recv_sem=stat_recv.at[l, h],
            device_id={"tp": lax.rem(t + i, tp)}, device_id_type=MESH,
        )

    def halo_copy(l):
        return pltpu.make_async_remote_copy(
            src_ref=tail.at[l], dst_ref=halo.at[l],
            send_sem=halo_send.at[l], recv_sem=halo_recv.at[l],
            device_id={"sp": s + 1}, device_id_type=MESH,
        )

    def halo_goes(l):
        return s < last if l else inner

    def over(h, body):
        first, count = parts[h]

        def step(c, carry):
            body(pl.multiple_of(first + c * CHUNK, CHUNK))
            return carry

        lax.fori_loop(0, count // CHUNK, step, 0)

    def scale(which, l, source, b, h, fresh):
        cut = pl.ds(pl.multiple_of(b * part, 128), part)

        def body(low):
            at = pl.ds(low, CHUNK)
            x = source[b, at, :].astype(F32)
            square = x * x
            total = square[:, 0:128]
            for j in range(1, part // 128):
                total = total + square[:, j * 128 : (j + 1) * 128]
            squares[which, at, :] = total if fresh else squares[which, at, :] + total
            scaled[which, b, at, :] = (x * gain[l : l + 1, cut].astype(F32)).astype(BF16)

        over(h, body)

    def accumulate(which, l, b, h, fresh):
        at = rows_of(h)
        for k, acc in ((SIG, acc_sig), (GATE, acc_gate)):
            w = banks[k][l, b].reshape(part, local)
            more = jnp.dot(scaled[which, b, at, :], w, preferred_element_type=F32)
            acc[which, at, :] = more if fresh else acc[which, at, :] + more

    def blend(which, h):
        def body(low):
            at = pl.ds(low, CHUNK)
            total = jnp.sum(squares[which, at, :], axis=1, keepdims=True)
            r = lax.rsqrt(total / width + EPS)
            v = (acc_sig[which, at, :] * r) * sigmoid(acc_gate[which, at, :] * r)
            v = v.astype(BF16)
            if which:
                back[at, :] = v
            else:
                padded[pl.ds(pl.multiple_of(hp + low, 8), CHUNK), :] = v.astype(F32)

        over(h, body)

    def send_tail(l):
        tail[l] = padded[rows : rows + hp, :].astype(BF16)

        @pl.when(halo_goes(l))
        def _():
            halo_copy(l).start()

    def settle(l):
        @pl.when(s >= middle if l == 0 else s > 0)
        def _():
            halo_copy(l).wait_recv()
            padded[0:hp, :] = halo[l].astype(F32)

        if l == 0:
            @pl.when(inner & (s < middle))
            def _():
                padded[0:hp, :] = back[rows - hp : rows, :].astype(F32)

        @pl.when(s == 0)
        def _():
            padded[0:hp, :] = jnp.zeros((hp, local), F32)

    def convolve(l, h):
        begin, count = parts[h]
        tap_rows = taps[:, l, :].astype(F32)
        first = hp - (kernel_taps - 1)
        lane = lax.broadcasted_iota(jnp.int32, (CHUNK, 128), 1)
        chunks = list(range(begin // CHUNK, (begin + count) // CHUNK))
        if chunks[0] == 0:
            chunks = chunks[1:] + chunks[:1]
        for c in chunks:
            if c == 0:
                settle(l)
            low = c * CHUNK
            total = jnp.broadcast_to(bias[l : l + 1, :].astype(F32), (CHUNK, local))
            for j in range(kernel_taps):
                start = low + first + j
                total = total + tap_rows[j : j + 1, :] * padded[start : start + CHUNK, :]
            filt[low : low + CHUNK, :] = total
            one = jnp.sum(total, axis=1, keepdims=True)
            two = jnp.sum(total * total, axis=1, keepdims=True)
            stat_cols[low : low + CHUNK, :] = jnp.where(
                lane == 0, one, jnp.where(lane == 1, two, 0.0)
            )
        at = slice(begin, begin + count)
        stat_rows[l, t, :, at] = jnp.transpose(stat_cols[at, :])[0:8, :]
        for i in range(1, tp):
            stat_copy(l, h, i, t).start()

    def activate(l, h):
        begin, count = parts[h]
        at = slice(begin, begin + count)
        ref = stat_rows.at[l, pl.ds(0, tp - 1), :, rows_of(h)]
        pltpu.make_async_copy(ref, ref, stat_recv.at[l, h]).wait()
        sums = stat_rows[l, 0, :, at]
        for b in range(1, tp):
            sums = sums + stat_rows[l, b, :, at]
        stat_cols[at, :] = jnp.transpose(
            jnp.concatenate([sums, jnp.zeros((120, count), F32)], axis=0)
        )
        gains, shifts = ln_gain[l : l + 1, :].astype(F32), ln_shift[l : l + 1, :].astype(F32)

        def body(low):
            at = pl.ds(low, CHUNK)
            average = stat_cols[at, 0:1] / channels
            spread = stat_cols[at, 1:2] / channels - average * average
            v = (filt[at, :] - average) * lax.rsqrt(spread + EPS) * gains + shifts
            acts[l, t, at, :] = (v * sigmoid(v)).astype(BF16)

        over(h, body)
        spread_start(acts.at[l], layers + l, h)

    def write(h):
        return pltpu.make_async_copy(
            final.at[rows_of(h)], result.at[rows_of(h)], final_sem
        )

    def update(l, h):
        begin, count = parts[h]
        tile = min(256, part)

        def body(c, carry):
            at = pl.ds(pl.multiple_of(begin + c * DEEP, DEEP), DEEP)
            for n in range(part // tile):
                cut = slice(n * tile, (n + 1) * tile)
                total = feats[l, t, at, cut].astype(F32)
                for b in range(tp):
                    w = out_all[l, b, :, :, :, cut].reshape(local, tile)
                    total = total + jnp.dot(acts[l, b, at, :], w, preferred_element_type=F32)
                if l + 1 < layers:
                    feats[l + 1, t, at, cut] = total.astype(BF16)
                else:
                    final[at, cut] = total.astype(BF16)
            return carry

        lax.fori_loop(0, count // DEEP, body, 0)
        if l + 1 == layers:
            write(h).start()

    far_n = 2 * layers
    both_in = (SIG, GATE)

    def spread_end(buf, n, h):
        spread_relay(buf, n, h)
        spread_near(buf, n, h)
        spread_rest(buf, n, h)

    def scale_all(which, l, source, h):
        for i, b in enumerate(near_blocks + far_blocks):
            scale(which, l, source, b, h, i == 0)

    def fetch(h):
        back_copy(h).wait_recv()

        def body(low):
            to = pl.ds(pl.multiple_of(hp + low, 8), CHUNK)
            padded[to, :] = back[pl.ds(low, CHUNK), :].astype(F32)

        over(h, body)

    def settle_far(h, blocks):
        for i, b in enumerate(blocks):
            accumulate(1, 0, b, h, i == 0)
        blend(1, h)
        back_copy(h).start()

    @pl.when(outer)
    def _():
        own_stream.wait()
        for k in range(3):
            load(0, k).wait()
        each(0, both_in, lift)
        for h in every:
            far_copy(h).start()
        each(0, both_in, lift_other)
        each(0, (OUT,), lift)
        for k in range(3):
            load(1, k).wait()
        each(1, (SIG,), lift)
        each(0, (OUT,), lift_other)
        each(1, (GATE, OUT), lift)
        each(1, range(3), lift_other)
        each(0, (OUT,), take(PAIR, False))
        each(1, range(3), take(PAIR, False))
        each(0, (OUT,), take(FAR_MID, False))
        each(1, (SIG,), take(FAR_MID, False), 0, 3)
        fetch(0)

    @pl.when(inner)
    def _():
        load(0, SIG).wait()
        load(0, GATE).wait()
        each(0, both_in, own_in)
        own_stream.wait()
        for h in every:
            spread_start(feats.at[0], 0, h)
        load(0, OUT).wait()
        each(0, (OUT,), onward(OWN))
        for k in range(3):
            load(1, k).wait()
        each(1, range(3), onward(OWN))
        for k in both_in:
            for q in range(pieces[k]):
                pass_on(0, k, q)
                take(FAR_MID, False)(0, k, q)
            spread_relay(feats.at[0], 0, k)
        each(0, (OUT,), own_in)
        each(1, both_in, own_in)
        each(0, (SIG,), take(FAR_END, False))
        far_copy(0).wait_recv()
        spread_start(far, far_n, 0)
        for h in every[2:]:
            spread_relay(feats.at[0], 0, h)
        each(0, (GATE,), take(FAR_END, False), 0, 3)
        for h in every[1:-1]:
            far_copy(h).wait_recv()
            spread_start(far, far_n, h)
        each(0, (GATE,), take(FAR_END, False), 3, 4)
        each(0, both_in, share_rest)
        for h in every:
            spread_near(feats.at[0], 0, h)
            spread_rest(feats.at[0], 0, h)
            scale_all(0, 0, feats.at[0], h)
        spread_end(far, far_n, 0)
        scale_all(1, 0, far, 0)
        each(0, (OUT,), got(FAR_MID))
        each(0, (OUT,), onward(FAR_MID))
        far_copy(every[-1]).wait_recv()
        spread_start(far, far_n, every[-1])
        for h in every[1:-1]:
            spread_relay(far, far_n, h)
        each(0, (OUT,), bypass(FAR_MID))
        for k in both_in:
            ready(0, k, FAR_MID)
        for h in every:
            for i, b in enumerate((s, mid2)):
                accumulate(0, 0, b, h, i == 0)
        each(1, (SIG,), take(FAR_MID), 0, 3)
        for h in every[1:-1]:
            spread_near(far, far_n, h)
            spread_rest(far, far_n, h)
            scale_all(1, 0, far, h)
        for k in both_in:
            ready(0, k, FAR_END)
            ready(0, k, PAIR)
        blocks = (s, mid2, end2, end)
        settle_far(0, blocks)
        each(0, (OUT,), pass_on, 0, 2)
        for h in every[1:-1]:
            settle_far(h, blocks)
        each(0, (OUT,), pass_on, 2, 4)
        spread_end(far, far_n, every[-1])
        scale_all(1, 0, far, every[-1])
        settle_far(every[-1], blocks)
        each(1, (SIG,), take(FAR_MID), 3, 4)
        each(1, (GATE,), take(FAR_MID), 0, 2)
        for h in every:
            for b in (end2, end):
                accumulate(0, 0, b, h, False)
            blend(0, h)
            if h == 0:
                send_tail(0)
        each(1, (SIG,), pass_on)
        each(1, (OUT,), own_in)
        each(1, (GATE,), got(FAR_MID), 2, 4)

    for h in every:
        if h + 1 < len(parts):
            @pl.when(outer)
            def _(h=h):
                fetch(h + 1)
        convolve(0, h)

    @pl.when(inner)
    def _():
        each(0, (OUT,), take(FAR_END))
        each(1, (GATE,), bypass(FAR_MID), 2, 4)
        each(1, (GATE,), onward(FAR_MID), 2, 4)

    @pl.when(outer)
    def _():
        each(1, (SIG,), take(FAR_MID, False), 3, 4)
        each(1, (GATE,), take(FAR_MID, False), 0, 2)

    for h in every:
        activate(0, h)
        if h == 0:
            @pl.when(outer)
            def _():
                each(0, (OUT,), take(FAR_END, False))

    @pl.when(inner)
    def _():
        each(1, (SIG,), take(FAR_END))

    for h in every:
        spread_relay(acts.at[0], layers, h)
        if h == 0:
            ready_all(0, OUT)
        spread_near(acts.at[0], layers, h)
        spread_rest(acts.at[0], layers, h)
        update(0, h)
        spread_start(feats.at[1], 1, h)

        @pl.when(inner)
        def _(h=h):
            each(1, (GATE,), pass_on, 2 * h, min(2 * h + 2, 4))

        @pl.when(outer)
        def _(h=h):
            each(1, (GATE,), take(FAR_MID, False), 2 + h, min(3 + h, 4))

    x = feats.at[1]
    for h in every:
        scale(0, 1, x, t, h, True)

    @pl.when(inner)
    def _():
        each(1, (GATE,), take(FAR_END), 0, 2)
        each(1, (OUT,), pass_on)

    @pl.when(outer)
    def _():
        each(1, (SIG,), take(FAR_END, False))

    for h in every:
        spread_near(x, 1, h)
        scale(0, 1, x, mate, h, False)

    @pl.when(inner)
    def _():
        each(1, (GATE,), take(FAR_END), 2, 4)

    @pl.when(outer)
    def _():
        each(1, (GATE,), take(FAR_END, False), 0, 2)

    spread_relay(x, 1, 0)

    @pl.when(inner)
    def _():
        each(1, (OUT,), take(FAR_MID))

    @pl.when(outer)
    def _():
        each(1, (GATE,), take(FAR_END, False), 2, 4)

    for k in both_in:
        ready_all(1, k)
    for h in every:
        for i, b in enumerate(near_blocks):
            accumulate(0, 1, b, h, i == 0)
    spread_relay(x, 1, 1)
    for h in every:
        spread_rest(x, 1, h)
        for b in far_blocks:
            scale(0, 1, x, b, h, False)
            accumulate(0, 1, b, h, False)
        blend(0, h)
        if h == 0:
            send_tail(1)

            @pl.when(inner)
            def _():
                each(1, (OUT,), take(FAR_END))

            @pl.when(outer)
            def _():
                each(1, (OUT,), take(FAR_MID, False))
        else:
            convolve(1, h - 1)
            if h + 1 < len(parts):
                spread_relay(x, 1, h + 1)
    convolve(1, every[-1])
    activate(1, 0)

    @pl.when(outer)
    def _():
        each(1, (OUT,), take(FAR_END, False))

    for h in every[1:]:
        activate(1, h)
    spread_relay(acts.at[1], layers + 1, 0)
    ready_all(1, OUT)
    for h in every:
        if h:
            spread_relay(acts.at[1], layers + 1, h)
        spread_near(acts.at[1], layers + 1, h)
        spread_rest(acts.at[1], layers + 1, h)
        update(1, h)

    @pl.when(outer)
    def _():
        pltpu.make_async_copy(feats.at[0, t], feats.at[0, t], far_send).wait()
        for l in range(layers):
            for k in range(3):
                sent(l, k, z_send, PAIR)
                count = sum(direct(l, k, q, pieces[k]) for q in range(pieces[k]))
                sent(l, k, end_send, PAIR, pieces[k] - count)
                if l or k == OUT:
                    for kind in (PAIR, FAR_MID, FAR_END):
                        sent(l, k, y_send, kind)

    @pl.when(inner)
    def _():
        spread_done(feats.at[0], 0)
        spread_done(far, far_n)
        pltpu.make_async_copy(back, back, back_send).wait()
        for l in range(layers):
            for k in range(3):
                sent(l, k, z_send, FAR_MID)
                sent(l, k, z_send, FAR_END)
                sent(l, k, y_send, FAR_MID)
                sent(l, k, y_send, FAR_END)
                if l or k == OUT:
                    for spot in (PAIR, FAR_MID, FAR_END):
                        sent(l, k, end_send, spot)
                count = sum(direct(l, k, q, pieces[k]) for q in range(pieces[k]))
                if count < pieces[k]:
                    sent(l, k, y_send, PAIR, count)

    for l in range(layers):
        if l:
            spread_done(feats.at[l], l)
        spread_done(acts.at[l], layers + l)
        for i in range(1, tp):
            ref = stat_rows.at[l, t]
            pltpu.make_async_copy(ref, ref, stat_send.at[l, i - 1]).wait()

        @pl.when(halo_goes(l))
        def _(l=l):
            halo_copy(l).wait_send()

    pltpu.make_async_copy(final, final, final_sem).wait()


def shards(counts, stream, norm_gain, w_signal, w_gate, conv_taps, conv_bias, ln_gain, ln_shift, w_out):
    groups, sp, tp = counts
    layers, deep, local = w_signal.shape
    rows, part = stream.shape
    kernel_taps = conv_taps.shape[1]
    hp = -(-(kernel_taps - 1) // 16) * 16
    width, channels = part * tp, local * tp

    folds = (
        groups == 2 and layers == 2 and sp == tp and sp // 2 == 2
        and rows % DEEP == 0 and rows > DEEP
    )
    wanted = FOLD_PIECES if folds else PIECES

    def cut(w):
        half = w.shape[1] // groups
        count = wanted if half % (16 * wanted) == 0 else 1
        return w.reshape(layers, groups, count, half // count, w.shape[2])

    w_signal, w_gate, w_out = cut(w_signal), cut(w_gate), cut(w_out)
    bank = lambda w: pltpu.VMEM((layers, sp) + w.shape[1:], BF16)
    most = max(w.shape[2] for w in (w_signal, w_gate, w_out))
    line = (layers, 3, most, sp)
    dma = lambda *shape: pltpu.SemaphoreType.DMA(shape)
    anywhere = pl.BlockSpec(memory_space=pl.ANY)
    inside = pl.BlockSpec(memory_space=pltpu.VMEM)
    count = max(1, rows // DEEP)
    spreads, chips = 2 * layers + 1, tp // 2
    if folds:
        body = fold_kernel
        scratch = [
            bank(w_signal), bank(w_gate), bank(w_out),
            pltpu.VMEM((layers, tp, rows, part), BF16),
            pltpu.VMEM((tp, rows, part), BF16),
            pltpu.VMEM((2, tp, rows, part), BF16),
            pltpu.VMEM((2, rows, 128), F32),
            pltpu.VMEM((2, rows, local), F32),
            pltpu.VMEM((2, rows, local), F32),
            pltpu.VMEM((rows, local), BF16),
            pltpu.VMEM((layers, hp, local), BF16),
            pltpu.VMEM((layers, hp, local), BF16),
            pltpu.VMEM((hp + rows, local), F32),
            pltpu.VMEM((rows, local), F32),
            pltpu.VMEM((rows, 128), F32),
            pltpu.VMEM((layers, tp, 8, rows), F32),
            pltpu.VMEM((layers, tp, rows, local), BF16),
            pltpu.VMEM((rows, part), BF16),
            dma(layers, 3), pltpu.SemaphoreType.DMA, pltpu.SemaphoreType.DMA,
            dma(layers, 3, 3), dma(layers, 3, 3), dma(layers, 3, most, 3),
            dma(layers, 3, 3), dma(layers, 3, 3),
            dma(spreads, chips - 1), dma(spreads, count, chips - 1),
            dma(spreads, chips), dma(spreads, count, chips),
            pltpu.SemaphoreType.DMA, dma(count), pltpu.SemaphoreType.DMA, dma(count),
            dma(layers), dma(layers), dma(layers, tp - 1), dma(layers, count),
        ]
    else:
        body = kernel
        scratch = [
            bank(w_signal), bank(w_gate), bank(w_out),
            pltpu.VMEM((layers, tp, rows, part), BF16),
            pltpu.VMEM((tp, rows, part), BF16),
            pltpu.VMEM((rows, 128), F32),
            pltpu.VMEM((rows, local), F32),
            pltpu.VMEM((rows, local), F32),
            pltpu.VMEM((layers, hp, local), BF16),
            pltpu.VMEM((layers, hp, local), BF16),
            pltpu.VMEM((hp + rows, local), F32),
            pltpu.VMEM((rows, local), F32),
            pltpu.VMEM((rows, 128), F32),
            pltpu.VMEM((layers, tp, 8, rows), F32),
            pltpu.VMEM((layers, tp, rows, local), BF16),
            dma(layers, 3), pltpu.SemaphoreType.DMA,
            dma(layers, 3, most), dma(*line), dma(*line), dma(*line), dma(*line),
            dma(2 * layers, tp), dma(2 * layers, tp), dma(2 * layers, tp), dma(2 * layers, tp),
            dma(layers), dma(layers), dma(layers, tp), dma(layers, tp),
        ]
    return pl.pallas_call(
        functools.partial(
            body, (groups, sp, tp, layers, rows, kernel_taps, hp, width, channels)
        ),
        out_shape=jax.ShapeDtypeStruct(stream.shape, BF16),
        in_specs=[anywhere, inside, anywhere, anywhere, inside, inside, inside, inside, anywhere],
        out_specs=anywhere if folds else inside,
        scratch_shapes=scratch,
        compiler_params=pltpu.CompilerParams(
            collective_id=0, has_side_effects=True, vmem_limit_bytes=60 * 1024 * 1024
        ),
    )(
        stream, norm_gain, w_signal, w_gate, jnp.transpose(conv_taps, (1, 0, 2)), conv_bias,
        ln_gain, ln_shift, w_out,
    )


def solution(mesh):
    counts = tuple(mesh.shape[name] for name in ("grp", "sp", "tp"))
    return jax.shard_map(
        functools.partial(shards, counts),
        mesh=mesh,
        in_specs=(
            P(("grp", "sp"), "tp"),
            P(),
            P(None, "sp", "tp"),
            P(None, "sp", "tp"),
            P(None, None, "tp"),
            P(None, "tp"),
            P(None, "tp"),
            P(None, "tp"),
            P(None, "sp", "tp"),
        ),
        out_specs=P(("grp", "sp"), "tp"),
        check_vma=False,
    )
```

```python
import functools

import jax
import jax.numpy as jnp
from jax import lax
from jax.experimental import pallas as pl
from jax.experimental.pallas import tpu as pltpu
from jax.sharding import PartitionSpec as P

MESH = pl.DeviceIdType.MESH
EPS = 1e-05
F32 = jnp.float32
BF16 = jnp.bfloat16
SIG, GATE, OUT = 0, 1, 2
CHUNK = 32
PIECES = 2
FOLD_PIECES = 4
DEEP = 128
PAIR, FAR_MID, FAR_END, OWN = 0, 1, 2, 3


def sigmoid(v):
    return 1.0 / (1.0 + jnp.exp(-v))


def kernel(
    sizes,
    stream, gain, w_signal, w_gate, taps, bias, ln_gain, ln_shift, w_out,
    result,
    sig_all, gate_all, out_all, feats, scaled_feats, inv, acc_sig, acc_gate,
    tail, halo, padded, filt, stat_cols, stat_rows, acts,
    load_sem, stream_sem, own_send, z_send, z_recv, y_send, y_recv,
    cross_send, cross_recv, core_send, core_recv,
    halo_send, halo_recv, stat_send, stat_recv,
):
    groups, sp, tp, layers, rows, kernel_taps, hp, width, channels = sizes
    g, s, t = lax.axis_index("grp"), lax.axis_index("sp"), lax.axis_index("tp")
    chips = tp // 2
    core, chip = lax.rem(t, 2), lax.div(t, 2)
    mate = t + 1 - 2 * core
    share = sp // tp
    banks = (sig_all, gate_all, out_all)
    held = (w_signal, w_gate, w_out)

    inner = (s > 0) & (s < sp - 1)
    pieces = [w.shape[2] for w in held]

    def load(l, k):
        return pltpu.make_async_copy(held[k].at[l], banks[k].at[l, s], load_sem.at[l, k])

    own_stream = pltpu.make_async_copy(stream, feats.at[0, t], stream_sem)
    own_stream.start()
    for l in range(layers):
        for k in range(3):
            load(l, k).start()

    barrier = pltpu.get_barrier_semaphore()

    def greet(where):
        pl.semaphore_signal(barrier, inc=1, device_id=where, device_id_type=MESH)

    @pl.when(s > 0)
    def _():
        greet({"sp": s - 1})

    @pl.when(s < sp - 1)
    def _():
        greet({"sp": s + 1})

    for i in range(1, groups):
        greet({"grp": lax.rem(g + i, groups)})
    for i in range(1, tp):
        greet({"tp": lax.rem(t + i, tp)})
    pl.semaphore_wait(
        barrier,
        jnp.where(s > 0, 1, 0) + jnp.where(s < sp - 1, 1, 0) + (groups - 1 + tp - 1),
    )

    def z_copy(l, k, q, shard, way, mine=False):
        ref = banks[k].at[l, shard, g, q]
        return pltpu.make_async_remote_copy(
            src_ref=ref, dst_ref=ref,
            send_sem=own_send.at[l, k, q] if mine and way else z_send.at[l, k, q, shard],
            recv_sem=z_recv.at[l, k, q, shard],
            device_id={"sp": s + 1 if way == 0 else s - 1}, device_id_type=MESH,
        )

    def y_copy(l, k, q, shard, half, where):
        ref = banks[k].at[l, shard, half, q]
        return pltpu.make_async_remote_copy(
            src_ref=ref, dst_ref=ref,
            send_sem=y_send.at[l, k, q, shard], recv_sem=y_recv.at[l, k, q, shard],
            device_id=where, device_id_type=MESH,
        )

    def own(l, k, done=False):
        if not done:
            load(l, k).wait()
        for way, there, end in ((0, s < sp - 1, s == 0), (1, s > 0, s == sp - 1)):
            @pl.when(there)
            def _(way=way, end=end):
                for q in range(pieces[k]):
                    copy = z_copy(l, k, q, s, way, True)
                    copy.wait_send() if done else copy.start()

                @pl.when(end)
                def _():
                    for q in range(pieces[k]):
                        where = {"sp": s + 1 if way == 0 else s - 1}
                        copy = y_copy(l, k, q, s, 1 - g, where)
                        copy.wait_send() if done else copy.start()

    def sides(d):
        left, right = s - 1 - d, s + 1 + d
        return (
            (0, left, left >= 0, s < sp - 1, (left > 0) | (d > 0)),
            (1, right, right <= sp - 1, s > 0, (right < sp - 1) | (d > 0)),
        )

    def relay(l, k, d, done=False):
        for way, shard, here, onward, across in sides(d):
            @pl.when(here)
            def _(way=way, shard=shard, onward=onward, across=across):
                for q in range(pieces[k]):
                    if not done:
                        z_copy(l, k, q, shard, way).wait_recv()

                    @pl.when(onward)
                    def _():
                        copy = z_copy(l, k, q, shard, way)
                        copy.wait_send() if done else copy.start()

                    @pl.when(across)
                    def _():
                        copy = y_copy(l, k, q, shard, g, {"grp": 1 - g})
                        copy.wait_send() if done else copy.start()

    def other_half(l, k, d):
        for _, shard, here, _, _ in sides(d):
            @pl.when(here)
            def _(shard=shard):
                for q in range(pieces[k]):
                    y_copy(l, k, q, shard, 1 - g, {"grp": 1 - g}).wait_recv()

    def cross_copy(buf, n, block, i):
        ref = buf.at[block]
        return pltpu.make_async_remote_copy(
            src_ref=ref, dst_ref=ref,
            send_sem=cross_send.at[n, i], recv_sem=cross_recv.at[n, block],
            device_id={"tp": lax.rem(chip + i, chips) * 2 + core}, device_id_type=MESH,
        )

    def core_copy(buf, n, block):
        ref = buf.at[block]
        return pltpu.make_async_remote_copy(
            src_ref=ref, dst_ref=ref,
            send_sem=core_send.at[n, block], recv_sem=core_recv.at[n, block],
            device_id={"tp": mate}, device_id_type=MESH,
        )

    def spread_start(buf, n):
        for i in range(1, chips):
            cross_copy(buf, n, t, i).start()
        core_copy(buf, n, t).start()

    def spread_relay(buf, n):
        for i in range(1, chips):
            block = lax.rem(chip + i, chips) * 2 + core
            cross_copy(buf, n, block, i).wait_recv()
            core_copy(buf, n, block).start()

    def spread_wait(buf, n):
        for j in range(chips):
            core_copy(buf, n, j * 2 + 1 - core).wait_recv()

    def spread_done(buf, n):
        for i in range(1, chips):
            cross_copy(buf, n, t, i).wait_send()
        for j in range(chips):
            core_copy(buf, n, j * 2 + core).wait_send()

    def stat_copy(l, i, block):
        return pltpu.make_async_remote_copy(
            src_ref=stat_rows.at[l, block], dst_ref=stat_rows.at[l, block],
            send_sem=stat_send.at[l, i], recv_sem=stat_recv.at[l, block],
            device_id={"tp": lax.rem(t + i, tp)}, device_id_type=MESH,
        )

    def halo_copy(l):
        return pltpu.make_async_remote_copy(
            src_ref=tail.at[l], dst_ref=halo.at[l],
            send_sem=halo_send.at[l], recv_sem=halo_recv.at[l],
            device_id={"sp": s + 1}, device_id_type=MESH,
        )

    def normalise(l):
        part = width // tp

        def body(c, carry):
            at = pl.ds(pl.multiple_of(c * CHUNK, CHUNK), CHUNK)
            total = jnp.zeros((CHUNK, 1), F32)
            for b in range(tp):
                x = feats[l, b, at, :].astype(F32)
                total = total + jnp.sum(x * x, axis=1, keepdims=True)
                scaled_feats[b, at, :] = (
                    x * gain[l : l + 1, b * part : (b + 1) * part].astype(F32)
                ).astype(BF16)
            inv[at, :] = jnp.broadcast_to(lax.rsqrt(total / width + EPS), (CHUNK, 128))
            return carry

        lax.fori_loop(0, rows // CHUNK, body, 0)

    local = channels // tp

    def project(l):
        for k, acc in ((SIG, acc_sig), (GATE, acc_gate)):
            def body(b, carry, k=k, acc=acc):
                w = banks[k][l, pl.ds(b * share, share)].reshape(width // tp, local)
                acc[...] += jnp.dot(scaled_feats[b], w, preferred_element_type=F32)
                return carry

            acc[...] = jnp.zeros_like(acc)
            for d in range(sp - 1):
                other_half(l, k, d)
            lax.fori_loop(0, tp, body, 0)

        def blend(c, carry):
            at = pl.ds(pl.multiple_of(c * CHUNK, CHUNK), CHUNK)
            r = inv[at, 0:1]
            v = (acc_sig[at, :] * r) * sigmoid(acc_gate[at, :] * r)
            to = pl.ds(pl.multiple_of(hp + c * CHUNK, 8), CHUNK)
            padded[to, :] = v.astype(BF16).astype(F32)
            return carry

        lax.fori_loop(0, rows // CHUNK, blend, 0)
        tail[l] = padded[rows : rows + hp, :].astype(BF16)

        @pl.when(s < sp - 1)
        def _():
            halo_copy(l).start()

    def convolve(l):
        def settle():
            @pl.when(s > 0)
            def _():
                halo_copy(l).wait_recv()
                padded[0:hp, :] = halo[l].astype(F32)

            @pl.when(s == 0)
            def _():
                padded[0:hp, :] = jnp.zeros((hp, local), F32)

        tap_rows = taps[:, l, :].astype(F32)
        first = hp - (kernel_taps - 1)
        lane = lax.broadcasted_iota(jnp.int32, (CHUNK, 128), 1)
        for c in [*range(1, rows // CHUNK), 0]:
            if c == 0:
                settle()
            low = c * CHUNK
            total = jnp.broadcast_to(bias[l : l + 1, :].astype(F32), (CHUNK, local))
            for j in range(kernel_taps):
                start = low + first + j
                total = total + tap_rows[j : j + 1, :] * padded[start : start + CHUNK, :]
            filt[low : low + CHUNK, :] = total
            one = jnp.sum(total, axis=1, keepdims=True)
            two = jnp.sum(total * total, axis=1, keepdims=True)
            stat_cols[low : low + CHUNK, :] = jnp.where(
                lane == 0, one, jnp.where(lane == 1, two, 0.0)
            )
        stat_rows[l, t] = jnp.transpose(stat_cols[...])[0:8, :]
        for i in range(1, tp):
            stat_copy(l, i, t).start()

    def activate(l):
        for i in range(1, tp):
            stat_copy(l, i, lax.rem(t + i, tp)).wait_recv()
        sums = jnp.sum(stat_rows[l], axis=0)
        stat_cols[...] = jnp.transpose(
            jnp.concatenate([sums, jnp.zeros((120, rows), F32)], axis=0)
        )
        gains, shifts = ln_gain[l : l + 1, :].astype(F32), ln_shift[l : l + 1, :].astype(F32)

        def body(c, carry):
            at = pl.ds(pl.multiple_of(c * CHUNK, CHUNK), CHUNK)
            average = stat_cols[at, 0:1] / channels
            spread = stat_cols[at, 1:2] / channels - average * average
            v = (filt[at, :] - average) * lax.rsqrt(spread + EPS) * gains + shifts
            acts[l, t, at, :] = (v * sigmoid(v)).astype(BF16)
            return carry

        lax.fori_loop(0, rows // CHUNK, body, 0)

    def update(l):
        columns = width // tp
        tile = min(256, columns)
        deep = 128

        def body(c, carry):
            at = pl.ds(pl.multiple_of(c * deep, deep), deep)
            for n in range(columns // tile):
                cut = slice(n * tile, (n + 1) * tile)
                total = feats[l, t, at, cut].astype(F32)
                for b in range(tp):
                    w = out_all[l, b * share : (b + 1) * share, :, :, :, cut].reshape(local, tile)
                    total = total + jnp.dot(acts[l, b, at, :], w, preferred_element_type=F32)
                if l + 1 < layers:
                    feats[l + 1, t, at, cut] = total.astype(BF16)
                else:
                    result[at, cut] = total.astype(BF16)
            return carry

        lax.fori_loop(0, rows // deep, body, 0)

    hops = range(sp - 1)
    own(0, SIG)
    own(0, GATE)
    own_stream.wait()
    spread_start(feats.at[0], 0)
    for l in range(layers):
        x_cut = [(d, k) for d in hops for k in (SIG, GATE)]
        middle = len(x_cut) - 3 if l == 0 else len(x_cut) - 2
        for i, (d, k) in enumerate(x_cut):
            if l and i == 0:
                continue
            if i == middle:
                if l:
                    own(l, OUT)
                spread_relay(feats.at[l], 2 * l)
            relay(l, k, d)
        if l == 0:
            own(l, OUT)
        spread_wait(feats.at[l], 2 * l)
        normalise(l)
        project(l)

        @pl.when(inner)
        def _(l=l):
            for d in hops:
                relay(l, OUT, d)

        if l + 1 < layers:
            own(l + 1, SIG)
            own(l + 1, GATE)
        convolve(l)

        @pl.when(jnp.logical_not(inner))
        def _(l=l):
            for d in hops:
                relay(l, OUT, d)

        activate(l)
        spread_start(acts.at[l], 2 * l + 1)
        if l + 1 < layers:
            relay(l + 1, SIG, 0)
        spread_relay(acts.at[l], 2 * l + 1)
        for d in hops:
            other_half(l, OUT, d)
        spread_wait(acts.at[l], 2 * l + 1)
        update(l)
        if l + 1 < layers:
            spread_start(feats.at[l + 1], 2 * l + 2)

    for l in range(layers):
        for k in (SIG, GATE, OUT):
            own(l, k, done=True)
            for d in hops:
                relay(l, k, d, done=True)
        spread_done(feats.at[l], 2 * l)
        spread_done(acts.at[l], 2 * l + 1)
        for i in range(1, tp):
            stat_copy(l, i, t).wait_send()

        @pl.when(s < sp - 1)
        def _(l=l):
            halo_copy(l).wait_send()


def direct(l, k, q, count):
    return l > 0 or q < count // 2 or count == 1


def fold_kernel(
    sizes,
    stream, gain_in, w_signal, w_gate, taps_in, bias_in, ln_gain_in, ln_shift_in, w_out,
    result, gain, taps, bias, ln_gain, ln_shift,
    sig_all, gate_all, out_all, feats, far, scaled, squares, acc_sig, acc_gate,
    back, tail, halo, padded, filt, stat_cols, stat_rows, acts,
    final, small_sem, load_sem, stream_sem, final_sem, z_send, end_send, z_recv, y_send, y_recv,
    cross_send, cross_recv, core_send, core_recv,
    far_send, far_recv, back_send, back_recv,
    halo_send, halo_recv, stat_send, stat_recv,
):
    groups, sp, tp, layers, rows, kernel_taps, hp, width, channels = sizes
    g, s, t = lax.axis_index("grp"), lax.axis_index("sp"), lax.axis_index("tp")
    chips = tp // 2
    core, chip = lax.rem(t, 2), lax.div(t, 2)
    mate = t + 1 - 2 * core
    last, middle = sp - 1, sp // 2
    outer = (s == 0) | (s == last)
    inner = jnp.logical_not(outer)
    pair = s + 1 - 2 * lax.rem(s, 2)
    mid = jnp.where(outer, pair, s)
    end = jnp.where(outer, s, pair)
    mid2, end2 = last - mid, last - end
    banks = (sig_all, gate_all, out_all)
    held = (w_signal, w_gate, w_out)
    pieces = [w.shape[2] for w in held]
    local, part = channels // tp, width // tp
    parts = [(rows - (h + 1) * DEEP, DEEP) for h in range(rows // DEEP)]
    every = range(len(parts))
    both_in = (SIG, GATE)
    other_group = {"grp": 1 - g}

    def load(l, k):
        return pltpu.make_async_copy(held[k].at[l], banks[k].at[l, s], load_sem.at[l, k])

    own_stream = pltpu.make_async_copy(stream, feats.at[0, t], stream_sem)
    small = [
        pltpu.make_async_copy(ref, to, small_sem.at[i])
        for i, (ref, to) in enumerate((
            (gain_in, gain), (taps_in, taps), (bias_in, bias),
            (ln_gain_in, ln_gain), (ln_shift_in, ln_shift),
        ))
    ]
    barrier = pltpu.get_barrier_semaphore()

    def greet(where):
        pl.semaphore_signal(barrier, inc=1, device_id=where, device_id_type=MESH)

    @pl.when(s > 0)
    def _():
        greet({"sp": s - 1})

    @pl.when(s < last)
    def _():
        greet({"sp": s + 1})

    for i in range(1, groups):
        greet({"grp": lax.rem(g + i, groups)})
    for i in range(1, tp):
        greet({"tp": lax.rem(t + i, tp)})
    for k in both_in:
        load(0, k).start()
    own_stream.start()
    load(0, OUT).start()
    for l in range(1, layers):
        for k in range(3):
            load(l, k).start()
    for copy in small:
        copy.start()
    pl.semaphore_wait(
        barrier,
        jnp.where(s > 0, 1, 0) + jnp.where(s < last, 1, 0) + (groups - 1 + tp - 1),
    )

    where = (pair, mid2, end2, s)

    def z_copy(l, k, q, kind, to, sems, spot):
        ref = banks[k].at[l, where[kind], g, q]
        return pltpu.make_async_remote_copy(
            src_ref=ref, dst_ref=ref,
            send_sem=sems.at[l, k, spot], recv_sem=z_recv.at[l, k, q, spot],
            device_id={"sp": to}, device_id_type=MESH,
        )

    def y_copy(l, k, q, kind, half, to, sems, spot):
        ref = banks[k].at[l, where[kind], half, q]
        return pltpu.make_async_remote_copy(
            src_ref=ref, dst_ref=ref,
            send_sem=sems.at[l, k, spot], recv_sem=y_recv.at[l, k, spot],
            device_id=to, device_id_type=MESH,
        )

    def across(l, k, q, kind):
        y_copy(l, k, q, kind, g, other_group, y_send, kind).start()

    def to_end(l, k, q, kind):
        z_copy(l, k, q, kind, end, end_send, PAIR if kind == OWN else kind).start()

    def to_middle(l, k, q, kind):
        z_copy(l, k, q, kind, mid2, z_send, FAR_MID if kind == OWN else FAR_END).start()

    def lift(l, k, q):
        z_copy(l, k, q, OWN, mid, z_send, PAIR).start()

    def lift_other(l, k, q):
        if direct(l, k, q, pieces[k]):
            y_copy(l, k, q, OWN, 1 - g, {"sp": mid}, end_send, PAIR).start()

    def arrived(l, k, q, kind):
        z_copy(l, k, q, kind, mid, z_send, kind).wait_recv()

    def each(l, kinds, act, low=0, high=4):
        for k in kinds:
            for q in range(pieces[k] * low // 4, pieces[k] * high // 4):
                act(l, k, q)

    def pass_on(l, k, q):
        arrived(l, k, q, PAIR)
        to_middle(l, k, q, PAIR)

    def take(kind, onward=True):
        def act(l, k, q):
            arrived(l, k, q, kind)
            if onward:
                to_end(l, k, q, kind)
            if not (onward and kind == FAR_MID and whole(l, k)):
                across(l, k, q, kind)
        return act

    def onward(kind):
        return lambda l, k, q: to_end(l, k, q, kind)

    def bypass(kind):
        return lambda l, k, q: across(l, k, q, kind)

    def share_rest(l, k, q):
        if not direct(l, k, q, pieces[k]):
            across(l, k, q, PAIR)

    def got(kind):
        return lambda l, k, q: arrived(l, k, q, kind)

    def own_in(l, k, q):
        to_middle(l, k, q, OWN)

    def whole(l, k):
        return l == layers - 1 and k == OUT

    def own_other(l, k, q):
        y_copy(l, k, q, OWN, 1 - g, {"sp": mid2}, y_send, FAR_MID).start()

    def ready(l, k, kind):
        ref = banks[k].at[l, where[kind], 1 - g]
        pltpu.make_async_copy(ref, ref, y_recv.at[l, k, kind]).wait()

    def ready_all(l, k):
        for kind in (PAIR, FAR_MID, FAR_END):
            ready(l, k, kind)

    def sent(l, k, sems, spot, low=0):
        ref = banks[k].at[l, s, g, pl.ds(low, pieces[k] - low)]
        pltpu.make_async_copy(ref, ref, sems.at[l, k, spot]).wait()

    def rows_of(h):
        return pl.ds(parts[h][0], parts[h][1])

    def cross_copy(buf, n, h, block, i):
        ref = buf.at[block, rows_of(h)]
        return pltpu.make_async_remote_copy(
            src_ref=ref, dst_ref=ref,
            send_sem=cross_send.at[n, i - 1], recv_sem=cross_recv.at[n, h, i - 1],
            device_id={"tp": lax.rem(chip + i, chips) * 2 + core}, device_id_type=MESH,
        )

    def core_copy(buf, n, h, block, i):
        ref = buf.at[block, rows_of(h)]
        return pltpu.make_async_remote_copy(
            src_ref=ref, dst_ref=ref,
            send_sem=core_send.at[n, i], recv_sem=core_recv.at[n, h, i],
            device_id={"tp": mate}, device_id_type=MESH,
        )

    def chip_at(i):
        return lax.rem(chip + i, chips) * 2

    def spread_start(buf, n, h):
        for i in range(1, chips):
            cross_copy(buf, n, h, t, i).start()
        core_copy(buf, n, h, t, 0).start()

    def spread_relay(buf, n, h):
        for i in range(1, chips):
            block = chip_at(i) + core
            cross_copy(buf, n, h, block, chips - i).wait_recv()
            core_copy(buf, n, h, block, i).start()

    def spread_near(buf, n, h):
        core_copy(buf, n, h, mate, 0).wait_recv()

    def spread_rest(buf, n, h):
        for i in range(1, chips):
            core_copy(buf, n, h, chip_at(i) + 1 - core, i).wait_recv()

    def spread_done(buf, n):
        ref = buf.at[t]
        for i in range(1, chips):
            pltpu.make_async_copy(ref, ref, cross_send.at[n, i - 1]).wait()
        for i in range(chips):
            pltpu.make_async_copy(ref, ref, core_send.at[n, i]).wait()

    far_blocks = [lax.rem(chip + i, chips) * 2 + c for i in range(1, chips) for c in (core, 1 - core)]
    near_blocks = [t, mate]

    def far_copy(h):
        return pltpu.make_async_remote_copy(
            src_ref=feats.at[0, t, rows_of(h)], dst_ref=far.at[t, rows_of(h)],
            send_sem=far_send, recv_sem=far_recv.at[h],
            device_id={"sp": mid}, device_id_type=MESH,
        )

    def back_copy(h):
        ref = back.at[rows_of(h)]
        return pltpu.make_async_remote_copy(
            src_ref=ref, dst_ref=ref,
            send_sem=back_send, recv_sem=back_recv.at[h],
            device_id={"sp": end}, device_id_type=MESH,
        )

    def stat_copy(l, h, i, block):
        ref = stat_rows.at[l, block, :, rows_of(h)]
        return pltpu.make_async_remote_copy(
            src_ref=ref, dst_ref=ref,
            send_sem=stat_send.at[l, i - 1], recv_sem=stat_recv.at[l, h],
            device_id={"tp": lax.rem(t + i, tp)}, device_id_type=MESH,
        )

    def halo_copy(l):
        return pltpu.make_async_remote_copy(
            src_ref=tail.at[l], dst_ref=halo.at[l],
            send_sem=halo_send.at[l], recv_sem=halo_recv.at[l],
            device_id={"sp": s + 1}, device_id_type=MESH,
        )

    def halo_goes(l):
        return s < last if l else inner

    def over(h, body):
        first, count = parts[h]

        def step(c, carry):
            body(pl.multiple_of(first + c * CHUNK, CHUNK))
            return carry

        lax.fori_loop(0, count // CHUNK, step, 0)

    def scale(which, l, source, b, h, fresh):
        cut = pl.ds(pl.multiple_of(b * part, 128), part)

        def body(low):
            at = pl.ds(low, CHUNK)
            x = source[b, at, :].astype(F32)
            square = x * x
            total = square[:, 0:128]
            for j in range(1, part // 128):
                total = total + square[:, j * 128 : (j + 1) * 128]
            squares[which, at, :] = total if fresh else squares[which, at, :] + total
            scaled[which, b, at, :] = (x * gain[l : l + 1, cut].astype(F32)).astype(BF16)

        over(h, body)

    def accumulate(which, l, b, h, fresh, kinds=(SIG, GATE)):
        at = rows_of(h)
        for k in kinds:
            acc = (acc_sig, acc_gate)[k]
            w = banks[k][l, b].reshape(part, local)
            more = jnp.dot(scaled[which, b, at, :], w, preferred_element_type=F32)
            acc[which, at, :] = more if fresh else acc[which, at, :] + more

    def blend(which, h):
        def body(low):
            at = pl.ds(low, CHUNK)
            total = jnp.sum(squares[which, at, :], axis=1, keepdims=True)
            r = lax.rsqrt(total / width + EPS)
            v = (acc_sig[which, at, :] * r) * sigmoid(acc_gate[which, at, :] * r)
            v = v.astype(BF16)
            if which:
                back[at, :] = v
            else:
                padded[pl.ds(pl.multiple_of(hp + low, 8), CHUNK), :] = v.astype(F32)

        over(h, body)

    def send_tail(l):
        tail[l] = padded[rows : rows + hp, :].astype(BF16)

        @pl.when(halo_goes(l))
        def _():
            halo_copy(l).start()

    def settle(l):
        @pl.when(s >= middle if l == 0 else s > 0)
        def _():
            halo_copy(l).wait_recv()
            padded[0:hp, :] = halo[l].astype(F32)

        if l == 0:
            @pl.when(inner & (s < middle))
            def _():
                padded[0:hp, :] = back[rows - hp : rows, :].astype(F32)

        @pl.when(s == 0)
        def _():
            padded[0:hp, :] = jnp.zeros((hp, local), F32)

    def convolve(l, h, stages=(0, 1)):
        begin, count = parts[h]
        tap_rows = taps[:, l, :].astype(F32)
        first = hp - (kernel_taps - 1)
        lane = lax.broadcasted_iota(jnp.int32, (CHUNK, 128), 1)
        chunks = list(range(begin // CHUNK, (begin + count) // CHUNK))
        chunks = (chunks[1:] if 0 in stages else []) + (chunks[:1] if 1 in stages else [])
        for c in chunks:
            if c == 0:
                settle(l)
            low = c * CHUNK
            total = jnp.broadcast_to(bias[l : l + 1, :].astype(F32), (CHUNK, local))
            for j in range(kernel_taps):
                start = low + first + j
                total = total + tap_rows[j : j + 1, :] * padded[start : start + CHUNK, :]
            filt[low : low + CHUNK, :] = total
            one = jnp.sum(total, axis=1, keepdims=True)
            two = jnp.sum(total * total, axis=1, keepdims=True)
            stat_cols[low : low + CHUNK, :] = jnp.where(
                lane == 0, one, jnp.where(lane == 1, two, 0.0)
            )
        if 1 not in stages:
            return
        at = slice(begin, begin + count)
        stat_rows[l, t, :, at] = jnp.transpose(stat_cols[at, :])[0:8, :]
        for i in range(1, tp):
            stat_copy(l, h, i, t).start()

    def activate(l, h):
        begin, count = parts[h]
        at = slice(begin, begin + count)
        ref = stat_rows.at[l, pl.ds(0, tp - 1), :, rows_of(h)]
        pltpu.make_async_copy(ref, ref, stat_recv.at[l, h]).wait()
        sums = stat_rows[l, 0, :, at]
        for b in range(1, tp):
            sums = sums + stat_rows[l, b, :, at]
        stat_cols[at, :] = jnp.transpose(
            jnp.concatenate([sums, jnp.zeros((120, count), F32)], axis=0)
        )
        gains, shifts = ln_gain[l : l + 1, :].astype(F32), ln_shift[l : l + 1, :].astype(F32)

        def body(low):
            at = pl.ds(low, CHUNK)
            average = stat_cols[at, 0:1] / channels
            spread = stat_cols[at, 1:2] / channels - average * average
            v = (filt[at, :] - average) * lax.rsqrt(spread + EPS) * gains + shifts
            acts[l, t, at, :] = (v * sigmoid(v)).astype(BF16)

        over(h, body)
        spread_start(acts.at[l], layers + l, h)

    def write(h):
        return pltpu.make_async_copy(
            final.at[rows_of(h)], result.at[rows_of(h)], final_sem
        )

    def update(l, h):
        begin, count = parts[h]
        tile = min(256, part)

        def body(c, carry):
            at = pl.ds(pl.multiple_of(begin + c * DEEP, DEEP), DEEP)
            for n in range(part // tile):
                cut = slice(n * tile, (n + 1) * tile)
                total = feats[l, t, at, cut].astype(F32)
                for b in range(tp):
                    w = out_all[l, b, :, :, :, cut].reshape(local, tile)
                    total = total + jnp.dot(acts[l, b, at, :], w, preferred_element_type=F32)
                if l + 1 < layers:
                    feats[l + 1, t, at, cut] = total.astype(BF16)
                else:
                    final[at, cut] = total.astype(BF16)
            return carry

        lax.fori_loop(0, count // DEEP, body, 0)
        if l + 1 == layers:
            write(h).start()

    far_n = 2 * layers

    def spread_end(buf, n, h):
        spread_relay(buf, n, h)
        spread_near(buf, n, h)
        spread_rest(buf, n, h)

    def scale_all(which, l, source, h):
        for i, b in enumerate(near_blocks + far_blocks):
            scale(which, l, source, b, h, i == 0)

    def fetch(h):
        back_copy(h).wait_recv()

        def body(low):
            to = pl.ds(pl.multiple_of(hp + low, 8), CHUNK)
            padded[to, :] = back[pl.ds(low, CHUNK), :].astype(F32)

        over(h, body)

    def settle_far(h, blocks):
        for i, b in enumerate(blocks):
            accumulate(1, 0, b, h, i == 0)
        blend(1, h)
        back_copy(h).start()

    @pl.when(outer)
    def _():
        for k in both_in:
            load(0, k).wait()
            each(0, (k,), lift)
        own_stream.wait()
        load(0, OUT).wait()
        for h in every:
            far_copy(h).start()
        each(0, both_in, lift_other)
        each(0, (OUT,), lift)
        for k in range(3):
            load(1, k).wait()
        each(1, (SIG,), lift)
        each(0, (OUT,), lift_other)
        each(1, (GATE,), lift)
        each(1, (SIG,), lift_other)
        each(1, (OUT,), lift)
        each(1, (GATE, OUT), lift_other)
        each(0, (OUT,), take(PAIR, False))
        each(1, range(3), take(PAIR, False))
        each(0, (OUT,), take(FAR_MID, False))
        each(1, (SIG,), take(FAR_MID, False), 0, 3)
        fetch(0)
        each(1, (SIG,), take(FAR_MID, False), 3, 4)

    @pl.when(inner)
    def _():
        for k in both_in:
            load(0, k).wait()
            each(0, (k,), own_in)
        own_stream.wait()
        for h in every:
            spread_start(feats.at[0], 0, h)
        load(0, OUT).wait()
        each(0, (OUT,), onward(OWN))
        for k in range(3):
            load(1, k).wait()
        each(1, range(3), onward(OWN))
        for k in both_in:
            for q in range(pieces[k]):
                pass_on(0, k, q)
                take(FAR_MID, False)(0, k, q)
            spread_relay(feats.at[0], 0, k)
        each(0, (OUT,), own_in)
        each(1, (SIG,), own_in)
        each(0, (SIG,), take(FAR_END, False))
        far_copy(0).wait_recv()
        spread_start(far, far_n, 0)
        for h in every[2:]:
            spread_relay(feats.at[0], 0, h)
        each(0, (GATE,), take(FAR_END, False), 0, 3)
        for h in every[1:-1]:
            far_copy(h).wait_recv()
            spread_start(far, far_n, h)
        each(0, (GATE,), take(FAR_END, False), 3, 4)
        each(0, both_in, share_rest)
        small[0].wait()
        for h in every:
            spread_near(feats.at[0], 0, h)
            spread_rest(feats.at[0], 0, h)
            scale_all(0, 0, feats.at[0], h)
            each(0, (OUT,), take(FAR_MID), h, h + 1)
        spread_end(far, far_n, 0)
        each(0, (OUT,), take(FAR_MID), len(parts), 4)
        scale_all(1, 0, far, 0)
        for k in both_in:
            ready(0, k, FAR_MID)
        for h in every[:1]:
            for i, b in enumerate((s, mid2)):
                accumulate(0, 0, b, h, i == 0)
        far_copy(every[-1]).wait_recv()
        spread_start(far, far_n, every[-1])
        for h in every[1:]:
            for i, b in enumerate((s, mid2)):
                accumulate(0, 0, b, h, i == 0)
        each(1, (SIG,), take(FAR_MID), 0, 1)
        for h in every[1:-1]:
            spread_relay(far, far_n, h)
        each(1, (SIG,), take(FAR_MID), 1, 3)
        for h in every[1:-1]:
            spread_near(far, far_n, h)
            spread_rest(far, far_n, h)
            scale_all(1, 0, far, h)
        for k in both_in:
            ready(0, k, FAR_END)
            ready(0, k, PAIR)
        blocks = (s, mid2, end2, end)
        settle_far(0, blocks)
        each(1, (SIG,), take(FAR_MID), 3, 4)
        each(0, (OUT,), pass_on, 0, 1)
        for h in every[1:-1]:
            settle_far(h, blocks)
        each(0, (OUT,), pass_on, 1, 3)
        spread_end(far, far_n, every[-1])
        scale_all(1, 0, far, every[-1])
        each(0, (OUT,), pass_on, 3, 4)
        each(1, (GATE,), own_in)
        settle_far(every[-1], blocks)
        each(0, (OUT,), share_rest)
        each(0, (OUT,), take(FAR_END), 0, 1)
        for h in every:
            for b in (end2, end):
                accumulate(0, 0, b, h, False)
            blend(0, h)
            if h == 0:
                send_tail(0)
            each(0, (OUT,), take(FAR_END), h + 1, h + 2)
        each(1, (SIG,), pass_on, 0, 2)

    @pl.when(outer)
    def _():
        small[0].wait()

    for copy in small[1:]:
        copy.wait()
    convolve(0, 0, (0,))
    for h in every:
        if h + 1 < len(parts):
            @pl.when(outer)
            def _(h=h):
                fetch(h + 1)

        convolve(0, h, (1,))
        if h + 1 < len(parts):
            convolve(0, h + 1, (0,))

        @pl.when(outer)
        def _(h=h):
            if h:
                each(0, (OUT,), take(FAR_END, False), h - 1, h)

        if h == 0:
            @pl.when(inner)
            def _():
                each(1, (SIG,), pass_on, 2, 3)

    @pl.when(inner)
    def _():
        each(1, (SIG,), pass_on, 3, 4)
        each(1, (GATE,), take(FAR_MID), 0, 2)

    for h in every:
        activate(0, h)
        if h == 0:
            @pl.when(outer)
            def _():
                each(0, (OUT,), take(FAR_END, False), 2, 4)

            @pl.when(inner)
            def _():
                each(1, (GATE,), take(FAR_MID), 2, 4)

    @pl.when(inner)
    def _():
        each(1, (SIG,), take(FAR_END), 0, 3)

    @pl.when(outer)
    def _():
        each(1, (GATE,), take(FAR_MID, False), 0, 2)

    for h in every:
        spread_relay(acts.at[0], layers, h)
        if h == 0:
            @pl.when(outer)
            def _():
                each(1, (GATE,), take(FAR_MID, False), 2, 3)

            ready_all(0, OUT)
        spread_near(acts.at[0], layers, h)
        spread_rest(acts.at[0], layers, h)
        update(0, h)
        spread_start(feats.at[1], 1, h)

        @pl.when(inner)
        def _(h=h):
            if h == 0:
                each(1, (SIG,), take(FAR_END), 3, 4)
            each(1, (GATE,), pass_on, 2 * h, min(2 * h + 2, 4))

        @pl.when(outer)
        def _(h=h):
            if h == 0:
                each(1, (GATE,), take(FAR_MID, False), 3, 4)
            else:
                each(1, (SIG,), take(FAR_END, False), h - 1, h)

    x = feats.at[1]
    for h in every:
        scale(0, 1, x, t, h, True)

    @pl.when(inner)
    def _():
        each(1, (OUT,), own_in)
        each(1, (GATE,), take(FAR_END), 0, 2)

    @pl.when(outer)
    def _():
        each(1, (SIG,), take(FAR_END, False), len(parts) - 1, 4)

    for h in every:
        spread_near(x, 1, h)
        scale(0, 1, x, mate, h, False)

    @pl.when(inner)
    def _():
        each(1, (GATE,), take(FAR_END), 2, 4)

    @pl.when(outer)
    def _():
        each(1, (GATE,), take(FAR_END, False), 0, 2)

    spread_relay(x, 1, 0)

    @pl.when(outer)
    def _():
        each(1, (GATE,), take(FAR_END, False), 2, 4)

    @pl.when(inner)
    def _():
        for q in range(pieces[OUT]):
            take(FAR_MID)(1, OUT, q)
            pass_on(1, OUT, q)
        each(1, (OUT,), own_other)

    home = lax.div(s, 2) == chip
    first_near, first_far = jnp.where(home, s, mid2), jnp.where(home, mid2, s)
    ready_all(1, SIG)
    ready(1, GATE, FAR_MID)
    for h in every:
        for i, b in enumerate(near_blocks):
            accumulate(0, 1, b, h, i == 0, (SIG,))
        accumulate(0, 1, first_near, h, True, (GATE,))

    def fold_far(h):
        spread_rest(x, 1, h)
        for b in far_blocks:
            scale(0, 1, x, b, h, False)
            accumulate(0, 1, b, h, False, (SIG,))
        accumulate(0, 1, first_far, h, False, (GATE,))

    fold_far(0)
    ready(1, GATE, PAIR)
    ready(1, GATE, FAR_END)
    spread_relay(x, 1, 1)

    @pl.when(outer)
    def _():
        each(1, (OUT,), take(FAR_MID, False), 0, 2)

    for h in every:
        if h:
            fold_far(h)
        for b in (pair, end2):
            accumulate(0, 1, b, h, False, (GATE,))
        blend(0, h)
        if h == 0:
            send_tail(1)

            @pl.when(outer)
            def _():
                each(1, (OUT,), take(FAR_MID, False), 2, 4)

            @pl.when(inner)
            def _():
                each(1, (OUT,), take(FAR_END), 0, 2)

            convolve(1, 0, (0,))
        else:
            for late in every[h + 1 : h + 2]:
                spread_relay(x, 1, late)
            convolve(1, h - 1, (1,))
            if h + 1 < len(parts):
                convolve(1, h, (0,))
            if h == 1:
                @pl.when(inner)
                def _():
                    each(1, (OUT,), take(FAR_END), 2, 4)

                @pl.when(outer)
                def _():
                    each(1, (OUT,), take(FAR_END, False), 0, 2)
    convolve(1, every[-1])
    activate(1, 0)

    @pl.when(outer)
    def _():
        each(1, (OUT,), take(FAR_END, False), 2, 4)

    for h in every[1:]:
        activate(1, h)
    spread_relay(acts.at[1], layers + 1, 0)
    ready_all(1, OUT)
    for h in every:
        if h:
            spread_relay(acts.at[1], layers + 1, h)
        spread_near(acts.at[1], layers + 1, h)
        spread_rest(acts.at[1], layers + 1, h)
        update(1, h)

    @pl.when(outer)
    def _():
        pltpu.make_async_copy(feats.at[0, t], feats.at[0, t], far_send).wait()
        for l in range(layers):
            for k in range(3):
                sent(l, k, z_send, PAIR)
                count = sum(direct(l, k, q, pieces[k]) for q in range(pieces[k]))
                sent(l, k, end_send, PAIR, pieces[k] - count)
                if l or k == OUT:
                    for kind in (PAIR, FAR_MID, FAR_END):
                        sent(l, k, y_send, kind)

    @pl.when(inner)
    def _():
        spread_done(feats.at[0], 0)
        spread_done(far, far_n)
        pltpu.make_async_copy(back, back, back_send).wait()
        for l in range(layers):
            for k in range(3):
                sent(l, k, z_send, FAR_MID)
                sent(l, k, z_send, FAR_END)
                sent(l, k, y_send, FAR_MID)
                sent(l, k, y_send, FAR_END)
                if l or k == OUT:
                    for spot in (PAIR, FAR_MID, FAR_END):
                        sent(l, k, end_send, spot)
                count = sum(direct(l, k, q, pieces[k]) for q in range(pieces[k]))
                if count < pieces[k]:
                    sent(l, k, y_send, PAIR, count)

    for l in range(layers):
        if l:
            spread_done(feats.at[l], l)
        spread_done(acts.at[l], layers + l)
        for i in range(1, tp):
            ref = stat_rows.at[l, t]
            pltpu.make_async_copy(ref, ref, stat_send.at[l, i - 1]).wait()

        @pl.when(halo_goes(l))
        def _(l=l):
            halo_copy(l).wait_send()

    pltpu.make_async_copy(final, final, final_sem).wait()


def shards(counts, stream, norm_gain, w_signal, w_gate, conv_taps, conv_bias, ln_gain, ln_shift, w_out):
    groups, sp, tp = counts
    layers, deep, local = w_signal.shape
    rows, part = stream.shape
    kernel_taps = conv_taps.shape[1]
    hp = -(-(kernel_taps - 1) // 16) * 16
    width, channels = part * tp, local * tp

    folds = (
        groups == 2 and layers == 2 and sp == tp and sp // 2 == 2
        and rows % DEEP == 0 and rows > DEEP
    )
    wanted = FOLD_PIECES if folds else PIECES

    def cut(w):
        half = w.shape[1] // groups
        count = wanted if half % (16 * wanted) == 0 else 1
        return w.reshape(layers, groups, count, half // count, w.shape[2])

    w_signal, w_gate, w_out = cut(w_signal), cut(w_gate), cut(w_out)
    bank = lambda w: pltpu.VMEM((layers, sp) + w.shape[1:], BF16)
    most = max(w.shape[2] for w in (w_signal, w_gate, w_out))
    line = (layers, 3, most, sp)
    dma = lambda *shape: pltpu.SemaphoreType.DMA(shape)
    anywhere = pl.BlockSpec(memory_space=pl.ANY)
    inside = pl.BlockSpec(memory_space=pltpu.VMEM)
    count = max(1, rows // DEEP)
    spreads, chips = 2 * layers + 1, tp // 2
    if folds:
        body = fold_kernel
        scratch = [
            pltpu.VMEM(norm_gain.shape, BF16),
            pltpu.VMEM((kernel_taps, layers, local), BF16),
            pltpu.VMEM(conv_bias.shape, BF16),
            pltpu.VMEM(ln_gain.shape, BF16),
            pltpu.VMEM(ln_shift.shape, BF16),
            bank(w_signal), bank(w_gate), bank(w_out),
            pltpu.VMEM((layers, tp, rows, part), BF16),
            pltpu.VMEM((tp, rows, part), BF16),
            pltpu.VMEM((2, tp, rows, part), BF16),
            pltpu.VMEM((2, rows, 128), F32),
            pltpu.VMEM((2, rows, local), F32),
            pltpu.VMEM((2, rows, local), F32),
            pltpu.VMEM((rows, local), BF16),
            pltpu.VMEM((layers, hp, local), BF16),
            pltpu.VMEM((layers, hp, local), BF16),
            pltpu.VMEM((hp + rows, local), F32),
            pltpu.VMEM((rows, local), F32),
            pltpu.VMEM((rows, 128), F32),
            pltpu.VMEM((layers, tp, 8, rows), F32),
            pltpu.VMEM((layers, tp, rows, local), BF16),
            pltpu.VMEM((rows, part), BF16),
            dma(5), dma(layers, 3), pltpu.SemaphoreType.DMA, pltpu.SemaphoreType.DMA,
            dma(layers, 3, 3), dma(layers, 3, 3), dma(layers, 3, most, 3),
            dma(layers, 3, 3), dma(layers, 3, 3),
            dma(spreads, chips - 1), dma(spreads, count, chips - 1),
            dma(spreads, chips), dma(spreads, count, chips),
            pltpu.SemaphoreType.DMA, dma(count), pltpu.SemaphoreType.DMA, dma(count),
            dma(layers), dma(layers), dma(layers, tp - 1), dma(layers, count),
        ]
    else:
        body = kernel
        scratch = [
            bank(w_signal), bank(w_gate), bank(w_out),
            pltpu.VMEM((layers, tp, rows, part), BF16),
            pltpu.VMEM((tp, rows, part), BF16),
            pltpu.VMEM((rows, 128), F32),
            pltpu.VMEM((rows, local), F32),
            pltpu.VMEM((rows, local), F32),
            pltpu.VMEM((layers, hp, local), BF16),
            pltpu.VMEM((layers, hp, local), BF16),
            pltpu.VMEM((hp + rows, local), F32),
            pltpu.VMEM((rows, local), F32),
            pltpu.VMEM((rows, 128), F32),
            pltpu.VMEM((layers, tp, 8, rows), F32),
            pltpu.VMEM((layers, tp, rows, local), BF16),
            dma(layers, 3), pltpu.SemaphoreType.DMA,
            dma(layers, 3, most), dma(*line), dma(*line), dma(*line), dma(*line),
            dma(2 * layers, tp), dma(2 * layers, tp), dma(2 * layers, tp), dma(2 * layers, tp),
            dma(layers), dma(layers), dma(layers, tp), dma(layers, tp),
        ]
    return pl.pallas_call(
        functools.partial(
            body, (groups, sp, tp, layers, rows, kernel_taps, hp, width, channels)
        ),
        out_shape=jax.ShapeDtypeStruct(stream.shape, BF16),
        in_specs=[anywhere] * 9 if folds else [
            anywhere, inside, anywhere, anywhere, inside, inside, inside, inside, anywhere,
        ],
        out_specs=anywhere if folds else inside,
        scratch_shapes=scratch,
        compiler_params=pltpu.CompilerParams(
            collective_id=0, has_side_effects=True, vmem_limit_bytes=60 * 1024 * 1024
        ),
    )(
        stream, norm_gain, w_signal, w_gate, jnp.transpose(conv_taps, (1, 0, 2)), conv_bias,
        ln_gain, ln_shift, w_out,
    )


def solution(mesh):
    counts = tuple(mesh.shape[name] for name in ("grp", "sp", "tp"))
    return jax.shard_map(
        functools.partial(shards, counts),
        mesh=mesh,
        in_specs=(
            P(("grp", "sp"), "tp"),
            P(),
            P(None, "sp", "tp"),
            P(None, "sp", "tp"),
            P(None, None, "tp"),
            P(None, "tp"),
            P(None, "tp"),
            P(None, "tp"),
            P(None, "sp", "tp"),
        ),
        out_specs=P(("grp", "sp"), "tp"),
        check_vma=False,
    )
```

```python
import functools

import jax
import jax.numpy as jnp
from jax import lax
from jax.experimental import pallas as pl
from jax.experimental.pallas import tpu as pltpu
from jax.sharding import PartitionSpec as P

MESH = pl.DeviceIdType.MESH
EPS = 1e-05
F32 = jnp.float32
BF16 = jnp.bfloat16
SIG, GATE, OUT = 0, 1, 2
CHUNK = 32
PIECES = 2
FOLD_PIECES = 4
DEEP = 128
PAIR, FAR_MID, FAR_END, OWN = 0, 1, 2, 3


def sigmoid(v):
    return 1.0 / (1.0 + jnp.exp(-v))


def kernel(
    sizes,
    stream, gain, w_signal, w_gate, taps, bias, ln_gain, ln_shift, w_out,
    result,
    sig_all, gate_all, out_all, feats, scaled_feats, inv, acc_sig, acc_gate,
    tail, halo, padded, filt, stat_cols, stat_rows, acts,
    load_sem, stream_sem, own_send, z_send, z_recv, y_send, y_recv,
    cross_send, cross_recv, core_send, core_recv,
    halo_send, halo_recv, stat_send, stat_recv,
):
    groups, sp, tp, layers, rows, kernel_taps, hp, width, channels = sizes
    g, s, t = lax.axis_index("grp"), lax.axis_index("sp"), lax.axis_index("tp")
    chips = tp // 2
    core, chip = lax.rem(t, 2), lax.div(t, 2)
    mate = t + 1 - 2 * core
    share = sp // tp
    banks = (sig_all, gate_all, out_all)
    held = (w_signal, w_gate, w_out)

    inner = (s > 0) & (s < sp - 1)
    pieces = [w.shape[2] for w in held]

    def load(l, k):
        return pltpu.make_async_copy(held[k].at[l], banks[k].at[l, s], load_sem.at[l, k])

    own_stream = pltpu.make_async_copy(stream, feats.at[0, t], stream_sem)
    own_stream.start()
    for l in range(layers):
        for k in range(3):
            load(l, k).start()

    barrier = pltpu.get_barrier_semaphore()

    def greet(where):
        pl.semaphore_signal(barrier, inc=1, device_id=where, device_id_type=MESH)

    @pl.when(s > 0)
    def _():
        greet({"sp": s - 1})

    @pl.when(s < sp - 1)
    def _():
        greet({"sp": s + 1})

    for i in range(1, groups):
        greet({"grp": lax.rem(g + i, groups)})
    for i in range(1, tp):
        greet({"tp": lax.rem(t + i, tp)})
    pl.semaphore_wait(
        barrier,
        jnp.where(s > 0, 1, 0) + jnp.where(s < sp - 1, 1, 0) + (groups - 1 + tp - 1),
    )

    def z_copy(l, k, q, shard, way, mine=False):
        ref = banks[k].at[l, shard, g, q]
        return pltpu.make_async_remote_copy(
            src_ref=ref, dst_ref=ref,
            send_sem=own_send.at[l, k, q] if mine and way else z_send.at[l, k, q, shard],
            recv_sem=z_recv.at[l, k, q, shard],
            device_id={"sp": s + 1 if way == 0 else s - 1}, device_id_type=MESH,
        )

    def y_copy(l, k, q, shard, half, where):
        ref = banks[k].at[l, shard, half, q]
        return pltpu.make_async_remote_copy(
            src_ref=ref, dst_ref=ref,
            send_sem=y_send.at[l, k, q, shard], recv_sem=y_recv.at[l, k, q, shard],
            device_id=where, device_id_type=MESH,
        )

    def own(l, k, done=False):
        if not done:
            load(l, k).wait()
        for way, there, end in ((0, s < sp - 1, s == 0), (1, s > 0, s == sp - 1)):
            @pl.when(there)
            def _(way=way, end=end):
                for q in range(pieces[k]):
                    copy = z_copy(l, k, q, s, way, True)
                    copy.wait_send() if done else copy.start()

                @pl.when(end)
                def _():
                    for q in range(pieces[k]):
                        where = {"sp": s + 1 if way == 0 else s - 1}
                        copy = y_copy(l, k, q, s, 1 - g, where)
                        copy.wait_send() if done else copy.start()

    def sides(d):
        left, right = s - 1 - d, s + 1 + d
        return (
            (0, left, left >= 0, s < sp - 1, (left > 0) | (d > 0)),
            (1, right, right <= sp - 1, s > 0, (right < sp - 1) | (d > 0)),
        )

    def relay(l, k, d, done=False):
        for way, shard, here, onward, across in sides(d):
            @pl.when(here)
            def _(way=way, shard=shard, onward=onward, across=across):
                for q in range(pieces[k]):
                    if not done:
                        z_copy(l, k, q, shard, way).wait_recv()

                    @pl.when(onward)
                    def _():
                        copy = z_copy(l, k, q, shard, way)
                        copy.wait_send() if done else copy.start()

                    @pl.when(across)
                    def _():
                        copy = y_copy(l, k, q, shard, g, {"grp": 1 - g})
                        copy.wait_send() if done else copy.start()

    def other_half(l, k, d):
        for _, shard, here, _, _ in sides(d):
            @pl.when(here)
            def _(shard=shard):
                for q in range(pieces[k]):
                    y_copy(l, k, q, shard, 1 - g, {"grp": 1 - g}).wait_recv()

    def cross_copy(buf, n, block, i):
        ref = buf.at[block]
        return pltpu.make_async_remote_copy(
            src_ref=ref, dst_ref=ref,
            send_sem=cross_send.at[n, i], recv_sem=cross_recv.at[n, block],
            device_id={"tp": lax.rem(chip + i, chips) * 2 + core}, device_id_type=MESH,
        )

    def core_copy(buf, n, block):
        ref = buf.at[block]
        return pltpu.make_async_remote_copy(
            src_ref=ref, dst_ref=ref,
            send_sem=core_send.at[n, block], recv_sem=core_recv.at[n, block],
            device_id={"tp": mate}, device_id_type=MESH,
        )

    def spread_start(buf, n):
        for i in range(1, chips):
            cross_copy(buf, n, t, i).start()
        core_copy(buf, n, t).start()

    def spread_relay(buf, n):
        for i in range(1, chips):
            block = lax.rem(chip + i, chips) * 2 + core
            cross_copy(buf, n, block, i).wait_recv()
            core_copy(buf, n, block).start()

    def spread_wait(buf, n):
        for j in range(chips):
            core_copy(buf, n, j * 2 + 1 - core).wait_recv()

    def spread_done(buf, n):
        for i in range(1, chips):
            cross_copy(buf, n, t, i).wait_send()
        for j in range(chips):
            core_copy(buf, n, j * 2 + core).wait_send()

    def stat_copy(l, i, block):
        return pltpu.make_async_remote_copy(
            src_ref=stat_rows.at[l, block], dst_ref=stat_rows.at[l, block],
            send_sem=stat_send.at[l, i], recv_sem=stat_recv.at[l, block],
            device_id={"tp": lax.rem(t + i, tp)}, device_id_type=MESH,
        )

    def halo_copy(l):
        return pltpu.make_async_remote_copy(
            src_ref=tail.at[l], dst_ref=halo.at[l],
            send_sem=halo_send.at[l], recv_sem=halo_recv.at[l],
            device_id={"sp": s + 1}, device_id_type=MESH,
        )

    def normalise(l):
        part = width // tp

        def body(c, carry):
            at = pl.ds(pl.multiple_of(c * CHUNK, CHUNK), CHUNK)
            total = jnp.zeros((CHUNK, 1), F32)
            for b in range(tp):
                x = feats[l, b, at, :].astype(F32)
                total = total + jnp.sum(x * x, axis=1, keepdims=True)
                scaled_feats[b, at, :] = (
                    x * gain[l : l + 1, b * part : (b + 1) * part].astype(F32)
                ).astype(BF16)
            inv[at, :] = jnp.broadcast_to(lax.rsqrt(total / width + EPS), (CHUNK, 128))
            return carry

        lax.fori_loop(0, rows // CHUNK, body, 0)

    local = channels // tp

    def project(l):
        for k, acc in ((SIG, acc_sig), (GATE, acc_gate)):
            def body(b, carry, k=k, acc=acc):
                w = banks[k][l, pl.ds(b * share, share)].reshape(width // tp, local)
                acc[...] += jnp.dot(scaled_feats[b], w, preferred_element_type=F32)
                return carry

            acc[...] = jnp.zeros_like(acc)
            for d in range(sp - 1):
                other_half(l, k, d)
            lax.fori_loop(0, tp, body, 0)

        def blend(c, carry):
            at = pl.ds(pl.multiple_of(c * CHUNK, CHUNK), CHUNK)
            r = inv[at, 0:1]
            v = (acc_sig[at, :] * r) * sigmoid(acc_gate[at, :] * r)
            to = pl.ds(pl.multiple_of(hp + c * CHUNK, 8), CHUNK)
            padded[to, :] = v.astype(BF16).astype(F32)
            return carry

        lax.fori_loop(0, rows // CHUNK, blend, 0)
        tail[l] = padded[rows : rows + hp, :].astype(BF16)

        @pl.when(s < sp - 1)
        def _():
            halo_copy(l).start()

    def convolve(l):
        def settle():
            @pl.when(s > 0)
            def _():
                halo_copy(l).wait_recv()
                padded[0:hp, :] = halo[l].astype(F32)

            @pl.when(s == 0)
            def _():
                padded[0:hp, :] = jnp.zeros((hp, local), F32)

        tap_rows = taps[:, l, :].astype(F32)
        first = hp - (kernel_taps - 1)
        lane = lax.broadcasted_iota(jnp.int32, (CHUNK, 128), 1)
        for c in [*range(1, rows // CHUNK), 0]:
            if c == 0:
                settle()
            low = c * CHUNK
            total = jnp.broadcast_to(bias[l : l + 1, :].astype(F32), (CHUNK, local))
            for j in range(kernel_taps):
                start = low + first + j
                total = total + tap_rows[j : j + 1, :] * padded[start : start + CHUNK, :]
            filt[low : low + CHUNK, :] = total
            one = jnp.sum(total, axis=1, keepdims=True)
            two = jnp.sum(total * total, axis=1, keepdims=True)
            stat_cols[low : low + CHUNK, :] = jnp.where(
                lane == 0, one, jnp.where(lane == 1, two, 0.0)
            )
        stat_rows[l, t] = jnp.transpose(stat_cols[...])[0:8, :]
        for i in range(1, tp):
            stat_copy(l, i, t).start()

    def activate(l):
        for i in range(1, tp):
            stat_copy(l, i, lax.rem(t + i, tp)).wait_recv()
        sums = jnp.sum(stat_rows[l], axis=0)
        stat_cols[...] = jnp.transpose(
            jnp.concatenate([sums, jnp.zeros((120, rows), F32)], axis=0)
        )
        gains, shifts = ln_gain[l : l + 1, :].astype(F32), ln_shift[l : l + 1, :].astype(F32)

        def body(c, carry):
            at = pl.ds(pl.multiple_of(c * CHUNK, CHUNK), CHUNK)
            average = stat_cols[at, 0:1] / channels
            spread = stat_cols[at, 1:2] / channels - average * average
            v = (filt[at, :] - average) * lax.rsqrt(spread + EPS) * gains + shifts
            acts[l, t, at, :] = (v * sigmoid(v)).astype(BF16)
            return carry

        lax.fori_loop(0, rows // CHUNK, body, 0)

    def update(l):
        columns = width // tp
        tile = min(256, columns)
        deep = 128

        def body(c, carry):
            at = pl.ds(pl.multiple_of(c * deep, deep), deep)
            for n in range(columns // tile):
                cut = slice(n * tile, (n + 1) * tile)
                total = feats[l, t, at, cut].astype(F32)
                for b in range(tp):
                    w = out_all[l, b * share : (b + 1) * share, :, :, :, cut].reshape(local, tile)
                    total = total + jnp.dot(acts[l, b, at, :], w, preferred_element_type=F32)
                if l + 1 < layers:
                    feats[l + 1, t, at, cut] = total.astype(BF16)
                else:
                    result[at, cut] = total.astype(BF16)
            return carry

        lax.fori_loop(0, rows // deep, body, 0)

    hops = range(sp - 1)
    own(0, SIG)
    own(0, GATE)
    own_stream.wait()
    spread_start(feats.at[0], 0)
    for l in range(layers):
        x_cut = [(d, k) for d in hops for k in (SIG, GATE)]
        middle = len(x_cut) - 3 if l == 0 else len(x_cut) - 2
        for i, (d, k) in enumerate(x_cut):
            if l and i == 0:
                continue
            if i == middle:
                if l:
                    own(l, OUT)
                spread_relay(feats.at[l], 2 * l)
            relay(l, k, d)
        if l == 0:
            own(l, OUT)
        spread_wait(feats.at[l], 2 * l)
        normalise(l)
        project(l)

        @pl.when(inner)
        def _(l=l):
            for d in hops:
                relay(l, OUT, d)

        if l + 1 < layers:
            own(l + 1, SIG)
            own(l + 1, GATE)
        convolve(l)

        @pl.when(jnp.logical_not(inner))
        def _(l=l):
            for d in hops:
                relay(l, OUT, d)

        activate(l)
        spread_start(acts.at[l], 2 * l + 1)
        if l + 1 < layers:
            relay(l + 1, SIG, 0)
        spread_relay(acts.at[l], 2 * l + 1)
        for d in hops:
            other_half(l, OUT, d)
        spread_wait(acts.at[l], 2 * l + 1)
        update(l)
        if l + 1 < layers:
            spread_start(feats.at[l + 1], 2 * l + 2)

    for l in range(layers):
        for k in (SIG, GATE, OUT):
            own(l, k, done=True)
            for d in hops:
                relay(l, k, d, done=True)
        spread_done(feats.at[l], 2 * l)
        spread_done(acts.at[l], 2 * l + 1)
        for i in range(1, tp):
            stat_copy(l, i, t).wait_send()

        @pl.when(s < sp - 1)
        def _(l=l):
            halo_copy(l).wait_send()


def direct(l, k, q, count):
    return l > 0 or q < count // 2 or count == 1


def fold_kernel(
    sizes,
    stream, gain_in, w_signal, w_gate, taps_in, bias_in, ln_gain_in, ln_shift_in, w_out,
    result, gain, taps, bias, ln_gain, ln_shift,
    sig_all, gate_all, out_all, feats, far, scaled, squares, acc_sig, acc_gate,
    back, tail, halo, padded, filt, stat_cols, stat_rows, acts,
    final, small_sem, load_sem, stream_sem, final_sem, z_send, end_send, z_recv, y_send, rest_send, y_recv,
    cross_send, cross_recv, core_send, core_recv,
    far_send, far_recv, back_send, back_recv,
    halo_send, halo_recv, stat_send, stat_recv,
):
    groups, sp, tp, layers, rows, kernel_taps, hp, width, channels = sizes
    g, s, t = lax.axis_index("grp"), lax.axis_index("sp"), lax.axis_index("tp")
    chips = tp // 2
    core, chip = lax.rem(t, 2), lax.div(t, 2)
    mate = t + 1 - 2 * core
    last, middle = sp - 1, sp // 2
    outer = (s == 0) | (s == last)
    inner = jnp.logical_not(outer)
    pair = s + 1 - 2 * lax.rem(s, 2)
    mid = jnp.where(outer, pair, s)
    end = jnp.where(outer, s, pair)
    mid2, end2 = last - mid, last - end
    banks = (sig_all, gate_all, out_all)
    held = (w_signal, w_gate, w_out)
    pieces = [w.shape[2] for w in held]
    local, part = channels // tp, width // tp
    parts = [(rows - (h + 1) * DEEP, DEEP) for h in range(rows // DEEP)]
    every = range(len(parts))
    both_in = (SIG, GATE)
    other_group = {"grp": 1 - g}

    def load(l, k):
        return pltpu.make_async_copy(held[k].at[l], banks[k].at[l, s], load_sem.at[l, k])

    own_stream = pltpu.make_async_copy(stream, feats.at[0, t], stream_sem)
    small = [
        pltpu.make_async_copy(ref, to, small_sem.at[i])
        for i, (ref, to) in enumerate((
            (gain_in, gain), (taps_in, taps), (bias_in, bias),
            (ln_gain_in, ln_gain), (ln_shift_in, ln_shift),
        ))
    ]
    barrier = pltpu.get_barrier_semaphore()

    def greet(where):
        pl.semaphore_signal(barrier, inc=1, device_id=where, device_id_type=MESH)

    @pl.when(s > 0)
    def _():
        greet({"sp": s - 1})

    @pl.when(s < last)
    def _():
        greet({"sp": s + 1})

    for i in range(1, groups):
        greet({"grp": lax.rem(g + i, groups)})
    for i in range(1, tp):
        greet({"tp": lax.rem(t + i, tp)})
    for k in both_in:
        load(0, k).start()
    own_stream.start()
    load(0, OUT).start()
    for l in range(1, layers):
        for k in range(3):
            load(l, k).start()
    for copy in small:
        copy.start()
    pl.semaphore_wait(
        barrier,
        jnp.where(s > 0, 1, 0) + jnp.where(s < last, 1, 0) + (groups - 1 + tp - 1),
    )

    where = (pair, mid2, end2, s)

    def z_copy(l, k, q, kind, to, sems, spot):
        ref = banks[k].at[l, where[kind], g, q]
        return pltpu.make_async_remote_copy(
            src_ref=ref, dst_ref=ref,
            send_sem=sems.at[l, k // OUT], recv_sem=z_recv.at[l, k, q, spot],
            device_id={"sp": to}, device_id_type=MESH,
        )

    def y_copy(l, k, q, kind, half, to, sems, spot):
        ref = banks[k].at[l, where[kind], half, q]
        return pltpu.make_async_remote_copy(
            src_ref=ref, dst_ref=ref,
            send_sem=sems.at[l, k // OUT], recv_sem=y_recv.at[l, k, spot],
            device_id=to, device_id_type=MESH,
        )

    def across(l, k, q, kind):
        y_copy(l, k, q, kind, g, other_group, y_send, kind).start()

    def to_end(l, k, q, kind):
        z_copy(l, k, q, kind, end, end_send, PAIR if kind == OWN else kind).start()

    def to_middle(l, k, q, kind):
        z_copy(l, k, q, kind, mid2, z_send, FAR_MID if kind == OWN else FAR_END).start()

    def lift(l, k, q):
        z_copy(l, k, q, OWN, mid, z_send, PAIR).start()

    def lift_other(l, k, q):
        if direct(l, k, q, pieces[k]):
            y_copy(l, k, q, OWN, 1 - g, {"sp": mid}, end_send, PAIR).start()

    def arrived(l, k, q, kind):
        z_copy(l, k, q, kind, mid, z_send, kind).wait_recv()

    def each(l, kinds, act, low=0, high=4):
        for k in kinds:
            for q in range(pieces[k] * low // 4, pieces[k] * high // 4):
                act(l, k, q)

    def pass_on(l, k, q):
        arrived(l, k, q, PAIR)
        to_middle(l, k, q, PAIR)

    def take(kind, onward=True):
        def act(l, k, q):
            arrived(l, k, q, kind)
            if onward:
                to_end(l, k, q, kind)
            if not (onward and kind == FAR_MID and whole(l, k)):
                across(l, k, q, kind)
        return act

    def onward(kind):
        return lambda l, k, q: to_end(l, k, q, kind)

    def bypass(kind):
        return lambda l, k, q: across(l, k, q, kind)

    def share_rest(l, k, q):
        if not direct(l, k, q, pieces[k]):
            y_copy(l, k, q, PAIR, g, other_group, rest_send, PAIR).start()

    def got(kind):
        return lambda l, k, q: arrived(l, k, q, kind)

    def own_in(l, k, q):
        to_middle(l, k, q, OWN)

    def whole(l, k):
        return l == layers - 1 and k == OUT

    def own_other(l, k, q):
        y_copy(l, k, q, OWN, 1 - g, {"sp": mid2}, y_send, FAR_MID).start()

    def ready(l, k, kind):
        ref = banks[k].at[l, where[kind], 1 - g]
        pltpu.make_async_copy(ref, ref, y_recv.at[l, k, kind]).wait()

    def ready_all(l, k):
        for kind in (PAIR, FAR_MID, FAR_END):
            ready(l, k, kind)

    def sent(sems, pick):
        for l in range(layers):
            for kinds in (both_in, (OUT,)):
                k = kinds[0]
                count, half = sum(pick(l, k, pieces[k]) for k in kinds), pieces[k]
                if count == 0:
                    continue
                if count % (2 * half) == 0:
                    ref = banks[k].at[l, pl.ds(0, count // (2 * half))]
                elif count % half == 0:
                    ref = banks[k].at[l, pl.ds(0, count // half), 0]
                else:
                    ref = banks[k].at[l, 0, 0, pl.ds(0, count)]
                pltpu.make_async_copy(ref, ref, sems.at[l, k // OUT]).wait()

    def straight(l, k, count):
        return sum(direct(l, k, q, count) for q in range(count))

    def rows_of(h):
        return pl.ds(parts[h][0], parts[h][1])

    def cross_copy(buf, n, h, block, i):
        ref = buf.at[block, rows_of(h)]
        return pltpu.make_async_remote_copy(
            src_ref=ref, dst_ref=ref,
            send_sem=cross_send.at[n, i - 1], recv_sem=cross_recv.at[n, h, i - 1],
            device_id={"tp": lax.rem(chip + i, chips) * 2 + core}, device_id_type=MESH,
        )

    def core_copy(buf, n, h, block, i):
        ref = buf.at[block, rows_of(h)]
        return pltpu.make_async_remote_copy(
            src_ref=ref, dst_ref=ref,
            send_sem=core_send.at[n, i], recv_sem=core_recv.at[n, h, i],
            device_id={"tp": mate}, device_id_type=MESH,
        )

    def chip_at(i):
        return lax.rem(chip + i, chips) * 2

    def spread_start(buf, n, h):
        for i in range(1, chips):
            cross_copy(buf, n, h, t, i).start()
        core_copy(buf, n, h, t, 0).start()

    def spread_relay(buf, n, h):
        for i in range(1, chips):
            block = chip_at(i) + core
            cross_copy(buf, n, h, block, chips - i).wait_recv()
            core_copy(buf, n, h, block, i).start()

    def spread_near(buf, n, h):
        core_copy(buf, n, h, mate, 0).wait_recv()

    def spread_rest(buf, n, h):
        for i in range(1, chips):
            core_copy(buf, n, h, chip_at(i) + 1 - core, i).wait_recv()

    def spread_done(buf, n):
        ref = buf.at[t]
        for i in range(1, chips):
            pltpu.make_async_copy(ref, ref, cross_send.at[n, i - 1]).wait()
        for i in range(chips):
            pltpu.make_async_copy(ref, ref, core_send.at[n, i]).wait()

    far_blocks = [lax.rem(chip + i, chips) * 2 + c for i in range(1, chips) for c in (core, 1 - core)]
    near_blocks = [t, mate]

    def far_copy(h):
        return pltpu.make_async_remote_copy(
            src_ref=feats.at[0, t, rows_of(h)], dst_ref=far.at[t, rows_of(h)],
            send_sem=far_send, recv_sem=far_recv.at[h],
            device_id={"sp": mid}, device_id_type=MESH,
        )

    def back_copy(h):
        ref = back.at[rows_of(h)]
        return pltpu.make_async_remote_copy(
            src_ref=ref, dst_ref=ref,
            send_sem=back_send, recv_sem=back_recv.at[h],
            device_id={"sp": end}, device_id_type=MESH,
        )

    def stat_copy(l, h, i, block):
        ref = stat_rows.at[l, block, :, rows_of(h)]
        return pltpu.make_async_remote_copy(
            src_ref=ref, dst_ref=ref,
            send_sem=stat_send.at[l, i - 1], recv_sem=stat_recv.at[l, h],
            device_id={"tp": lax.rem(t + i, tp)}, device_id_type=MESH,
        )

    def halo_copy(l):
        return pltpu.make_async_remote_copy(
            src_ref=tail.at[l], dst_ref=halo.at[l],
            send_sem=halo_send.at[l], recv_sem=halo_recv.at[l],
            device_id={"sp": s + 1}, device_id_type=MESH,
        )

    def halo_goes(l):
        return s < last if l else inner

    def over(h, body):
        first, count = parts[h]

        def step(c, carry):
            body(pl.multiple_of(first + c * CHUNK, CHUNK))
            return carry

        lax.fori_loop(0, count // CHUNK, step, 0)

    def scale(which, l, source, b, h, fresh):
        cut = pl.ds(pl.multiple_of(b * part, 128), part)

        def body(low):
            at = pl.ds(low, CHUNK)
            x = source[b, at, :].astype(F32)
            square = x * x
            total = square[:, 0:128]
            for j in range(1, part // 128):
                total = total + square[:, j * 128 : (j + 1) * 128]
            squares[which, at, :] = total if fresh else squares[which, at, :] + total
            scaled[which, b, at, :] = (x * gain[l : l + 1, cut].astype(F32)).astype(BF16)

        over(h, body)

    def accumulate(which, l, b, h, fresh, kinds=(SIG, GATE)):
        at = rows_of(h)
        for k in kinds:
            acc = (acc_sig, acc_gate)[k]
            w = banks[k][l, b].reshape(part, local)
            more = jnp.dot(scaled[which, b, at, :], w, preferred_element_type=F32)
            acc[which, at, :] = more if fresh else acc[which, at, :] + more

    def blend(which, h):
        def body(low):
            at = pl.ds(low, CHUNK)
            total = jnp.sum(squares[which, at, :], axis=1, keepdims=True)
            r = lax.rsqrt(total / width + EPS)
            v = (acc_sig[which, at, :] * r) * sigmoid(acc_gate[which, at, :] * r)
            v = v.astype(BF16)
            if which:
                back[at, :] = v
            else:
                padded[pl.ds(pl.multiple_of(hp + low, 8), CHUNK), :] = v.astype(F32)

        over(h, body)

    def send_tail(l):
        tail[l] = padded[rows : rows + hp, :].astype(BF16)

        @pl.when(halo_goes(l))
        def _():
            halo_copy(l).start()

    def settle(l):
        @pl.when(s >= middle if l == 0 else s > 0)
        def _():
            halo_copy(l).wait_recv()
            padded[0:hp, :] = halo[l].astype(F32)

        if l == 0:
            @pl.when(inner & (s < middle))
            def _():
                padded[0:hp, :] = back[rows - hp : rows, :].astype(F32)

        @pl.when(s == 0)
        def _():
            padded[0:hp, :] = jnp.zeros((hp, local), F32)

    def convolve(l, h, stages=(0, 1)):
        begin, count = parts[h]
        tap_rows = taps[:, l, :].astype(F32)
        first = hp - (kernel_taps - 1)
        lane = lax.broadcasted_iota(jnp.int32, (CHUNK, 128), 1)
        chunks = list(range(begin // CHUNK, (begin + count) // CHUNK))
        chunks = (chunks[1:] if 0 in stages else []) + (chunks[:1] if 1 in stages else [])
        for c in chunks:
            if c == 0:
                settle(l)
            low = c * CHUNK
            total = jnp.broadcast_to(bias[l : l + 1, :].astype(F32), (CHUNK, local))
            for j in range(kernel_taps):
                start = low + first + j
                total = total + tap_rows[j : j + 1, :] * padded[start : start + CHUNK, :]
            filt[low : low + CHUNK, :] = total
            one = jnp.sum(total, axis=1, keepdims=True)
            two = jnp.sum(total * total, axis=1, keepdims=True)
            stat_cols[low : low + CHUNK, :] = jnp.where(
                lane == 0, one, jnp.where(lane == 1, two, 0.0)
            )
        if 1 not in stages:
            return
        at = slice(begin, begin + count)
        stat_rows[l, t, :, at] = jnp.transpose(stat_cols[at, :])[0:8, :]
        for i in range(1, tp):
            stat_copy(l, h, i, t).start()

    def activate(l, h):
        begin, count = parts[h]
        at = slice(begin, begin + count)
        ref = stat_rows.at[l, pl.ds(0, tp - 1), :, rows_of(h)]
        pltpu.make_async_copy(ref, ref, stat_recv.at[l, h]).wait()
        sums = stat_rows[l, 0, :, at]
        for b in range(1, tp):
            sums = sums + stat_rows[l, b, :, at]
        stat_cols[at, :] = jnp.transpose(
            jnp.concatenate([sums, jnp.zeros((120, count), F32)], axis=0)
        )
        gains, shifts = ln_gain[l : l + 1, :].astype(F32), ln_shift[l : l + 1, :].astype(F32)

        def body(low):
            at = pl.ds(low, CHUNK)
            average = stat_cols[at, 0:1] / channels
            spread = stat_cols[at, 1:2] / channels - average * average
            v = (filt[at, :] - average) * lax.rsqrt(spread + EPS) * gains + shifts
            acts[l, t, at, :] = (v * sigmoid(v)).astype(BF16)

        over(h, body)
        spread_start(acts.at[l], layers + l, h)

    def write(h):
        return pltpu.make_async_copy(
            final.at[rows_of(h)], result.at[rows_of(h)], final_sem
        )

    def update(l, h):
        begin, count = parts[h]
        tile = min(256, part)

        def body(c, carry):
            at = pl.ds(pl.multiple_of(begin + c * DEEP, DEEP), DEEP)
            for n in range(part // tile):
                cut = slice(n * tile, (n + 1) * tile)
                total = feats[l, t, at, cut].astype(F32)
                for b in range(tp):
                    w = out_all[l, b, :, :, :, cut].reshape(local, tile)
                    total = total + jnp.dot(acts[l, b, at, :], w, preferred_element_type=F32)
                if l + 1 < layers:
                    feats[l + 1, t, at, cut] = total.astype(BF16)
                else:
                    final[at, cut] = total.astype(BF16)
            return carry

        lax.fori_loop(0, count // DEEP, body, 0)
        if l + 1 == layers:
            write(h).start()

    far_n = 2 * layers

    def spread_end(buf, n, h):
        spread_relay(buf, n, h)
        spread_near(buf, n, h)
        spread_rest(buf, n, h)

    def scale_all(which, l, source, h):
        for i, b in enumerate(near_blocks + far_blocks):
            scale(which, l, source, b, h, i == 0)

    def fetch(h):
        back_copy(h).wait_recv()

        def body(low):
            to = pl.ds(pl.multiple_of(hp + low, 8), CHUNK)
            padded[to, :] = back[pl.ds(low, CHUNK), :].astype(F32)

        over(h, body)

    def settle_far(h, blocks):
        for i, b in enumerate(blocks):
            accumulate(1, 0, b, h, i == 0)
        blend(1, h)
        back_copy(h).start()

    @pl.when(outer)
    def _():
        for k in both_in:
            load(0, k).wait()
            each(0, (k,), lift)
        own_stream.wait()
        load(0, OUT).wait()
        for h in every:
            far_copy(h).start()
        each(0, both_in, lift_other)
        each(0, (OUT,), lift)
        for k in range(3):
            load(1, k).wait()
        each(1, (SIG,), lift)
        each(0, (OUT,), lift_other)
        each(1, (GATE,), lift)
        each(1, (SIG,), lift_other)
        each(1, (OUT,), lift)
        each(1, (GATE, OUT), lift_other)
        each(0, (OUT,), take(PAIR, False))
        each(1, range(3), take(PAIR, False))
        each(0, (OUT,), take(FAR_MID, False))
        each(1, (SIG,), take(FAR_MID, False), 0, 3)
        fetch(0)
        each(1, (SIG,), take(FAR_MID, False), 3, 4)

    @pl.when(inner)
    def _():
        for k in both_in:
            load(0, k).wait()
            each(0, (k,), own_in)
        own_stream.wait()
        for h in every:
            spread_start(feats.at[0], 0, h)
        load(0, OUT).wait()
        each(0, (OUT,), onward(OWN))
        for k in range(3):
            load(1, k).wait()
        each(1, range(3), onward(OWN))
        for k in both_in:
            for q in range(pieces[k]):
                pass_on(0, k, q)
                take(FAR_MID, False)(0, k, q)
            spread_relay(feats.at[0], 0, k)
        each(0, (OUT,), own_in)
        each(1, (SIG,), own_in)
        each(0, (SIG,), take(FAR_END, False))
        far_copy(0).wait_recv()
        spread_start(far, far_n, 0)
        for h in every[2:]:
            spread_relay(feats.at[0], 0, h)
        each(0, (GATE,), take(FAR_END, False), 0, 3)
        for h in every[1:-1]:
            far_copy(h).wait_recv()
            spread_start(far, far_n, h)
        each(0, (GATE,), take(FAR_END, False), 3, 4)
        each(0, both_in, share_rest)
        small[0].wait()
        for h in every:
            spread_near(feats.at[0], 0, h)
            spread_rest(feats.at[0], 0, h)
            scale_all(0, 0, feats.at[0], h)
            each(0, (OUT,), take(FAR_MID), h, h + 1)
        spread_end(far, far_n, 0)
        each(0, (OUT,), take(FAR_MID), len(parts), 4)
        scale_all(1, 0, far, 0)
        for k in both_in:
            ready(0, k, FAR_MID)
        for h in every[:1]:
            for i, b in enumerate((s, mid2)):
                accumulate(0, 0, b, h, i == 0)
        far_copy(every[-1]).wait_recv()
        spread_start(far, far_n, every[-1])
        for h in every[1:]:
            for i, b in enumerate((s, mid2)):
                accumulate(0, 0, b, h, i == 0)
        each(1, (SIG,), take(FAR_MID), 0, 1)
        for h in every[1:-1]:
            spread_relay(far, far_n, h)
        each(1, (SIG,), take(FAR_MID), 1, 3)
        for h in every[1:-1]:
            spread_near(far, far_n, h)
            spread_rest(far, far_n, h)
            scale_all(1, 0, far, h)
        for k in both_in:
            ready(0, k, FAR_END)
            ready(0, k, PAIR)
        blocks = (s, mid2, end2, end)
        settle_far(0, blocks)
        each(1, (SIG,), take(FAR_MID), 3, 4)
        each(0, (OUT,), pass_on, 0, 1)
        for h in every[1:-1]:
            settle_far(h, blocks)
        each(0, (OUT,), pass_on, 1, 3)
        spread_end(far, far_n, every[-1])
        scale_all(1, 0, far, every[-1])
        each(0, (OUT,), pass_on, 3, 4)
        each(1, (GATE,), own_in)
        settle_far(every[-1], blocks)
        each(0, (OUT,), share_rest)
        each(0, (OUT,), take(FAR_END), 0, 1)
        for h in every:
            for b in (end2, end):
                accumulate(0, 0, b, h, False)
            blend(0, h)
            if h == 0:
                send_tail(0)
            each(0, (OUT,), take(FAR_END), h + 1, h + 2)
        each(1, (SIG,), pass_on, 0, 2)

    @pl.when(outer)
    def _():
        small[0].wait()

    for copy in small[1:]:
        copy.wait()
    convolve(0, 0, (0,))
    for h in every:
        if h + 1 < len(parts):
            @pl.when(outer)
            def _(h=h):
                fetch(h + 1)

        convolve(0, h, (1,))
        if h + 1 < len(parts):
            convolve(0, h + 1, (0,))

        @pl.when(outer)
        def _(h=h):
            if h:
                each(0, (OUT,), take(FAR_END, False), h - 1, h)

        if h == 0:
            @pl.when(inner)
            def _():
                each(1, (SIG,), pass_on, 2, 3)

    @pl.when(inner)
    def _():
        each(1, (SIG,), pass_on, 3, 4)
        each(1, (GATE,), take(FAR_MID), 0, 2)

    for h in every:
        activate(0, h)
        if h == 0:
            @pl.when(outer)
            def _():
                each(0, (OUT,), take(FAR_END, False), 2, 4)

            @pl.when(inner)
            def _():
                each(1, (GATE,), take(FAR_MID), 2, 4)

    @pl.when(inner)
    def _():
        each(1, (SIG,), take(FAR_END), 0, 1)
        each(1, (GATE,), pass_on, 0, 1)

    @pl.when(outer)
    def _():
        each(1, (GATE,), take(FAR_MID, False), 0, 2)

    for h in every:
        spread_relay(acts.at[0], layers, h)
        if h == 0:
            ready_all(0, OUT)
        spread_near(acts.at[0], layers, h)
        spread_rest(acts.at[0], layers, h)
        update(0, h)
        spread_start(feats.at[1], 1, h)

        @pl.when(inner)
        def _(h=h):
            for q in range(2 * h + 1, min(2 * h + 3, 4)):
                each(1, (SIG,), take(FAR_END), q, q + 1)
                each(1, (GATE,), pass_on, q, q + 1)

        @pl.when(outer)
        def _(h=h):
            if h == 0:
                each(1, (GATE,), take(FAR_MID, False), 2, 4)
            else:
                each(1, (SIG,), take(FAR_END, False), h - 1, h)

    x = feats.at[1]
    for h in every:
        scale(0, 1, x, t, h, True)

    @pl.when(inner)
    def _():
        each(1, (OUT,), own_in)
        each(1, (GATE,), take(FAR_END), 0, 2)

    @pl.when(outer)
    def _():
        each(1, (SIG,), take(FAR_END, False), len(parts) - 1, 4)

    for h in every:
        spread_near(x, 1, h)
        scale(0, 1, x, mate, h, False)

    home = lax.div(s, 2) == chip
    first_near, first_far = jnp.where(home, s, mid2), jnp.where(home, mid2, s)

    def fold_far(h):
        spread_rest(x, 1, h)
        for b in far_blocks:
            scale(0, 1, x, b, h, False)
            accumulate(0, 1, b, h, False, (SIG,))
        accumulate(0, 1, first_far, h, False, (GATE,))

    @pl.when(inner)
    def _():
        each(1, (GATE,), take(FAR_END), 2, 4)

    for step in range(4):
        @pl.when(inner)
        def _(step=step):
            if step == 0:
                spread_relay(x, 1, 0)
            each(1, (OUT,), take(FAR_MID), step, step + 1)
            each(1, (OUT,), pass_on, step, step + 1)
            if step == 3:
                each(1, (OUT,), own_other)

        @pl.when(outer)
        def _(step=step):
            each(1, (GATE,), take(FAR_END, False), step, step + 1)
            if step == 0:
                spread_relay(x, 1, 0)

        if step == 0:
            ready(1, GATE, FAR_MID)
            for h in every:
                accumulate(0, 1, first_near, h, True, (GATE,))
        if step == 1:
            ready_all(1, SIG)
            for h in every:
                for i, b in enumerate(near_blocks):
                    accumulate(0, 1, b, h, i == 0, (SIG,))
        if step == 2:
            fold_far(0)
    def take_out(kind_outer, kind_inner, low, high):
        @pl.when(outer)
        def _():
            each(1, (OUT,), take(kind_outer, False), low, high)

        if kind_inner is not None:
            @pl.when(inner)
            def _():
                each(1, (OUT,), take(kind_inner), low, high)

    spread_relay(x, 1, 1)
    fold_far(1)
    take_out(FAR_MID, FAR_END, 0, 1)
    ready(1, GATE, PAIR)
    ready(1, GATE, FAR_END)
    take_out(FAR_MID, FAR_END, 1, 2)
    for h in every:
        if h > 1:
            spread_relay(x, 1, h)
            convolve(1, h - 1, (0,))
            take_out(FAR_MID, None, 3, 4)
            fold_far(h)
            take_out(FAR_END, None, 0, 1)
        for b in (pair, end2):
            accumulate(0, 1, b, h, False, (GATE,))
        blend(0, h)
        if h == 0:
            send_tail(1)
            take_out(FAR_MID, FAR_END, 2, 3)
            convolve(1, 0, (0,))
        else:
            convolve(1, h - 1, (1,))
            if h == 1:
                @pl.when(inner)
                def _():
                    each(1, (OUT,), take(FAR_END), 3, 4)
    take_out(FAR_END, None, 1, 2)
    convolve(1, every[-1])
    take_out(FAR_END, None, 2, 3)
    activate(1, 0)
    take_out(FAR_END, None, 3, 4)
    for h in every[1:]:
        activate(1, h)
    for h in every:
        spread_relay(acts.at[1], layers + 1, h)
    ready_all(1, OUT)
    for h in every:
        spread_near(acts.at[1], layers + 1, h)
        spread_rest(acts.at[1], layers + 1, h)
        update(1, h)

    @pl.when(outer)
    def _():
        pltpu.make_async_copy(feats.at[0, t], feats.at[0, t], far_send).wait()
        sent(z_send, lambda l, k, n: n)
        sent(end_send, straight)
        sent(y_send, lambda l, k, n: 3 * n if l or k == OUT else 0)

    @pl.when(inner)
    def _():
        spread_done(feats.at[0], 0)
        spread_done(far, far_n)
        pltpu.make_async_copy(back, back, back_send).wait()
        sent(z_send, lambda l, k, n: 2 * n)
        sent(y_send, lambda l, k, n: 2 * n)
        sent(end_send, lambda l, k, n: 3 * n if l or k == OUT else 0)
        sent(rest_send, lambda l, k, n: n - straight(l, k, n))

    for l in range(layers):
        if l:
            spread_done(feats.at[l], l)
        spread_done(acts.at[l], layers + l)
        for i in range(1, tp):
            ref = stat_rows.at[l, t]
            pltpu.make_async_copy(ref, ref, stat_send.at[l, i - 1]).wait()

        @pl.when(halo_goes(l))
        def _(l=l):
            halo_copy(l).wait_send()

    pltpu.make_async_copy(final, final, final_sem).wait()


def shards(counts, stream, norm_gain, w_signal, w_gate, conv_taps, conv_bias, ln_gain, ln_shift, w_out):
    groups, sp, tp = counts
    layers, deep, local = w_signal.shape
    rows, part = stream.shape
    kernel_taps = conv_taps.shape[1]
    hp = -(-(kernel_taps - 1) // 16) * 16
    width, channels = part * tp, local * tp

    folds = (
        groups == 2 and layers == 2 and sp == tp and sp // 2 == 2
        and rows % DEEP == 0 and rows > DEEP
    )
    wanted = FOLD_PIECES if folds else PIECES

    def cut(w):
        half = w.shape[1] // groups
        count = wanted if half % (16 * wanted) == 0 else 1
        return w.reshape(layers, groups, count, half // count, w.shape[2])

    w_signal, w_gate, w_out = cut(w_signal), cut(w_gate), cut(w_out)
    bank = lambda w: pltpu.VMEM((layers, sp) + w.shape[1:], BF16)
    most = max(w.shape[2] for w in (w_signal, w_gate, w_out))
    line = (layers, 3, most, sp)
    dma = lambda *shape: pltpu.SemaphoreType.DMA(shape)
    anywhere = pl.BlockSpec(memory_space=pl.ANY)
    inside = pl.BlockSpec(memory_space=pltpu.VMEM)
    count = max(1, rows // DEEP)
    spreads, chips = 2 * layers + 1, tp // 2
    if folds:
        body = fold_kernel
        scratch = [
            pltpu.VMEM(norm_gain.shape, BF16),
            pltpu.VMEM((kernel_taps, layers, local), BF16),
            pltpu.VMEM(conv_bias.shape, BF16),
            pltpu.VMEM(ln_gain.shape, BF16),
            pltpu.VMEM(ln_shift.shape, BF16),
            bank(w_signal), bank(w_gate), bank(w_out),
            pltpu.VMEM((layers, tp, rows, part), BF16),
            pltpu.VMEM((tp, rows, part), BF16),
            pltpu.VMEM((2, tp, rows, part), BF16),
            pltpu.VMEM((2, rows, 128), F32),
            pltpu.VMEM((2, rows, local), F32),
            pltpu.VMEM((2, rows, local), F32),
            pltpu.VMEM((rows, local), BF16),
            pltpu.VMEM((layers, hp, local), BF16),
            pltpu.VMEM((layers, hp, local), BF16),
            pltpu.VMEM((hp + rows, local), F32),
            pltpu.VMEM((rows, local), F32),
            pltpu.VMEM((rows, 128), F32),
            pltpu.VMEM((layers, tp, 8, rows), F32),
            pltpu.VMEM((layers, tp, rows, local), BF16),
            pltpu.VMEM((rows, part), BF16),
            dma(5), dma(layers, 3), pltpu.SemaphoreType.DMA, pltpu.SemaphoreType.DMA,
            dma(layers, 2), dma(layers, 2), dma(layers, 3, most, 3),
            dma(layers, 2), dma(layers, 2), dma(layers, 3, 3),
            dma(spreads, chips - 1), dma(spreads, count, chips - 1),
            dma(spreads, chips), dma(spreads, count, chips),
            pltpu.SemaphoreType.DMA, dma(count), pltpu.SemaphoreType.DMA, dma(count),
            dma(layers), dma(layers), dma(layers, tp - 1), dma(layers, count),
        ]
    else:
        body = kernel
        scratch = [
            bank(w_signal), bank(w_gate), bank(w_out),
            pltpu.VMEM((layers, tp, rows, part), BF16),
            pltpu.VMEM((tp, rows, part), BF16),
            pltpu.VMEM((rows, 128), F32),
            pltpu.VMEM((rows, local), F32),
            pltpu.VMEM((rows, local), F32),
            pltpu.VMEM((layers, hp, local), BF16),
            pltpu.VMEM((layers, hp, local), BF16),
            pltpu.VMEM((hp + rows, local), F32),
            pltpu.VMEM((rows, local), F32),
            pltpu.VMEM((rows, 128), F32),
            pltpu.VMEM((layers, tp, 8, rows), F32),
            pltpu.VMEM((layers, tp, rows, local), BF16),
            dma(layers, 3), pltpu.SemaphoreType.DMA,
            dma(layers, 3, most), dma(*line), dma(*line), dma(*line), dma(*line),
            dma(2 * layers, tp), dma(2 * layers, tp), dma(2 * layers, tp), dma(2 * layers, tp),
            dma(layers), dma(layers), dma(layers, tp), dma(layers, tp),
        ]
    return pl.pallas_call(
        functools.partial(
            body, (groups, sp, tp, layers, rows, kernel_taps, hp, width, channels)
        ),
        out_shape=jax.ShapeDtypeStruct(stream.shape, BF16),
        in_specs=[anywhere] * 9 if folds else [
            anywhere, inside, anywhere, anywhere, inside, inside, inside, inside, anywhere,
        ],
        out_specs=anywhere if folds else inside,
        scratch_shapes=scratch,
        compiler_params=pltpu.CompilerParams(
            collective_id=0, has_side_effects=True, vmem_limit_bytes=60 * 1024 * 1024
        ),
    )(
        stream, norm_gain, w_signal, w_gate, jnp.transpose(conv_taps, (1, 0, 2)), conv_bias,
        ln_gain, ln_shift, w_out,
    )


def solution(mesh):
    counts = tuple(mesh.shape[name] for name in ("grp", "sp", "tp"))
    return jax.shard_map(
        functools.partial(shards, counts),
        mesh=mesh,
        in_specs=(
            P(("grp", "sp"), "tp"),
            P(),
            P(None, "sp", "tp"),
            P(None, "sp", "tp"),
            P(None, None, "tp"),
            P(None, "tp"),
            P(None, "tp"),
            P(None, "tp"),
            P(None, "sp", "tp"),
        ),
        out_specs=P(("grp", "sp"), "tp"),
        check_vma=False,
    )
```

```python
import functools

import jax
import jax.numpy as jnp
from jax import lax
from jax.experimental import pallas as pl
from jax.experimental.pallas import tpu as pltpu
from jax.sharding import PartitionSpec as P

MESH = pl.DeviceIdType.MESH
EPS = 1e-05
F32 = jnp.float32
BF16 = jnp.bfloat16
SIG, GATE, OUT = 0, 1, 2
CHUNK = 32
PIECES = 2
FOLD_PIECES = 4
DEEP = 128
PAIR, FAR_MID, FAR_END, OWN = 0, 1, 2, 3


def sigmoid(v):
    return 1.0 / (1.0 + jnp.exp(-v))


def kernel(
    sizes,
    stream, gain, w_signal, w_gate, taps, bias, ln_gain, ln_shift, w_out,
    result,
    sig_all, gate_all, out_all, feats, scaled_feats, inv, acc_sig, acc_gate,
    tail, halo, padded, filt, stat_cols, stat_rows, acts,
    load_sem, stream_sem, own_send, z_send, z_recv, y_send, y_recv,
    cross_send, cross_recv, core_send, core_recv,
    halo_send, halo_recv, stat_send, stat_recv,
):
    groups, sp, tp, layers, rows, kernel_taps, hp, width, channels = sizes
    g, s, t = lax.axis_index("grp"), lax.axis_index("sp"), lax.axis_index("tp")
    chips = tp // 2
    core, chip = lax.rem(t, 2), lax.div(t, 2)
    mate = t + 1 - 2 * core
    share = sp // tp
    banks = (sig_all, gate_all, out_all)
    held = (w_signal, w_gate, w_out)

    inner = (s > 0) & (s < sp - 1)
    pieces = [w.shape[2] for w in held]

    def load(l, k):
        return pltpu.make_async_copy(held[k].at[l], banks[k].at[l, s], load_sem.at[l, k])

    own_stream = pltpu.make_async_copy(stream, feats.at[0, t], stream_sem)
    own_stream.start()
    for l in range(layers):
        for k in range(3):
            load(l, k).start()

    barrier = pltpu.get_barrier_semaphore()

    def greet(where):
        pl.semaphore_signal(barrier, inc=1, device_id=where, device_id_type=MESH)

    @pl.when(s > 0)
    def _():
        greet({"sp": s - 1})

    @pl.when(s < sp - 1)
    def _():
        greet({"sp": s + 1})

    for i in range(1, groups):
        greet({"grp": lax.rem(g + i, groups)})
    for i in range(1, tp):
        greet({"tp": lax.rem(t + i, tp)})
    pl.semaphore_wait(
        barrier,
        jnp.where(s > 0, 1, 0) + jnp.where(s < sp - 1, 1, 0) + (groups - 1 + tp - 1),
    )

    def z_copy(l, k, q, shard, way, mine=False):
        ref = banks[k].at[l, shard, g, q]
        return pltpu.make_async_remote_copy(
            src_ref=ref, dst_ref=ref,
            send_sem=own_send.at[l, k, q] if mine and way else z_send.at[l, k, q, shard],
            recv_sem=z_recv.at[l, k, q, shard],
            device_id={"sp": s + 1 if way == 0 else s - 1}, device_id_type=MESH,
        )

    def y_copy(l, k, q, shard, half, where):
        ref = banks[k].at[l, shard, half, q]
        return pltpu.make_async_remote_copy(
            src_ref=ref, dst_ref=ref,
            send_sem=y_send.at[l, k, q, shard], recv_sem=y_recv.at[l, k, q, shard],
            device_id=where, device_id_type=MESH,
        )

    def own(l, k, done=False):
        if not done:
            load(l, k).wait()
        for way, there, end in ((0, s < sp - 1, s == 0), (1, s > 0, s == sp - 1)):
            @pl.when(there)
            def _(way=way, end=end):
                for q in range(pieces[k]):
                    copy = z_copy(l, k, q, s, way, True)
                    copy.wait_send() if done else copy.start()

                @pl.when(end)
                def _():
                    for q in range(pieces[k]):
                        where = {"sp": s + 1 if way == 0 else s - 1}
                        copy = y_copy(l, k, q, s, 1 - g, where)
                        copy.wait_send() if done else copy.start()

    def sides(d):
        left, right = s - 1 - d, s + 1 + d
        return (
            (0, left, left >= 0, s < sp - 1, (left > 0) | (d > 0)),
            (1, right, right <= sp - 1, s > 0, (right < sp - 1) | (d > 0)),
        )

    def relay(l, k, d, done=False):
        for way, shard, here, onward, across in sides(d):
            @pl.when(here)
            def _(way=way, shard=shard, onward=onward, across=across):
                for q in range(pieces[k]):
                    if not done:
                        z_copy(l, k, q, shard, way).wait_recv()

                    @pl.when(onward)
                    def _():
                        copy = z_copy(l, k, q, shard, way)
                        copy.wait_send() if done else copy.start()

                    @pl.when(across)
                    def _():
                        copy = y_copy(l, k, q, shard, g, {"grp": 1 - g})
                        copy.wait_send() if done else copy.start()

    def other_half(l, k, d):
        for _, shard, here, _, _ in sides(d):
            @pl.when(here)
            def _(shard=shard):
                for q in range(pieces[k]):
                    y_copy(l, k, q, shard, 1 - g, {"grp": 1 - g}).wait_recv()

    def cross_copy(buf, n, block, i):
        ref = buf.at[block]
        return pltpu.make_async_remote_copy(
            src_ref=ref, dst_ref=ref,
            send_sem=cross_send.at[n, i], recv_sem=cross_recv.at[n, block],
            device_id={"tp": lax.rem(chip + i, chips) * 2 + core}, device_id_type=MESH,
        )

    def core_copy(buf, n, block):
        ref = buf.at[block]
        return pltpu.make_async_remote_copy(
            src_ref=ref, dst_ref=ref,
            send_sem=core_send.at[n, block], recv_sem=core_recv.at[n, block],
            device_id={"tp": mate}, device_id_type=MESH,
        )

    def spread_start(buf, n):
        for i in range(1, chips):
            cross_copy(buf, n, t, i).start()
        core_copy(buf, n, t).start()

    def spread_relay(buf, n):
        for i in range(1, chips):
            block = lax.rem(chip + i, chips) * 2 + core
            cross_copy(buf, n, block, i).wait_recv()
            core_copy(buf, n, block).start()

    def spread_wait(buf, n):
        for j in range(chips):
            core_copy(buf, n, j * 2 + 1 - core).wait_recv()

    def spread_done(buf, n):
        for i in range(1, chips):
            cross_copy(buf, n, t, i).wait_send()
        for j in range(chips):
            core_copy(buf, n, j * 2 + core).wait_send()

    def stat_copy(l, i, block):
        return pltpu.make_async_remote_copy(
            src_ref=stat_rows.at[l, block], dst_ref=stat_rows.at[l, block],
            send_sem=stat_send.at[l, i], recv_sem=stat_recv.at[l, block],
            device_id={"tp": lax.rem(t + i, tp)}, device_id_type=MESH,
        )

    def halo_copy(l):
        return pltpu.make_async_remote_copy(
            src_ref=tail.at[l], dst_ref=halo.at[l],
            send_sem=halo_send.at[l], recv_sem=halo_recv.at[l],
            device_id={"sp": s + 1}, device_id_type=MESH,
        )

    def normalise(l):
        part = width // tp

        def body(c, carry):
            at = pl.ds(pl.multiple_of(c * CHUNK, CHUNK), CHUNK)
            total = jnp.zeros((CHUNK, 1), F32)
            for b in range(tp):
                x = feats[l, b, at, :].astype(F32)
                total = total + jnp.sum(x * x, axis=1, keepdims=True)
                scaled_feats[b, at, :] = (
                    x * gain[l : l + 1, b * part : (b + 1) * part].astype(F32)
                ).astype(BF16)
            inv[at, :] = jnp.broadcast_to(lax.rsqrt(total / width + EPS), (CHUNK, 128))
            return carry

        lax.fori_loop(0, rows // CHUNK, body, 0)

    local = channels // tp

    def project(l):
        for k, acc in ((SIG, acc_sig), (GATE, acc_gate)):
            def body(b, carry, k=k, acc=acc):
                w = banks[k][l, pl.ds(b * share, share)].reshape(width // tp, local)
                acc[...] += jnp.dot(scaled_feats[b], w, preferred_element_type=F32)
                return carry

            acc[...] = jnp.zeros_like(acc)
            for d in range(sp - 1):
                other_half(l, k, d)
            lax.fori_loop(0, tp, body, 0)

        def blend(c, carry):
            at = pl.ds(pl.multiple_of(c * CHUNK, CHUNK), CHUNK)
            r = inv[at, 0:1]
            v = (acc_sig[at, :] * r) * sigmoid(acc_gate[at, :] * r)
            to = pl.ds(pl.multiple_of(hp + c * CHUNK, 8), CHUNK)
            padded[to, :] = v.astype(BF16).astype(F32)
            return carry

        lax.fori_loop(0, rows // CHUNK, blend, 0)
        tail[l] = padded[rows : rows + hp, :].astype(BF16)

        @pl.when(s < sp - 1)
        def _():
            halo_copy(l).start()

    def convolve(l):
        def settle():
            @pl.when(s > 0)
            def _():
                halo_copy(l).wait_recv()
                padded[0:hp, :] = halo[l].astype(F32)

            @pl.when(s == 0)
            def _():
                padded[0:hp, :] = jnp.zeros((hp, local), F32)

        tap_rows = taps[:, l, :].astype(F32)
        first = hp - (kernel_taps - 1)
        lane = lax.broadcasted_iota(jnp.int32, (CHUNK, 128), 1)
        for c in [*range(1, rows // CHUNK), 0]:
            if c == 0:
                settle()
            low = c * CHUNK
            total = jnp.broadcast_to(bias[l : l + 1, :].astype(F32), (CHUNK, local))
            for j in range(kernel_taps):
                start = low + first + j
                total = total + tap_rows[j : j + 1, :] * padded[start : start + CHUNK, :]
            filt[low : low + CHUNK, :] = total
            one = jnp.sum(total, axis=1, keepdims=True)
            two = jnp.sum(total * total, axis=1, keepdims=True)
            stat_cols[low : low + CHUNK, :] = jnp.where(
                lane == 0, one, jnp.where(lane == 1, two, 0.0)
            )
        stat_rows[l, t] = jnp.transpose(stat_cols[...])[0:8, :]
        for i in range(1, tp):
            stat_copy(l, i, t).start()

    def activate(l):
        for i in range(1, tp):
            stat_copy(l, i, lax.rem(t + i, tp)).wait_recv()
        sums = jnp.sum(stat_rows[l], axis=0)
        stat_cols[...] = jnp.transpose(
            jnp.concatenate([sums, jnp.zeros((120, rows), F32)], axis=0)
        )
        gains, shifts = ln_gain[l : l + 1, :].astype(F32), ln_shift[l : l + 1, :].astype(F32)

        def body(c, carry):
            at = pl.ds(pl.multiple_of(c * CHUNK, CHUNK), CHUNK)
            average = stat_cols[at, 0:1] / channels
            spread = stat_cols[at, 1:2] / channels - average * average
            v = (filt[at, :] - average) * lax.rsqrt(spread + EPS) * gains + shifts
            acts[l, t, at, :] = (v * sigmoid(v)).astype(BF16)
            return carry

        lax.fori_loop(0, rows // CHUNK, body, 0)

    def update(l):
        columns = width // tp
        tile = min(256, columns)
        deep = 128

        def body(c, carry):
            at = pl.ds(pl.multiple_of(c * deep, deep), deep)
            for n in range(columns // tile):
                cut = slice(n * tile, (n + 1) * tile)
                total = feats[l, t, at, cut].astype(F32)
                for b in range(tp):
                    w = out_all[l, b * share : (b + 1) * share, :, :, :, cut].reshape(local, tile)
                    total = total + jnp.dot(acts[l, b, at, :], w, preferred_element_type=F32)
                if l + 1 < layers:
                    feats[l + 1, t, at, cut] = total.astype(BF16)
                else:
                    result[at, cut] = total.astype(BF16)
            return carry

        lax.fori_loop(0, rows // deep, body, 0)

    hops = range(sp - 1)
    own(0, SIG)
    own(0, GATE)
    own_stream.wait()
    spread_start(feats.at[0], 0)
    for l in range(layers):
        x_cut = [(d, k) for d in hops for k in (SIG, GATE)]
        middle = len(x_cut) - 3 if l == 0 else len(x_cut) - 2
        for i, (d, k) in enumerate(x_cut):
            if l and i == 0:
                continue
            if i == middle:
                if l:
                    own(l, OUT)
                spread_relay(feats.at[l], 2 * l)
            relay(l, k, d)
        if l == 0:
            own(l, OUT)
        spread_wait(feats.at[l], 2 * l)
        normalise(l)
        project(l)

        @pl.when(inner)
        def _(l=l):
            for d in hops:
                relay(l, OUT, d)

        if l + 1 < layers:
            own(l + 1, SIG)
            own(l + 1, GATE)
        convolve(l)

        @pl.when(jnp.logical_not(inner))
        def _(l=l):
            for d in hops:
                relay(l, OUT, d)

        activate(l)
        spread_start(acts.at[l], 2 * l + 1)
        if l + 1 < layers:
            relay(l + 1, SIG, 0)
        spread_relay(acts.at[l], 2 * l + 1)
        for d in hops:
            other_half(l, OUT, d)
        spread_wait(acts.at[l], 2 * l + 1)
        update(l)
        if l + 1 < layers:
            spread_start(feats.at[l + 1], 2 * l + 2)

    for l in range(layers):
        for k in (SIG, GATE, OUT):
            own(l, k, done=True)
            for d in hops:
                relay(l, k, d, done=True)
        spread_done(feats.at[l], 2 * l)
        spread_done(acts.at[l], 2 * l + 1)
        for i in range(1, tp):
            stat_copy(l, i, t).wait_send()

        @pl.when(s < sp - 1)
        def _(l=l):
            halo_copy(l).wait_send()


def direct(l, k, q, count):
    return l > 0 or q < count // 2 or count == 1


def fold_kernel(
    sizes,
    stream, gain_in, w_signal, w_gate, taps_in, bias_in, ln_gain_in, ln_shift_in, w_out,
    result, gain, taps, bias, ln_gain, ln_shift,
    sig_all, gate_all, out_all, feats, far, scaled, squares, acc_sig, acc_gate,
    back, tail, halo, padded, filt, stat_cols, stat_rows, acts,
    final, partial, small_sem, load_sem, stream_sem, final_sem, z_send, end_send, z_recv, y_send, rest_send, y_recv,
    cross_send, cross_recv, core_send, core_recv,
    far_send, far_recv, back_send, back_recv,
    halo_send, halo_recv, stat_send, stat_recv,
):
    groups, sp, tp, layers, rows, kernel_taps, hp, width, channels = sizes
    g, s, t = lax.axis_index("grp"), lax.axis_index("sp"), lax.axis_index("tp")
    chips = tp // 2
    core, chip = lax.rem(t, 2), lax.div(t, 2)
    mate = t + 1 - 2 * core
    last, middle = sp - 1, sp // 2
    outer = (s == 0) | (s == last)
    inner = jnp.logical_not(outer)
    pair = s + 1 - 2 * lax.rem(s, 2)
    mid = jnp.where(outer, pair, s)
    end = jnp.where(outer, s, pair)
    mid2, end2 = last - mid, last - end
    banks = (sig_all, gate_all, out_all)
    held = (w_signal, w_gate, w_out)
    pieces = [w.shape[2] for w in held]
    local, part = channels // tp, width // tp
    parts = [(rows - (h + 1) * DEEP, DEEP) for h in range(rows // DEEP)]
    every = range(len(parts))
    both_in = (SIG, GATE)
    other_group = {"grp": 1 - g}

    def load(l, k):
        return pltpu.make_async_copy(held[k].at[l], banks[k].at[l, s], load_sem.at[l, k])

    own_stream = pltpu.make_async_copy(stream, feats.at[0, t], stream_sem)
    small = [
        pltpu.make_async_copy(ref, to, small_sem.at[i])
        for i, (ref, to) in enumerate((
            (gain_in, gain), (taps_in, taps), (bias_in, bias),
            (ln_gain_in, ln_gain), (ln_shift_in, ln_shift),
        ))
    ]
    barrier = pltpu.get_barrier_semaphore()

    def greet(where):
        pl.semaphore_signal(barrier, inc=1, device_id=where, device_id_type=MESH)

    @pl.when(s > 0)
    def _():
        greet({"sp": s - 1})

    @pl.when(s < last)
    def _():
        greet({"sp": s + 1})

    for i in range(1, groups):
        greet({"grp": lax.rem(g + i, groups)})
    for i in range(1, tp):
        greet({"tp": lax.rem(t + i, tp)})
    for k in both_in:
        load(0, k).start()
    own_stream.start()
    load(0, OUT).start()
    for l in range(1, layers):
        for k in range(3):
            load(l, k).start()
    for copy in small:
        copy.start()
    pl.semaphore_wait(
        barrier,
        jnp.where(s > 0, 1, 0) + jnp.where(s < last, 1, 0) + (groups - 1 + tp - 1),
    )

    where = (pair, mid2, end2, s)

    def z_copy(l, k, q, kind, to, sems, spot):
        ref = banks[k].at[l, where[kind], g, q]
        return pltpu.make_async_remote_copy(
            src_ref=ref, dst_ref=ref,
            send_sem=sems.at[l, k // OUT], recv_sem=z_recv.at[l, k, q, spot],
            device_id={"sp": to}, device_id_type=MESH,
        )

    def y_copy(l, k, q, kind, half, to, sems, spot):
        ref = banks[k].at[l, where[kind], half, q]
        return pltpu.make_async_remote_copy(
            src_ref=ref, dst_ref=ref,
            send_sem=sems.at[l, k // OUT], recv_sem=y_recv.at[l, k, spot],
            device_id=to, device_id_type=MESH,
        )

    def across(l, k, q, kind):
        y_copy(l, k, q, kind, g, other_group, y_send, kind).start()

    def to_end(l, k, q, kind):
        z_copy(l, k, q, kind, end, end_send, PAIR if kind == OWN else kind).start()

    def to_middle(l, k, q, kind):
        z_copy(l, k, q, kind, mid2, z_send, FAR_MID if kind == OWN else FAR_END).start()

    def lift(l, k, q):
        z_copy(l, k, q, OWN, mid, z_send, PAIR).start()

    def lift_other(l, k, q):
        if direct(l, k, q, pieces[k]):
            y_copy(l, k, q, OWN, 1 - g, {"sp": mid}, end_send, PAIR).start()

    def arrived(l, k, q, kind):
        z_copy(l, k, q, kind, mid, z_send, kind).wait_recv()

    def each(l, kinds, act, low=0, high=4):
        for k in kinds:
            for q in range(pieces[k] * low // 4, pieces[k] * high // 4):
                act(l, k, q)

    def pass_on(l, k, q):
        arrived(l, k, q, PAIR)
        to_middle(l, k, q, PAIR)

    def take(kind, onward=True):
        def act(l, k, q):
            arrived(l, k, q, kind)
            if onward:
                to_end(l, k, q, kind)
            if not (onward and kind == FAR_MID and whole(l, k)):
                across(l, k, q, kind)
        return act

    def onward(kind):
        return lambda l, k, q: to_end(l, k, q, kind)

    def bypass(kind):
        return lambda l, k, q: across(l, k, q, kind)

    def share_rest(l, k, q):
        if not direct(l, k, q, pieces[k]):
            y_copy(l, k, q, PAIR, g, other_group, rest_send, PAIR).start()

    def got(kind):
        return lambda l, k, q: arrived(l, k, q, kind)

    def own_in(l, k, q):
        to_middle(l, k, q, OWN)

    def whole(l, k):
        return l == layers - 1 and k == OUT

    def own_other(l, k, q):
        y_copy(l, k, q, OWN, 1 - g, {"sp": mid2}, y_send, FAR_MID).start()

    def ready(l, k, kind):
        ref = banks[k].at[l, where[kind], 1 - g]
        pltpu.make_async_copy(ref, ref, y_recv.at[l, k, kind]).wait()

    def ready_all(l, k):
        for kind in (PAIR, FAR_MID, FAR_END):
            ready(l, k, kind)

    def sent(sems, pick):
        for l in range(layers):
            for kinds in (both_in, (OUT,)):
                k = kinds[0]
                count, half = sum(pick(l, k, pieces[k]) for k in kinds), pieces[k]
                if count == 0:
                    continue
                if count % (2 * half) == 0:
                    ref = banks[k].at[l, pl.ds(0, count // (2 * half))]
                elif count % half == 0:
                    ref = banks[k].at[l, pl.ds(0, count // half), 0]
                else:
                    ref = banks[k].at[l, 0, 0, pl.ds(0, count)]
                pltpu.make_async_copy(ref, ref, sems.at[l, k // OUT]).wait()

    def straight(l, k, count):
        return sum(direct(l, k, q, count) for q in range(count))

    def rows_of(h):
        return pl.ds(parts[h][0], parts[h][1])

    def cross_copy(buf, n, h, block, i):
        ref = buf.at[block, rows_of(h)]
        return pltpu.make_async_remote_copy(
            src_ref=ref, dst_ref=ref,
            send_sem=cross_send.at[n, i - 1], recv_sem=cross_recv.at[n, h, i - 1],
            device_id={"tp": lax.rem(chip + i, chips) * 2 + core}, device_id_type=MESH,
        )

    def core_copy(buf, n, h, block, i):
        ref = buf.at[block, rows_of(h)]
        return pltpu.make_async_remote_copy(
            src_ref=ref, dst_ref=ref,
            send_sem=core_send.at[n, i], recv_sem=core_recv.at[n, h, i],
            device_id={"tp": mate}, device_id_type=MESH,
        )

    def chip_at(i):
        return lax.rem(chip + i, chips) * 2

    def spread_start(buf, n, h):
        for i in range(1, chips):
            cross_copy(buf, n, h, t, i).start()
        core_copy(buf, n, h, t, 0).start()

    def spread_relay(buf, n, h):
        for i in range(1, chips):
            block = chip_at(i) + core
            cross_copy(buf, n, h, block, chips - i).wait_recv()
            core_copy(buf, n, h, block, i).start()

    def spread_near(buf, n, h):
        core_copy(buf, n, h, mate, 0).wait_recv()

    def spread_rest(buf, n, h):
        for i in range(1, chips):
            core_copy(buf, n, h, chip_at(i) + 1 - core, i).wait_recv()

    def spread_done(buf, n):
        ref = buf.at[t]
        for i in range(1, chips):
            pltpu.make_async_copy(ref, ref, cross_send.at[n, i - 1]).wait()
        for i in range(chips):
            pltpu.make_async_copy(ref, ref, core_send.at[n, i]).wait()

    far_blocks = [lax.rem(chip + i, chips) * 2 + c for i in range(1, chips) for c in (core, 1 - core)]
    near_blocks = [t, mate]

    def far_copy(h):
        return pltpu.make_async_remote_copy(
            src_ref=feats.at[0, t, rows_of(h)], dst_ref=far.at[t, rows_of(h)],
            send_sem=far_send, recv_sem=far_recv.at[h],
            device_id={"sp": mid}, device_id_type=MESH,
        )

    def back_copy(h):
        ref = back.at[rows_of(h)]
        return pltpu.make_async_remote_copy(
            src_ref=ref, dst_ref=ref,
            send_sem=back_send, recv_sem=back_recv.at[h],
            device_id={"sp": end}, device_id_type=MESH,
        )

    def stat_copy(l, h, i, block):
        ref = stat_rows.at[l, block, :, rows_of(h)]
        return pltpu.make_async_remote_copy(
            src_ref=ref, dst_ref=ref,
            send_sem=stat_send.at[l, i - 1], recv_sem=stat_recv.at[l, h],
            device_id={"tp": lax.rem(t + i, tp)}, device_id_type=MESH,
        )

    def halo_copy(l):
        return pltpu.make_async_remote_copy(
            src_ref=tail.at[l], dst_ref=halo.at[l],
            send_sem=halo_send.at[l], recv_sem=halo_recv.at[l],
            device_id={"sp": s + 1}, device_id_type=MESH,
        )

    def halo_goes(l):
        return s < last if l else inner

    def over(h, body):
        first, count = parts[h]

        def step(c, carry):
            body(pl.multiple_of(first + c * CHUNK, CHUNK))
            return carry

        lax.fori_loop(0, count // CHUNK, step, 0)

    def scale(which, l, source, b, h, fresh):
        cut = pl.ds(pl.multiple_of(b * part, 128), part)

        def body(low):
            at = pl.ds(low, CHUNK)
            x = source[b, at, :].astype(F32)
            square = x * x
            total = square[:, 0:128]
            for j in range(1, part // 128):
                total = total + square[:, j * 128 : (j + 1) * 128]
            squares[which, at, :] = total if fresh else squares[which, at, :] + total
            scaled[which, b, at, :] = (x * gain[l : l + 1, cut].astype(F32)).astype(BF16)

        over(h, body)

    def accumulate(which, l, b, h, fresh, kinds=(SIG, GATE)):
        at = rows_of(h)
        for k in kinds:
            acc = (acc_sig, acc_gate)[k]
            w = banks[k][l, b].reshape(part, local)
            more = jnp.dot(scaled[which, b, at, :], w, preferred_element_type=F32)
            acc[which, at, :] = more if fresh else acc[which, at, :] + more

    def blend(which, h):
        def body(low):
            at = pl.ds(low, CHUNK)
            total = jnp.sum(squares[which, at, :], axis=1, keepdims=True)
            r = lax.rsqrt(total / width + EPS)
            v = (acc_sig[which, at, :] * r) * sigmoid(acc_gate[which, at, :] * r)
            v = v.astype(BF16)
            if which:
                back[at, :] = v
            else:
                padded[pl.ds(pl.multiple_of(hp + low, 8), CHUNK), :] = v.astype(F32)

        over(h, body)

    def send_tail(l):
        tail[l] = padded[rows : rows + hp, :].astype(BF16)

        @pl.when(halo_goes(l))
        def _():
            halo_copy(l).start()

    def settle(l):
        @pl.when(s >= middle if l == 0 else s > 0)
        def _():
            halo_copy(l).wait_recv()
            padded[0:hp, :] = halo[l].astype(F32)

        if l == 0:
            @pl.when(inner & (s < middle))
            def _():
                padded[0:hp, :] = back[rows - hp : rows, :].astype(F32)

        @pl.when(s == 0)
        def _():
            padded[0:hp, :] = jnp.zeros((hp, local), F32)

    def convolve(l, h, stages=(0, 1)):
        begin, count = parts[h]
        tap_rows = taps[:, l, :].astype(F32)
        first = hp - (kernel_taps - 1)
        lane = lax.broadcasted_iota(jnp.int32, (CHUNK, 128), 1)
        chunks = list(range(begin // CHUNK, (begin + count) // CHUNK))
        chunks = (chunks[1:] if 0 in stages else []) + (chunks[:1] if 1 in stages else [])
        for c in chunks:
            if c == 0:
                settle(l)
            low = c * CHUNK
            total = jnp.broadcast_to(bias[l : l + 1, :].astype(F32), (CHUNK, local))
            for j in range(kernel_taps):
                start = low + first + j
                total = total + tap_rows[j : j + 1, :] * padded[start : start + CHUNK, :]
            filt[low : low + CHUNK, :] = total
            one = jnp.sum(total, axis=1, keepdims=True)
            two = jnp.sum(total * total, axis=1, keepdims=True)
            stat_cols[low : low + CHUNK, :] = jnp.where(
                lane == 0, one, jnp.where(lane == 1, two, 0.0)
            )
        if 1 not in stages:
            return
        at = slice(begin, begin + count)
        stat_rows[l, t, :, at] = jnp.transpose(stat_cols[at, :])[0:8, :]
        for i in range(1, tp):
            stat_copy(l, h, i, t).start()

    def activate(l, h):
        begin, count = parts[h]
        at = slice(begin, begin + count)
        ref = stat_rows.at[l, pl.ds(0, tp - 1), :, rows_of(h)]
        pltpu.make_async_copy(ref, ref, stat_recv.at[l, h]).wait()
        sums = stat_rows[l, 0, :, at]
        for b in range(1, tp):
            sums = sums + stat_rows[l, b, :, at]
        stat_cols[at, :] = jnp.transpose(
            jnp.concatenate([sums, jnp.zeros((120, count), F32)], axis=0)
        )
        gains, shifts = ln_gain[l : l + 1, :].astype(F32), ln_shift[l : l + 1, :].astype(F32)

        def body(low):
            at = pl.ds(low, CHUNK)
            average = stat_cols[at, 0:1] / channels
            spread = stat_cols[at, 1:2] / channels - average * average
            v = (filt[at, :] - average) * lax.rsqrt(spread + EPS) * gains + shifts
            acts[l, t, at, :] = (v * sigmoid(v)).astype(BF16)

        over(h, body)
        spread_start(acts.at[l], layers + l, h)

    def write(h):
        return pltpu.make_async_copy(
            final.at[rows_of(h)], result.at[rows_of(h)], final_sem
        )

    def update(l, h, blocks, fresh=True, finish=True):
        at = rows_of(h)
        tile = min(256, part)
        for n in range(part // tile):
            cut = slice(n * tile, (n + 1) * tile)
            total = feats[l, t, at, cut].astype(F32) if fresh else partial[:, cut]
            for b in blocks:
                w = out_all[l, b, :, :, :, cut].reshape(local, tile)
                total = total + jnp.dot(acts[l, b, at, :], w, preferred_element_type=F32)
            if not finish:
                partial[:, cut] = total
            elif l + 1 < layers:
                feats[l + 1, t, at, cut] = total.astype(BF16)
            else:
                final[at, cut] = total.astype(BF16)
        if finish and l + 1 == layers:
            write(h).start()

    far_n = 2 * layers

    def spread_end(buf, n, h):
        spread_relay(buf, n, h)
        spread_near(buf, n, h)
        spread_rest(buf, n, h)

    def scale_all(which, l, source, h):
        for i, b in enumerate(near_blocks + far_blocks):
            scale(which, l, source, b, h, i == 0)

    def fetch(h):
        back_copy(h).wait_recv()

        def body(low):
            to = pl.ds(pl.multiple_of(hp + low, 8), CHUNK)
            padded[to, :] = back[pl.ds(low, CHUNK), :].astype(F32)

        over(h, body)

    def settle_far(h, blocks):
        for i, b in enumerate(blocks):
            accumulate(1, 0, b, h, i == 0)
        blend(1, h)
        back_copy(h).start()

    @pl.when(outer)
    def _():
        for k in both_in:
            load(0, k).wait()
            each(0, (k,), lift)
        own_stream.wait()
        load(0, OUT).wait()
        for h in every:
            far_copy(h).start()
        each(0, both_in, lift_other)
        each(0, (OUT,), lift)
        for k in range(3):
            load(1, k).wait()
        each(1, (SIG,), lift)
        each(0, (OUT,), lift_other)
        each(1, (GATE,), lift)
        each(1, (SIG,), lift_other)
        each(1, (OUT,), lift)
        each(1, (GATE, OUT), lift_other)
        each(0, (OUT,), take(PAIR, False))
        each(1, range(3), take(PAIR, False))
        each(0, (OUT,), take(FAR_MID, False))
        each(1, (SIG,), take(FAR_MID, False), 0, 3)
        fetch(0)
        each(1, (SIG,), take(FAR_MID, False), 3, 4)

    @pl.when(inner)
    def _():
        for k in both_in:
            load(0, k).wait()
            each(0, (k,), own_in)
        own_stream.wait()
        for h in every:
            spread_start(feats.at[0], 0, h)
        load(0, OUT).wait()
        each(0, (OUT,), onward(OWN))
        for k in range(3):
            load(1, k).wait()
        each(1, range(3), onward(OWN))
        for k in both_in:
            for q in range(pieces[k]):
                pass_on(0, k, q)
                take(FAR_MID, False)(0, k, q)
            spread_relay(feats.at[0], 0, k)
        each(0, (OUT,), own_in)
        each(1, (SIG,), own_in)
        each(0, (SIG,), take(FAR_END, False))
        far_copy(0).wait_recv()
        spread_start(far, far_n, 0)
        for h in every[2:]:
            spread_relay(feats.at[0], 0, h)
        each(0, (GATE,), take(FAR_END, False), 0, 3)
        for h in every[1:-1]:
            far_copy(h).wait_recv()
            spread_start(far, far_n, h)
        each(0, (GATE,), take(FAR_END, False), 3, 4)
        each(0, both_in, share_rest)
        small[0].wait()
        for h in every:
            spread_near(feats.at[0], 0, h)
            spread_rest(feats.at[0], 0, h)
            scale_all(0, 0, feats.at[0], h)
            each(0, (OUT,), take(FAR_MID), h, h + 1)
        spread_end(far, far_n, 0)
        each(0, (OUT,), take(FAR_MID), len(parts), 4)
        scale_all(1, 0, far, 0)
        for k in both_in:
            ready(0, k, FAR_MID)
        for h in every[:1]:
            for i, b in enumerate((s, mid2)):
                accumulate(0, 0, b, h, i == 0)
        far_copy(every[-1]).wait_recv()
        spread_start(far, far_n, every[-1])
        for h in every[1:]:
            for i, b in enumerate((s, mid2)):
                accumulate(0, 0, b, h, i == 0)
        each(1, (SIG,), take(FAR_MID), 0, 1)
        for h in every[1:-1]:
            spread_relay(far, far_n, h)
        each(1, (SIG,), take(FAR_MID), 1, 3)
        for h in every[1:-1]:
            spread_near(far, far_n, h)
            spread_rest(far, far_n, h)
            scale_all(1, 0, far, h)
        for k in both_in:
            ready(0, k, FAR_END)
            ready(0, k, PAIR)
        blocks = (s, mid2, end2, end)
        settle_far(0, blocks)
        each(1, (SIG,), take(FAR_MID), 3, 4)
        each(0, (OUT,), pass_on, 0, 1)
        for h in every[1:-1]:
            settle_far(h, blocks)
        each(0, (OUT,), pass_on, 1, 3)
        spread_end(far, far_n, every[-1])
        scale_all(1, 0, far, every[-1])
        each(0, (OUT,), pass_on, 3, 4)
        each(1, (GATE,), own_in)
        settle_far(every[-1], blocks)
        each(0, (OUT,), share_rest)
        each(0, (OUT,), take(FAR_END), 0, 1)
        for h in every:
            for b in (end2, end):
                accumulate(0, 0, b, h, False)
            blend(0, h)
            if h == 0:
                send_tail(0)
            each(0, (OUT,), take(FAR_END), h + 1, h + 2)
        each(1, (SIG,), pass_on, 0, 2)

    @pl.when(outer)
    def _():
        small[0].wait()

    for copy in small[1:]:
        copy.wait()
    convolve(0, 0, (0,))
    for h in every:
        if h + 1 < len(parts):
            @pl.when(outer)
            def _(h=h):
                fetch(h + 1)

        convolve(0, h, (1,))
        if h + 1 < len(parts):
            convolve(0, h + 1, (0,))

        @pl.when(outer)
        def _(h=h):
            if h:
                each(0, (OUT,), take(FAR_END, False), h - 1, h)

        if h == 0:
            @pl.when(inner)
            def _():
                each(1, (SIG,), pass_on, 2, 3)

    @pl.when(inner)
    def _():
        each(1, (SIG,), pass_on, 3, 4)
        each(1, (GATE,), take(FAR_MID), 0, 2)

    for h in every:
        activate(0, h)
        if h == 0:
            @pl.when(outer)
            def _():
                each(0, (OUT,), take(FAR_END, False), 2, 4)

            @pl.when(inner)
            def _():
                each(1, (GATE,), take(FAR_MID), 2, 4)

    @pl.when(inner)
    def _():
        each(1, (SIG,), take(FAR_END), 0, 1)
        each(1, (GATE,), pass_on, 0, 1)

    @pl.when(outer)
    def _():
        each(1, (GATE,), take(FAR_MID, False), 0, 2)

    for h in every:
        spread_relay(acts.at[0], layers, h)
        spread_near(acts.at[0], layers, h)
        spread_rest(acts.at[0], layers, h)
        if h == 0:
            ready(0, OUT, PAIR)
            ready(0, OUT, FAR_MID)
            update(0, h, (s, pair, mid2), finish=False)
            ready(0, OUT, FAR_END)
            update(0, h, (end2,), fresh=False)
        else:
            update(0, h, range(tp))
        spread_start(feats.at[1], 1, h)

        @pl.when(inner)
        def _(h=h):
            for q in range(2 * h + 1, min(2 * h + 3, 4)):
                each(1, (SIG,), take(FAR_END), q, q + 1)
                each(1, (GATE,), pass_on, q, q + 1)

        @pl.when(outer)
        def _(h=h):
            if h == 0:
                each(1, (GATE,), take(FAR_MID, False), 2, 4)
            else:
                each(1, (SIG,), take(FAR_END, False), h - 1, h)

    x = feats.at[1]
    for h in every:
        scale(0, 1, x, t, h, True)

    @pl.when(inner)
    def _():
        each(1, (OUT,), own_in)
        each(1, (GATE,), take(FAR_END), 0, 2)

    @pl.when(outer)
    def _():
        each(1, (SIG,), take(FAR_END, False), len(parts) - 1, 4)

    for h in every:
        spread_near(x, 1, h)
        scale(0, 1, x, mate, h, False)

    home = lax.div(s, 2) == chip
    first_near, first_far = jnp.where(home, s, mid2), jnp.where(home, mid2, s)

    def fold_far(h):
        for c in (core, 1 - core):
            for i in range(1, chips):
                b = chip_at(i) + c
                scale(0, 1, x, b, h, False)
                accumulate(0, 1, b, h, False, (SIG,))
            if c is core:
                spread_rest(x, 1, h)
        accumulate(0, 1, first_far, h, False, (GATE,))

    @pl.when(inner)
    def _():
        each(1, (GATE,), take(FAR_END), 2, 4)

    for step in range(4):
        @pl.when(inner)
        def _(step=step):
            if step == 0:
                spread_relay(x, 1, 0)
            each(1, (OUT,), take(FAR_MID), step, step + 1)
            each(1, (OUT,), pass_on, step, step + 1)
            if step == 3:
                each(1, (OUT,), own_other)

        @pl.when(outer)
        def _(step=step):
            each(1, (GATE,), take(FAR_END, False), step, step + 1)
            if step == 0:
                spread_relay(x, 1, 0)

        if step == 0:
            ready(1, GATE, FAR_MID)
            for h in every:
                accumulate(0, 1, first_near, h, True, (GATE,))
        if step == 1:
            ready_all(1, SIG)
            for h in every:
                for i, b in enumerate(near_blocks):
                    accumulate(0, 1, b, h, i == 0, (SIG,))
        if step == 2:
            fold_far(0)
    def take_out(kind_outer, kind_inner, low, high):
        @pl.when(outer)
        def _():
            each(1, (OUT,), take(kind_outer, False), low, high)

        if kind_inner is not None:
            @pl.when(inner)
            def _():
                each(1, (OUT,), take(kind_inner), low, high)

    spread_relay(x, 1, 1)
    fold_far(1)
    take_out(FAR_MID, FAR_END, 0, 1)
    ready(1, GATE, PAIR)
    ready(1, GATE, FAR_END)
    take_out(FAR_MID, FAR_END, 1, 2)
    for h in every:
        if h > 1:
            spread_relay(x, 1, h)
            convolve(1, h - 1, (0,))
            take_out(FAR_MID, None, 3, 4)
            fold_far(h)
            take_out(FAR_END, None, 0, 1)
        for b in (pair, end2):
            accumulate(0, 1, b, h, False, (GATE,))
        blend(0, h)
        if h == 0:
            send_tail(1)
            take_out(FAR_MID, FAR_END, 2, 3)
            convolve(1, 0, (0,))
        else:
            convolve(1, h - 1, (1,))
            if h == 1:
                @pl.when(inner)
                def _():
                    each(1, (OUT,), take(FAR_END), 3, 4)
    take_out(FAR_END, None, 1, 2)
    convolve(1, every[-1])
    take_out(FAR_END, None, 2, 3)
    activate(1, 0)
    take_out(FAR_END, None, 3, 4)
    for h in every[1:]:
        activate(1, h)
    gathered, n = acts.at[1], layers + 1
    for h in every[:2]:
        spread_relay(gathered, n, h)
    ready_all(1, OUT)
    for h in every[:-1]:
        spread_near(gathered, n, h)
        spread_rest(gathered, n, h)
        update(1, h, range(tp))
        if h + 2 < len(parts):
            spread_relay(gathered, n, h + 2)
    h = every[-1]
    spread_near(gathered, n, h)
    early = near_blocks + [chip_at(i) + core for i in range(1, chips)]
    update(1, h, early, finish=False)
    spread_rest(gathered, n, h)
    update(1, h, [chip_at(i) + 1 - core for i in range(1, chips)], fresh=False)

    @pl.when(outer)
    def _():
        pltpu.make_async_copy(feats.at[0, t], feats.at[0, t], far_send).wait()
        sent(z_send, lambda l, k, n: n)
        sent(end_send, straight)
        sent(y_send, lambda l, k, n: 3 * n if l or k == OUT else 0)

    @pl.when(inner)
    def _():
        spread_done(feats.at[0], 0)
        spread_done(far, far_n)
        pltpu.make_async_copy(back, back, back_send).wait()
        sent(z_send, lambda l, k, n: 2 * n)
        sent(y_send, lambda l, k, n: 2 * n)
        sent(end_send, lambda l, k, n: 3 * n if l or k == OUT else 0)
        sent(rest_send, lambda l, k, n: n - straight(l, k, n))

    for l in range(layers):
        if l:
            spread_done(feats.at[l], l)
        spread_done(acts.at[l], layers + l)
        for i in range(1, tp):
            ref = stat_rows.at[l, t]
            pltpu.make_async_copy(ref, ref, stat_send.at[l, i - 1]).wait()

        @pl.when(halo_goes(l))
        def _(l=l):
            halo_copy(l).wait_send()

    pltpu.make_async_copy(final, final, final_sem).wait()


def shards(counts, stream, norm_gain, w_signal, w_gate, conv_taps, conv_bias, ln_gain, ln_shift, w_out):
    groups, sp, tp = counts
    layers, deep, local = w_signal.shape
    rows, part = stream.shape
    kernel_taps = conv_taps.shape[1]
    hp = -(-(kernel_taps - 1) // 16) * 16
    width, channels = part * tp, local * tp

    folds = (
        groups == 2 and layers == 2 and sp == tp and sp // 2 == 2
        and rows % DEEP == 0 and rows > DEEP
    )
    wanted = FOLD_PIECES if folds else PIECES

    def cut(w):
        half = w.shape[1] // groups
        count = wanted if half % (16 * wanted) == 0 else 1
        return w.reshape(layers, groups, count, half // count, w.shape[2])

    w_signal, w_gate, w_out = cut(w_signal), cut(w_gate), cut(w_out)
    bank = lambda w: pltpu.VMEM((layers, sp) + w.shape[1:], BF16)
    most = max(w.shape[2] for w in (w_signal, w_gate, w_out))
    line = (layers, 3, most, sp)
    dma = lambda *shape: pltpu.SemaphoreType.DMA(shape)
    anywhere = pl.BlockSpec(memory_space=pl.ANY)
    inside = pl.BlockSpec(memory_space=pltpu.VMEM)
    count = max(1, rows // DEEP)
    spreads, chips = 2 * layers + 1, tp // 2
    if folds:
        body = fold_kernel
        scratch = [
            pltpu.VMEM(norm_gain.shape, BF16),
            pltpu.VMEM((kernel_taps, layers, local), BF16),
            pltpu.VMEM(conv_bias.shape, BF16),
            pltpu.VMEM(ln_gain.shape, BF16),
            pltpu.VMEM(ln_shift.shape, BF16),
            bank(w_signal), bank(w_gate), bank(w_out),
            pltpu.VMEM((layers, tp, rows, part), BF16),
            pltpu.VMEM((tp, rows, part), BF16),
            pltpu.VMEM((2, tp, rows, part), BF16),
            pltpu.VMEM((2, rows, 128), F32),
            pltpu.VMEM((2, rows, local), F32),
            pltpu.VMEM((2, rows, local), F32),
            pltpu.VMEM((rows, local), BF16),
            pltpu.VMEM((layers, hp, local), BF16),
            pltpu.VMEM((layers, hp, local), BF16),
            pltpu.VMEM((hp + rows, local), F32),
            pltpu.VMEM((rows, local), F32),
            pltpu.VMEM((rows, 128), F32),
            pltpu.VMEM((layers, tp, 8, rows), F32),
            pltpu.VMEM((layers, tp, rows, local), BF16),
            pltpu.VMEM((rows, part), BF16),
            pltpu.VMEM((DEEP, part), F32),
            dma(5), dma(layers, 3), pltpu.SemaphoreType.DMA, pltpu.SemaphoreType.DMA,
            dma(layers, 2), dma(layers, 2), dma(layers, 3, most, 3),
            dma(layers, 2), dma(layers, 2), dma(layers, 3, 3),
            dma(spreads, chips - 1), dma(spreads, count, chips - 1),
            dma(spreads, chips), dma(spreads, count, chips),
            pltpu.SemaphoreType.DMA, dma(count), pltpu.SemaphoreType.DMA, dma(count),
            dma(layers), dma(layers), dma(layers, tp - 1), dma(layers, count),
        ]
    else:
        body = kernel
        scratch = [
            bank(w_signal), bank(w_gate), bank(w_out),
            pltpu.VMEM((layers, tp, rows, part), BF16),
            pltpu.VMEM((tp, rows, part), BF16),
            pltpu.VMEM((rows, 128), F32),
            pltpu.VMEM((rows, local), F32),
            pltpu.VMEM((rows, local), F32),
            pltpu.VMEM((layers, hp, local), BF16),
            pltpu.VMEM((layers, hp, local), BF16),
            pltpu.VMEM((hp + rows, local), F32),
            pltpu.VMEM((rows, local), F32),
            pltpu.VMEM((rows, 128), F32),
            pltpu.VMEM((layers, tp, 8, rows), F32),
            pltpu.VMEM((layers, tp, rows, local), BF16),
            dma(layers, 3), pltpu.SemaphoreType.DMA,
            dma(layers, 3, most), dma(*line), dma(*line), dma(*line), dma(*line),
            dma(2 * layers, tp), dma(2 * layers, tp), dma(2 * layers, tp), dma(2 * layers, tp),
            dma(layers), dma(layers), dma(layers, tp), dma(layers, tp),
        ]
    return pl.pallas_call(
        functools.partial(
            body, (groups, sp, tp, layers, rows, kernel_taps, hp, width, channels)
        ),
        out_shape=jax.ShapeDtypeStruct(stream.shape, BF16),
        in_specs=[anywhere] * 9 if folds else [
            anywhere, inside, anywhere, anywhere, inside, inside, inside, inside, anywhere,
        ],
        out_specs=anywhere if folds else inside,
        scratch_shapes=scratch,
        compiler_params=pltpu.CompilerParams(
            collective_id=0, has_side_effects=True, vmem_limit_bytes=60 * 1024 * 1024
        ),
    )(
        stream, norm_gain, w_signal, w_gate, jnp.transpose(conv_taps, (1, 0, 2)), conv_bias,
        ln_gain, ln_shift, w_out,
    )


def solution(mesh):
    counts = tuple(mesh.shape[name] for name in ("grp", "sp", "tp"))
    return jax.shard_map(
        functools.partial(shards, counts),
        mesh=mesh,
        in_specs=(
            P(("grp", "sp"), "tp"),
            P(),
            P(None, "sp", "tp"),
            P(None, "sp", "tp"),
            P(None, None, "tp"),
            P(None, "tp"),
            P(None, "tp"),
            P(None, "tp"),
            P(None, "sp", "tp"),
        ),
        out_specs=P(("grp", "sp"), "tp"),
        check_vma=False,
    )
```
